256 devices in a mesh: kv: 32 (over z, y), tp: 8 (over x, core).
Axes of the slice: x: 4, y: 4, z: 8, core: 2. Of those that a mesh axis runs over, the one named last changes fastest.
Arguments:
- residual_in: bfloat16 [256, 2048], P(None, ('kv', 'tp')), may hold values from -14 to 14
- delta_state: float32 [256, 32, 128, 128], P('kv', 'tp'), may hold values from -1 to 1
- norm_gain_first: float32 [2048], P('kv'), may hold values from 0.1 to 1.9
- gate_first: bfloat16 [2048, 5632], P('kv', 'tp'), may hold values from -0.125 to 0.125
- up_first: bfloat16 [2048, 5632], P('kv', 'tp'), may hold values from -0.125 to 0.125
- down_first: bfloat16 [5632, 2048], P('tp', 'kv'), may hold values from -0.15625 to 0.15625
- norm_gain_mixer: float32 [2048], P('kv'), may hold values from 0.1 to 1.9
- query_weight: bfloat16 [2048, 2048], P('kv', 'tp'), may hold values from -0.125 to 0.125
- key_weight: bfloat16 [2048, 2048], P('kv', 'tp'), may hold values from -0.125 to 0.125
- value_weight: bfloat16 [2048, 4096], P('kv', 'tp'), may hold values from -0.125 to 0.125
- output_gate_weight: bfloat16 [2048, 4096], P('kv', 'tp'), may hold values from -0.125 to 0.125
- beta_weight: bfloat16 [2048, 32], P('kv'), may hold values from -0.125 to 0.125
- decay_weight: bfloat16 [2048, 32], P('kv'), may hold values from -0.125 to 0.125
- decay_rate: float32 [32], P('tp'), may hold values from -2.3 to 1.1
- decay_bias: float32 [32], P('tp'), may hold values from -1 to 1
- head_gain: float32 [128], replicated, may hold values from 0.1 to 1.9
- out_weight: bfloat16 [4096, 2048], P('tp', 'kv'), may hold values from -0.125 to 0.125
- norm_gain_second: float32 [2048], P('kv'), may hold values from 0.1 to 1.9
- gate_second: bfloat16 [2048, 5632], P('kv', 'tp'), may hold values from -0.125 to 0.125
- up_second: bfloat16 [2048, 5632], P('kv', 'tp'), may hold values from -0.125 to 0.125
- down_second: bfloat16 [5632, 2048], P('tp', 'kv'), may hold values from -0.15625 to 0.15625
Outputs:
- residual_out: bfloat16 [256, 2048], P(None, ('kv', 'tp'))
- delta_state_out: float32 [256, 32, 128, 128], P('kv', 'tp')
The draws below stay inside these ranges and needn't reach their ends.
All inputs are finite; a program needn't handle non-finite values.
Results may differ from the reference program's by a relative error of at most 0.03.
Values may be sent and summed in bfloat16 or wider, within the bound.
A program may use at most 64 MiB of HBM per device.

```python
import jax
import jax.numpy as jnp
from jax import lax

D = 2048
FF = 5632
K_HEADS = 16
HEAD = 128
V_HEADS = 32
KW = 2048
VW = 4096
BATCH = 256
N_TP = 8


def draw_residual_in(key, part):
    keys = jax.random.split(key, 4)
    region = jnp.arange(D, dtype=jnp.int32) // (D // 8)
    region_scale = jnp.exp(jax.random.uniform(keys[0], (8,), jnp.float32, -0.6, 0.6))
    column_scale = region_scale[region] * jnp.exp(jax.random.uniform(keys[1], (D,), jnp.float32, -0.2, 0.2))
    base = jnp.clip(jax.random.normal(keys[2], (BATCH, D), jnp.float32), -4.0, 4.0)
    row_scale = jnp.exp(jax.random.uniform(keys[3], (BATCH, 1), jnp.float32, -0.4, 0.4))
    return (base * row_scale * column_scale[None, :]).astype(jnp.bfloat16)


def shard_levels(own_key, dims, cuts, smallest, largest):
    loudness, own = 1.0, jax.random.fold_in(own_key, 6)
    for dim, shards_of in cuts:
        draws = jnp.exp(jax.random.uniform(jax.random.fold_in(own, dim), (shards_of,), jnp.float32, smallest / len(cuts), largest / len(cuts)))
        loudness = loudness * jnp.repeat(draws, dims[dim] // shards_of).reshape([-1 if axis == dim else 1 for axis in range(len(dims))])
    return loudness


def bell_draw(rng, dims, spread, reach, cuts=(), kind=jnp.bfloat16):
    factor_of = shard_levels(rng, dims, cuts, -0.22, 0.18) if cuts else 1.0
    result = jax.random.normal(rng, dims, jnp.float32) * spread * factor_of
    return jnp.minimum(jnp.maximum(result, -reach), reach).astype(kind)


def setup_inputs(seed: int = 0) -> dict:
    key_list = jax.random.split(jax.random.key(seed), 22)
    return {
        "residual_in": draw_residual_in(jax.random.fold_in(key_list[21], 71), 0),
        "delta_state": bell_draw(key_list[1], (BATCH, V_HEADS, HEAD, HEAD), 0.2, 1.0, ((0, 32), (1, 8)), jnp.float32),
        "norm_gain_first": jnp.clip(1.0 + 0.18 * jax.random.normal(key_list[2], (D,), jnp.float32), 0.1, 1.9),
        "gate_first": bell_draw(key_list[3], (D, FF), D ** -0.5, 0.125, ((0, 32), (1, 8))),
        "up_first": bell_draw(key_list[4], (D, FF), D ** -0.5, 0.125, ((0, 32), (1, 8))),
        "down_first": bell_draw(key_list[5], (FF, D), (FF // 4) ** -0.5, 0.15625, ((0, 8), (1, 32))),
        "norm_gain_mixer": jnp.clip(1.0 + 0.18 * jax.random.normal(key_list[6], (D,), jnp.float32), 0.1, 1.9),
        "query_weight": bell_draw(key_list[7], (D, KW), D ** -0.5, 0.125, ((0, 32), (1, 8))),
        "key_weight": bell_draw(key_list[8], (D, KW), D ** -0.5, 0.125, ((0, 32), (1, 8))),
        "value_weight": bell_draw(key_list[9], (D, VW), D ** -0.5, 0.125, ((0, 32), (1, 8))),
        "output_gate_weight": bell_draw(key_list[10], (D, VW), D ** -0.5, 0.125, ((0, 32), (1, 8))),
        "beta_weight": bell_draw(key_list[11], (D, V_HEADS), D ** -0.5, 0.125, ((0, 32),)),
        "decay_weight": bell_draw(key_list[12], (D, V_HEADS), D ** -0.5, 0.125, ((0, 32),)),
        "decay_rate": jnp.clip(-2.3 + 3.4 * jax.random.uniform(key_list[13], (V_HEADS,), jnp.float32) ** shard_levels(key_list[13], (V_HEADS,), ((0, 8),), -0.2, 0.2), -2.3, 1.1),
        "decay_bias": jnp.clip(jax.random.uniform(key_list[14], (V_HEADS,), jnp.float32, -1.0, 1.0) * shard_levels(key_list[14], (V_HEADS,), ((0, 8),), -0.4, 0.0), -1.0, 1.0),
        "head_gain": jnp.clip(1.0 + 0.18 * jax.random.normal(key_list[15], (HEAD,), jnp.float32), 0.1, 1.9),
        "out_weight": bell_draw(key_list[16], (VW, D), (VW // 2) ** -0.5, 0.125, ((0, 8), (1, 32))),
        "norm_gain_second": jnp.clip(1.0 + 0.18 * jax.random.normal(key_list[17], (D,), jnp.float32), 0.1, 1.9),
        "gate_second": bell_draw(key_list[18], (D, FF), D ** -0.5, 0.125, ((0, 32), (1, 8))),
        "up_second": bell_draw(key_list[19], (D, FF), D ** -0.5, 0.125, ((0, 32), (1, 8))),
        "down_second": bell_draw(key_list[20], (FF, D), (FF // 4) ** -0.5, 0.15625, ((0, 8), (1, 32))),
    }


epsilon = 1e-06

def head_sums(left_side, right_side):
    left_parts = left_side.reshape(left_side.shape[0], N_TP, -1).astype(jnp.float32)
    weights = right_side.reshape(N_TP, -1, right_side.shape[1]).astype(jnp.float32)
    pieces = jnp.einsum('btf,tfd->tbd', left_parts, weights)
    rounded = lax.optimization_barrier(pieces.astype(jnp.bfloat16))
    return lax.optimization_barrier(jnp.sum(rounded.astype(jnp.float32), axis=0))

def norm_parts(residual, norm_gain):
    as_float = residual.astype(jnp.float32)
    rowscale = lax.rsqrt(lax.optimization_barrier(jnp.sum(as_float * as_float, axis=1, keepdims=True)) / D + epsilon)
    scaled = (as_float * norm_gain).astype(jnp.bfloat16)
    return (as_float, rowscale, scaled)

def half_ffn(residual, norm_gain, gate_weight, up_weight, down_weight):
    as_float, rowscale, scaled = norm_parts(residual, norm_gain)
    gate_act = jnp.dot(scaled, gate_weight, preferred_element_type=jnp.float32) * rowscale
    up_act = jnp.dot(scaled, up_weight, preferred_element_type=jnp.float32) * rowscale
    hidden = (jax.nn.silu(gate_act) * up_act).astype(jnp.bfloat16)
    branch = head_sums(hidden, down_weight)
    return (as_float + 0.5 * branch).astype(jnp.bfloat16)

def unit_heads(projected, head_size):
    activated = jax.nn.silu(projected).reshape(projected.shape[0], -1, head_size)
    return activated * lax.rsqrt(lax.optimization_barrier(jnp.sum(activated * activated, axis=-1, keepdims=True)) + epsilon)

def delta_step(old_state, key_rows, queries, values, beta_gate, decay_gate):
    faded_state = old_state * decay_gate[:, :, None, None]
    predicted = jnp.einsum('rhab,rha->rhb', faded_state, key_rows, precision=lax.Precision.HIGHEST)
    correction = beta_gate[:, :, None] * (values - predicted)
    updated = faded_state + key_rows[:, :, :, None] * correction[:, :, None, :]
    reading = jnp.einsum('rhab,rha->rhb', updated, queries, precision=lax.Precision.HIGHEST)
    return (updated, reading)

def advance(inputs):
    return delta_step(*inputs)

def reference(residual_in, delta_state, norm_gain_first, gate_first, up_first, down_first, norm_gain_mixer, query_weight, key_weight, value_weight, output_gate_weight, beta_weight, decay_weight, decay_rate, decay_bias, head_gain, out_weight, norm_gain_second, gate_second, up_second, down_second):
    after_first = half_ffn(residual_in, norm_gain_first, gate_first, up_first, down_first)
    as_float, rowscale, scaled = norm_parts(after_first, norm_gain_mixer)

    def project(weight):
        return jnp.dot(scaled, weight, preferred_element_type=jnp.float32) * rowscale
    repeat_count = V_HEADS // K_HEADS
    queries = jnp.repeat(unit_heads(project(query_weight), HEAD) * HEAD ** (-0.5), repeat_count, axis=1)
    key_rows = jnp.repeat(unit_heads(project(key_weight), HEAD), repeat_count, axis=1)
    values = jax.nn.silu(project(value_weight)).reshape(BATCH, V_HEADS, HEAD)
    out_gate = jax.nn.silu(project(output_gate_weight)).reshape(BATCH, V_HEADS, HEAD)
    beta_gate = jax.nn.sigmoid(project(beta_weight))
    decay_gate = jnp.exp(-jnp.exp(decay_rate)[None, :] * jax.nn.softplus(project(decay_weight) + decay_bias[None, :]))
    groups = BATCH // 8
    stacked = tuple((item.reshape((groups, BATCH // groups) + item.shape[1:]) for item in (delta_state, key_rows, queries, values, beta_gate, decay_gate)))
    new_state, reading = lax.map(advance, stacked)
    new_state = new_state.reshape(BATCH, V_HEADS, HEAD, HEAD)
    reading = reading.reshape(BATCH, V_HEADS, HEAD)
    normed = reading * lax.rsqrt(lax.optimization_barrier(jnp.mean(reading * reading, axis=-1, keepdims=True)) + epsilon)
    normed = (normed * head_gain * out_gate).reshape(BATCH, VW).astype(jnp.bfloat16)
    after_mixer = (as_float + head_sums(normed, out_weight)).astype(jnp.bfloat16)
    residual_out = half_ffn(after_mixer, norm_gain_second, gate_second, up_second, down_second)
    return (residual_out, new_state)
```

```python
import jax
import jax.numpy as jnp
from jax import lax
from jax.experimental import pallas as pl
from jax.experimental.pallas import tpu as pltpu
from jax.sharding import PartitionSpec as P

MESH = pl.DeviceIdType.MESH
BF, F32 = jnp.bfloat16, jnp.float32
D, EPS = 2048, 1e-6
NZ, NY, NT = 8, 4, 8
PLANE = NY * NT
KV = NZ * NY
ROWS = 256
KEEP, GROUP = 22, 24
HID = NZ * KEEP
PAD = NZ * GROUP
HEAD = 128

X1, X2, X3, RS1, RS2, AG1, AG2, PR1, PR2, PR3, MIX, EXT, NRM = range(13)
GU1, GU2, DD, MW, WO, GN = range(13, 19)
N_SEM = 19


def dot(a, b, ca, cb):
    return lax.dot_general(a, b, (((ca,), (cb,)), ((), ())), preferred_element_type=F32)


def iota(shape, dim):
    return lax.broadcasted_iota(jnp.int32, shape, dim)


def one_hot(cond):
    return jnp.where(cond, 1.0, 0.0).astype(BF)


def silu(v):
    return v / (1.0 + jnp.exp(-v))


def kernel(
    res, state, gain1, gain2, gain3, gate1, up1, down1, gate2, up2, down2,
    wq, wk, wv, wg, wbeta, wdecay, rate, bias, hgain, wo,
    out, k_out, c_out, d_out,
    s_buf, s_sem, send, recv,
    gu_src, gu_rcv, dd_src, dd_rcv, mw_src, mw_rcv, wo_src, wo_rcv, gn,
    a_w, d_w, g_col,
    xg, rs_src, rs_rcv, hg, pr_src, pr_rcv, m_src, m_rcv, e_src, e_rcv, n_src, n_rcv,
):
    kv = lax.axis_index("kv")
    t = lax.axis_index("tp")
    z, y = lax.div(kv, NY), lax.rem(kv, NY)
    me = y * NT + t

    barrier = pltpu.get_barrier_semaphore()

    def hello_plane(o, c):
        p = lax.rem(me + o, PLANE)
        peer = (z * NY + lax.div(p, NT), lax.rem(p, NT))
        pl.semaphore_signal(barrier, inc=1, device_id=peer, device_id_type=MESH)
        return c

    def hello_kv(o, c):
        pz = lax.rem(z + 1 + lax.div(o, NY), NZ)
        peer = (pz * NY + lax.rem(o, NY), t)
        pl.semaphore_signal(barrier, inc=1, device_id=peer, device_id_type=MESH)
        return c

    lax.fori_loop(1, PLANE, hello_plane, 0)
    lax.fori_loop(0, KV - NY, hello_kv, 0)

    fetch = pltpu.make_async_copy(state, s_buf, s_sem)
    fetch.start()

    def put(src, dst, k, peer):
        pltpu.make_async_remote_copy(
            src_ref=src, dst_ref=dst, send_sem=send.at[k], recv_sem=recv.at[k], device_id=peer, device_id_type=MESH
        ).start()

    def arrived(part, k):
        pltpu.make_async_copy(part, part, recv.at[k]).wait()

    def left(part, k):
        pltpu.make_async_copy(part, part, send.at[k]).wait()

    def to_y(src, dst, k, each):
        def step(o, c):
            p = lax.rem(y + o, NY)
            put(src.at[p] if each else src.at[y], dst.at[y], k, (z * NY + p, t))
            return c

        lax.fori_loop(1, NY, step, 0)
        if each:
            dst[y] = src[y]

    def to_z(src, dst, k, each):
        def step(o, c):
            p = lax.rem(z + o, NZ)
            put(src.at[p] if each else src.at[z], dst.at[z], k, (p * NY + y, t))
            return c

        lax.fori_loop(1, NZ, step, 0)
        if each:
            dst[z] = src[z]

    def to_plane(src, dst, k, each):
        def step(o, c):
            p = lax.rem(me + o, PLANE)
            put(src.at[p] if each else src.at[me], dst.at[me], k, (z * NY + lax.div(p, NT), lax.rem(p, NT)))
            return c

        lax.fori_loop(1, PLANE, step, 0)
        if each:
            dst[me] = src[me]

    eye8 = one_hot(iota((8, 8), 0) == iota((8, 8), 1))
    low = one_hot(iota((64, 128), 0) == iota((64, 128), 1))
    high = one_hot(iota((64, 128), 0) + 64 == iota((64, 128), 1))
    own0 = dot(eye8, res[...], 1, 1)
    xg[0, me] = own0.astype(BF)

    def gate_up(i, gate, up):
        both = dot(gate[...], low, 0, 0) + dot(up[...], high, 0, 0)
        gu_src[i] = both.astype(BF).reshape(NY, HID, 128)

    gate_up(0, gate1, up1)
    eye64 = iota((64, 64), 0) == iota((64, 64), 1)
    gn[y, 0:8] = jnp.broadcast_to(gain1[...], (8, 64))
    gn[y, 8:16] = jnp.broadcast_to(gain2[...], (8, 64))
    gn[y, 16:24] = jnp.broadcast_to(gain3[...], (8, 64))

    pl.semaphore_wait(barrier, PLANE - 1 + KV - NY)

    to_plane(xg.at[0], xg.at[0], X1, False)
    to_y(gn, gn, GN, False)
    to_y(gu_src.at[0], gu_rcv.at[0], GU1, True)

    dd = dot(down1[...], low, 1, 0) + dot(down2[...], high, 1, 0)
    dd_src[...] = dd.astype(BF).reshape(NY, HID, 128)
    to_y(dd_src, dd_rcv, DD, True)

    sel_b = one_hot((iota((32, 128), 0) == iota((32, 128), 1) + 4 * t) & (iota((32, 128), 1) < 4))
    sel_d = one_hot((iota((32, 128), 0) == iota((32, 128), 1) - 4 + 4 * t) & (iota((32, 128), 1) >= 4) & (iota((32, 128), 1) < 8))
    extra = (dot(wbeta[...], sel_b, 1, 0) + dot(wdecay[...], sel_d, 1, 0)).astype(BF)
    blocks = []
    for w in (wq, wk, wv, wg):
        blocks += [(w, j) for j in range(w.shape[1] // 128)]
    for p in range(NY):
        for b in range(3):
            w, j = blocks[3 * p + b]
            mw_src[p, b] = w[:, 128 * j : 128 * (j + 1)]
        mw_src[p, 3] = extra
    to_y(mw_src, mw_rcv, MW, True)

    wo_t = dot(one_hot(eye64), wo[...], 1, 1).astype(BF)
    for p in range(NY):
        wo_src[p] = wo_t[:, 128 * p : 128 * (p + 1)]
    to_y(wo_src, wo_rcv, WO, True)

    gate_up(1, gate2, up2)
    to_y(gu_src.at[1], gu_rcv.at[1], GU2, True)

    def spread(r, c):
        group = jnp.zeros_like(r)
        for i in range(1, NZ):
            group = group + jnp.where(r >= GROUP * i, 1, 0)
        return one_hot((c == r - (GROUP - KEEP) * group) & (r - GROUP * group < KEEP))

    pick = spread(iota((PAD, HID), 0), iota((PAD, HID), 1))
    pick_t = spread(iota((HID, PAD), 1), iota((HID, PAD), 0))
    lane = iota((PAD, 128), 1)

    def make_gate_up(i):
        parts = [dot(pick, gu_rcv[i, p], 1, 0) for p in range(NY)]
        for h in range(2):
            a, b = parts[2 * h], parts[2 * h + 1]
            a_w[i, 0:PAD, 128 * h : 128 * (h + 1)] = jnp.where(lane < 64, a, pltpu.roll(b, 64, 1)).astype(BF)
            a_w[i, PAD : 2 * PAD, 128 * h : 128 * (h + 1)] = jnp.where(lane < 64, pltpu.roll(a, 64, 1), b).astype(BF)

    def make_down():
        for p in range(NY):
            both = dot(dd_rcv[p], pick_t, 0, 0).astype(BF)
            d_w[0, 64 * p : 64 * (p + 1)] = both[0:64]
            d_w[1, 64 * p : 64 * (p + 1)] = both[64:128]

    arrived(gn.at[pl.ds(0, NY - 1)], GN)
    for i in range(3):
        for p in range(NY):
            row = gn[p, 8 * i : 8 * i + 1]
            col = jnp.sum(jnp.where(eye64, jnp.broadcast_to(row, (64, 64)), 0.0), axis=1, keepdims=True)
            g_col[i, 64 * p : 64 * (p + 1)] = jnp.broadcast_to(col, (64, 128))
    arrived(gu_rcv.at[0, pl.ds(0, NY - 1)], GU1)
    make_gate_up(0)

    def gathered(i, k):
        arrived(xg.at[i, pl.ds(0, PLANE - 1)], k)
        x = xg[i].astype(F32).reshape(ROWS, ROWS)
        gain = jnp.concatenate([g_col[i], g_col[i]], axis=1)
        return x * x, (x * gain).astype(BF)

    def half_ffn(i, ix, kx, krs, kag, kpr, prepare):
        squares, scaled = gathered(ix, kx)
        part = dot(a_w[i], scaled, 1, 0)
        total = jnp.sum(squares, axis=0, keepdims=True)
        coarse = total.astype(BF).astype(F32)
        row = iota((NZ, GROUP, ROWS), 1)
        gate = part[0:PAD].reshape(NZ, GROUP, ROWS)
        up = part[PAD : 2 * PAD].reshape(NZ, GROUP, ROWS)
        gate = jnp.where(row == KEEP, coarse.reshape(1, 1, ROWS), gate)
        gate = jnp.where(row == KEEP + 1, (total - coarse).reshape(1, 1, ROWS), gate)
        both = jnp.concatenate([gate, up], axis=1).astype(BF)
        rs_src[i] = both.reshape(NZ, 2 * GROUP // 8, 8, ROWS)
        to_z(rs_src.at[i], rs_rcv.at[i], krs, True)
        prepare()
        arrived(rs_rcv.at[i, pl.ds(0, NZ - 1)], krs)
        both = jnp.sum(rs_rcv[i].astype(F32), axis=0).reshape(2 * GROUP, ROWS)
        gate, up = both[0:GROUP], both[GROUP:]
        scale = lax.rsqrt((gate[KEEP : KEEP + 1] + gate[KEEP + 1 : KEEP + 2]) / D + EPS)
        hidden = silu(gate * scale) * (up * scale)
        hidden = jnp.where(iota((GROUP, ROWS), 0) < KEEP, hidden, 0.0)
        hg[i, z] = hidden.reshape(GROUP // 8, 8, ROWS).astype(BF)
        to_z(hg.at[i], hg.at[i], kag, False)
        arrived(hg.at[i, pl.ds(0, NZ - 1)], kag)
        h = hg[i].astype(F32).reshape(PAD, ROWS).astype(BF)
        return summed(dot(d_w[i], h, 1, 0), 2 * i, kpr)

    def summed(part, j, k):
        pr_src[j] = part.reshape(PLANE, 8, ROWS).astype(BF)
        to_plane(pr_src.at[j], pr_rcv.at[j], k, True)
        arrived(pr_rcv.at[j, pl.ds(0, PLANE - 1)], k)
        return jnp.sum(pr_rcv[j].astype(F32), axis=0)

    def first_prepare():
        arrived(dd_rcv.at[pl.ds(0, NY - 1)], DD)
        make_down()
        arrived(mw_rcv.at[pl.ds(0, NY - 1)], MW)
        arrived(wo_rcv.at[pl.ds(0, NY - 1)], WO)
        arrived(gu_rcv.at[1, pl.ds(0, NY - 1)], GU2)
        make_gate_up(1)

    branch = half_ffn(0, 0, X1, RS1, AG1, PR1, first_prepare)
    own1 = (own0 + 0.5 * branch).astype(BF)
    xg[1, me] = own1
    to_plane(xg.at[1], xg.at[1], X2, False)

    squares, scaled = gathered(1, X2)
    coarse = squares.astype(BF)
    fine = (squares - coarse.astype(F32)).astype(BF)
    at8 = one_hot(iota((ROWS, 128), 1) == 8)
    for b in range(4):
        w = mw_rcv[:, b].reshape(ROWS, 128)
        part = dot(scaled, w, 0, 0)
        if b < 3:
            m_src[:, :, 128 * b : 128 * (b + 1)] = part.reshape(KV, 8, 128).astype(BF)
        else:
            part = part + dot(coarse, at8, 0, 0) + dot(fine, at8, 0, 0)
            e_src[...] = part.reshape(KV, 8, 128)

    def mix_step(o, c):
        p = lax.rem(kv + o, KV)
        put(m_src.at[p], m_rcv.at[kv], MIX, (p, t))
        return c

    lax.fori_loop(1, KV, mix_step, 0)

    def ext_step(o, c):
        p = lax.rem(z + o, NZ) * NY + y
        put(e_src.at[p], e_rcv.at[z], EXT, (p, t))
        return c

    lax.fori_loop(1, NZ, ext_step, 0)
    m_rcv[kv] = m_src[kv]
    e_rcv[z] = e_src[kv]
    fetch.wait()
    arrived(e_rcv.at[pl.ds(0, NZ - 1)], EXT)
    arrived(m_rcv.at[pl.ds(0, KV - 1)], MIX)

    ext = jnp.sum(e_rcv[...], axis=0)
    rowscale = lax.rsqrt(ext[:, 8:9] / D + EPS)
    quarters = [jnp.zeros((8, 384), F32) for _ in range(NY)]
    for s in range(KV):
        quarters[s % NY] = quarters[s % NY] + m_rcv[s].astype(F32)
    heads = []
    for p in range(NY):
        for b in range(3):
            heads.append(quarters[p][:, 128 * b : 128 * (b + 1)] * rowscale)

    def unit(v):
        a = silu(v)
        return a * lax.rsqrt(jnp.sum(a * a, axis=-1, keepdims=True) + EPS)

    q = [unit(heads[m]) * HEAD**-0.5 for m in range(2)]
    k = [unit(heads[2 + m]) for m in range(2)]
    q_t = [jnp.transpose(v) for v in q]
    k_t = [jnp.transpose(v) for v in k]
    kq = [jnp.sum(k[m] * q[m], axis=-1, keepdims=True) for m in range(2)]
    ext = ext * rowscale
    for h in range(4):
        m = h // 2
        val = silu(heads[4 + h])
        gate = silu(heads[8 + h])
        pre = ext[:, h : h + 1]
        beta = 1.0 / (1.0 + jnp.exp(-pre))
        pre = ext[:, 4 + h : 5 + h] + bias[0, h]
        soft = jnp.maximum(pre, 0.0) + jnp.log1p(jnp.exp(-jnp.abs(pre)))
        decay = jnp.exp(-jnp.exp(jnp.full((8, 1), rate[0, h], F32)) * soft)
        by_k, by_q = [], []
        for r in range(8):
            s = s_buf[r, h]
            by_k.append(jnp.sum(s * k_t[m][:, r : r + 1], axis=0, keepdims=True))
            by_q.append(jnp.sum(s * q_t[m][:, r : r + 1], axis=0, keepdims=True))
        by_k = jnp.concatenate(by_k, axis=0)
        by_q = jnp.concatenate(by_q, axis=0)
        corr = beta * (val - decay * by_k)
        reading = decay * by_q + kq[m] * corr
        norm = lax.rsqrt(jnp.mean(reading * reading, axis=-1, keepdims=True) + EPS)
        n_src[h] = (reading * norm * hgain[...] * gate).astype(BF)
        c_out[:, h] = corr
        d_out[:, h : h + 1] = decay
    for m in range(2):
        k_out[:, m] = k[m]

    def norm_step(o, c):
        p = lax.rem(kv + o, KV)
        put(n_src.at[lax.rem(p, NY)], n_rcv.at[kv], NRM, (p, t))
        return c

    lax.fori_loop(1, KV, norm_step, 0)
    n_rcv[kv] = n_src[y]
    arrived(n_rcv.at[pl.ds(0, KV - 1)], NRM)
    normed = n_rcv[...].astype(F32).reshape(ROWS, HEAD).astype(BF)
    branch = summed(dot(wo_rcv[...].reshape(ROWS, HEAD), normed, 1, 1), 1, PR2)
    own2 = (own1.astype(F32) + branch).astype(BF)
    xg[2, me] = own2
    to_plane(xg.at[2], xg.at[2], X3, False)

    branch = half_ffn(1, 2, X3, RS2, AG2, PR3, lambda: None)
    own3 = (own2.astype(F32) + 0.5 * branch).astype(BF)
    out[...] = dot(own3, eye8, 0, 0).astype(BF)

    for i, kk in enumerate((X1, X2, X3)):
        left(xg.at[i, pl.ds(0, PLANE - 1)], kk)
    for i, kk in enumerate((PR1, PR2, PR3)):
        left(pr_src.at[i, pl.ds(0, PLANE - 1)], kk)
    for i, kk in enumerate((RS1, RS2)):
        left(rs_src.at[i, pl.ds(0, NZ - 1)], kk)
    for i, kk in enumerate((AG1, AG2)):
        left(hg.at[i, pl.ds(0, NZ - 1)], kk)
    for i, kk in enumerate((GU1, GU2)):
        left(gu_src.at[i, pl.ds(0, NY - 1)], kk)
    left(dd_src.at[pl.ds(0, NY - 1)], DD)
    left(mw_src.at[pl.ds(0, NY - 1)], MW)
    left(wo_src.at[pl.ds(0, NY - 1)], WO)
    left(gn.at[pl.ds(0, NY - 1)], GN)
    left(m_src.at[pl.ds(0, KV - 1)], MIX)
    left(e_src.at[pl.ds(0, NZ - 1)], EXT)
    left(n_rcv.at[pl.ds(0, KV - 1)], NRM)


def layer(res, state, gain1, gate1, up1, down1, gain2, wq, wk, wv, wg, wbeta, wdecay, rate, bias, hgain, wo, gain3, gate2, up2, down2):
    vmem = pl.BlockSpec(memory_space=pltpu.VMEM)
    smem = pl.BlockSpec(memory_space=pltpu.SMEM)
    specs = [vmem, pl.BlockSpec(memory_space=pl.ANY)] + [vmem] * 15 + [smem] * 2 + [vmem] * 2
    out, k, corr, decay = pl.pallas_call(
        kernel,
        out_shape=(
            jax.ShapeDtypeStruct((ROWS, 8), BF),
            jax.ShapeDtypeStruct((8, 2, HEAD), F32),
            jax.ShapeDtypeStruct((8, 4, HEAD), F32),
            jax.ShapeDtypeStruct((8, 4), F32),
        ),
        in_specs=specs,
        out_specs=(vmem,) * 4,
        scratch_shapes=[
            pltpu.VMEM((8, 4, HEAD, HEAD), F32),
            pltpu.SemaphoreType.DMA,
            pltpu.SemaphoreType.DMA((N_SEM,)),
            pltpu.SemaphoreType.DMA((N_SEM,)),
            pltpu.VMEM((2, NY, HID, 128), BF),
            pltpu.VMEM((2, NY, HID, 128), BF),
            pltpu.VMEM((NY, HID, 128), BF),
            pltpu.VMEM((NY, HID, 128), BF),
            pltpu.VMEM((NY, 4, 64, 128), BF),
            pltpu.VMEM((NY, 4, 64, 128), BF),
            pltpu.VMEM((NY, 64, 128), BF),
            pltpu.VMEM((NY, 64, 128), BF),
            pltpu.VMEM((NY, 24, 64), F32),
            pltpu.VMEM((2, 2 * PAD, ROWS), BF),
            pltpu.VMEM((2, ROWS, PAD), BF),
            pltpu.VMEM((3, ROWS, 128), F32),
            pltpu.VMEM((3, PLANE, 8, ROWS), BF),
            pltpu.VMEM((2, NZ, 2 * GROUP // 8, 8, ROWS), BF),
            pltpu.VMEM((2, NZ, 2 * GROUP // 8, 8, ROWS), BF),
            pltpu.VMEM((2, NZ, GROUP // 8, 8, ROWS), BF),
            pltpu.VMEM((3, PLANE, 8, ROWS), BF),
            pltpu.VMEM((3, PLANE, 8, ROWS), BF),
            pltpu.VMEM((KV, 8, 384), BF),
            pltpu.VMEM((KV, 8, 384), BF),
            pltpu.VMEM((KV, 8, 128), F32),
            pltpu.VMEM((NZ, 8, 128), F32),
            pltpu.VMEM((4, 8, HEAD), BF),
            pltpu.VMEM((KV, 8, HEAD), BF),
        ],
        compiler_params=pltpu.CompilerParams(collective_id=0, has_side_effects=True, vmem_limit_bytes=48 << 20),
    )(
        res, state, gain1[None], gain2[None], gain3[None], gate1, up1, down1, gate2, up2, down2,
        wq, wk, wv, wg, wbeta, wdecay, rate[None], bias[None], hgain[None], wo,
    )
    keys = jnp.repeat(k, 2, axis=1)
    return out, state * decay[:, :, None, None] + keys[:, :, :, None] * corr[:, :, None, :]


def solution(mesh):
    placed = (
        P(None, ("kv", "tp")),
        P("kv", "tp", None, None),
        P("kv"),
        P("kv", "tp"),
        P("kv", "tp"),
        P("tp", "kv"),
        P("kv"),
        P("kv", "tp"),
        P("kv", "tp"),
        P("kv", "tp"),
        P("kv", "tp"),
        P("kv", None),
        P("kv", None),
        P("tp"),
        P("tp"),
        P(),
        P("tp", "kv"),
        P("kv"),
        P("kv", "tp"),
        P("kv", "tp"),
        P("tp", "kv"),
    )
    return jax.shard_map(
        layer,
        mesh=mesh,
        in_specs=placed,
        out_specs=(P(None, ("kv", "tp")), P("kv", "tp", None, None)),
        check_vma=False,
    )
```

```python
import jax
import jax.numpy as jnp
from jax import lax
from jax.experimental import pallas as pl
from jax.experimental.pallas import tpu as pltpu
from jax.sharding import PartitionSpec as P

MESH = pl.DeviceIdType.MESH
BF, F32 = jnp.bfloat16, jnp.float32
D, EPS = 2048, 1e-6
NZ, NY, NT = 8, 4, 8
PLANE = NY * NT
KV = NZ * NY
ROWS = 256
KEEP, GROUP = 22, 24
HID = NZ * KEEP
PAD = NZ * GROUP
HEAD = 128

X1, X2, X3, RS1, RS2, AG1, AG2, PR1, PR2, PR3, MIX, EXT, NRM = range(13)
GU1, GU2, DD, MW, WO, GN = range(13, 19)
N_SEM = 19
STATE_SPACE = pltpu.HBM


def dot(a, b, ca, cb):
    return lax.dot_general(a, b, (((ca,), (cb,)), ((), ())), preferred_element_type=F32)


def iota(shape, dim):
    return lax.broadcasted_iota(jnp.int32, shape, dim)


def one_hot(cond):
    return jnp.where(cond, 1.0, 0.0).astype(BF)


def silu(v):
    return v / (1.0 + jnp.exp(-v))


def kernel(
    res_h, state, gain1_h, gain2_h, gain3_h, gate1_h, up1_h, down1_h, gate2_h, up2_h, down2_h,
    wq_h, wk_h, wv_h, wg_h, wbeta_h, wdecay_h, rate_h, bias_h, hgain_h, wo_h,
    out, state_out,
    res, s_buf, gain1, gain2, gain3, gate1, up1, down1, gate2, up2, down2,
    wq, wk, wv, wg, wbeta, wdecay, rate, bias, hgain, wo,
    in_sem, out_sem, send, recv,
    gu_src, gu_rcv, dd_src, dd_rcv, mw_src, mw_rcv, wo_src, wo_rcv, gn,
    a_w, d_w, g_col,
    xg, rs_src, rs_rcv, hg, pr_src, pr_rcv, m_src, m_rcv, e_src, e_rcv, n_src, n_rcv,
):
    kv = lax.axis_index("kv")
    t = lax.axis_index("tp")
    z, y = lax.div(kv, NY), lax.rem(kv, NY)
    me = y * NT + t

    barrier = pltpu.get_barrier_semaphore()

    def hello_plane(o, c):
        p = lax.rem(me + o, PLANE)
        peer = (z * NY + lax.div(p, NT), lax.rem(p, NT))
        pl.semaphore_signal(barrier, inc=1, device_id=peer, device_id_type=MESH)
        return c

    def hello_kv(o, c):
        pz = lax.rem(z + 1 + lax.div(o, NY), NZ)
        peer = (pz * NY + lax.rem(o, NY), t)
        pl.semaphore_signal(barrier, inc=1, device_id=peer, device_id_type=MESH)
        return c

    lax.fori_loop(1, PLANE, hello_plane, 0)
    lax.fori_loop(0, KV - NY, hello_kv, 0)

    named = {}
    for i, (src, dst) in enumerate((
        (res_h, res), (gate1_h, gate1), (up1_h, up1), (gain1_h, gain1), (gain2_h, gain2), (gain3_h, gain3),
        (down1_h, down1), (down2_h, down2), (wbeta_h, wbeta), (wdecay_h, wdecay), (wq_h, wq), (wk_h, wk), (wv_h, wv), (wg_h, wg),
        (wo_h, wo), (gate2_h, gate2), (up2_h, up2), (rate_h, rate), (bias_h, bias), (hgain_h, hgain), (state, s_buf),
    )):
        named[id(dst)] = pltpu.make_async_copy(src, dst, in_sem.at[i])
        named[id(dst)].start()

    def ready(*refs):
        for ref in refs:
            named[id(ref)].wait()

    def put(src, dst, k, peer):
        pltpu.make_async_remote_copy(
            src_ref=src, dst_ref=dst, send_sem=send.at[k], recv_sem=recv.at[k], device_id=peer, device_id_type=MESH
        ).start()

    def arrived(part, k):
        pltpu.make_async_copy(part, part, recv.at[k]).wait()

    def left(part, k):
        pltpu.make_async_copy(part, part, send.at[k]).wait()

    def to_y(src, dst, k, each):
        def step(o, c):
            p = lax.rem(y + o, NY)
            put(src.at[p] if each else src.at[y], dst.at[y], k, (z * NY + p, t))
            return c

        lax.fori_loop(1, NY, step, 0)
        if each:
            dst[y] = src[y]

    def to_z(src, dst, k, each):
        def step(o, c):
            p = lax.rem(z + o, NZ)
            put(src.at[p] if each else src.at[z], dst.at[z], k, (p * NY + y, t))
            return c

        lax.fori_loop(1, NZ, step, 0)
        if each:
            dst[z] = src[z]

    def to_plane(src, dst, k, each):
        def step(o, c):
            p = lax.rem(me + o, PLANE)
            put(src.at[p] if each else src.at[me], dst.at[me], k, (z * NY + lax.div(p, NT), lax.rem(p, NT)))
            return c

        lax.fori_loop(1, PLANE, step, 0)
        if each:
            dst[me] = src[me]

    low = one_hot(iota((64, 128), 0) == iota((64, 128), 1))
    high = one_hot(iota((64, 128), 0) + 64 == iota((64, 128), 1))
    ready(res)
    own0 = res[...].astype(F32)
    xg[0, me] = res[...]

    def beside(a, b):
        ready(a, b)
        both = dot(a[...], low, 0, 0) + dot(b[...], high, 0, 0)
        return both.astype(BF).reshape(NY, HID, 128)

    gu_src[0] = beside(gate1, up1)
    ready(gain1, gain2, gain3)
    eye64 = iota((64, 64), 0) == iota((64, 64), 1)
    gn[y, 0:8] = jnp.broadcast_to(gain1[...], (8, 64))
    gn[y, 8:16] = jnp.broadcast_to(gain2[...], (8, 64))
    gn[y, 16:24] = jnp.broadcast_to(gain3[...], (8, 64))

    pl.semaphore_wait(barrier, PLANE - 1 + KV - NY)

    to_plane(xg.at[0], xg.at[0], X1, False)
    to_y(gn, gn, GN, False)
    to_y(gu_src.at[0], gu_rcv.at[0], GU1, True)

    dd_src[...] = beside(down1, down2)
    to_y(dd_src, dd_rcv, DD, True)

    sel_b = one_hot((iota((32, 128), 0) == iota((32, 128), 1) + 4 * t) & (iota((32, 128), 1) < 4))
    sel_d = one_hot((iota((32, 128), 0) == iota((32, 128), 1) - 4 + 4 * t) & (iota((32, 128), 1) >= 4) & (iota((32, 128), 1) < 8))
    ready(wbeta, wdecay, wq, wk, wv, wg)
    extra = (dot(wbeta[...], sel_b, 0, 0) + dot(wdecay[...], sel_d, 0, 0)).astype(BF)
    blocks = []
    for w in (wq, wk, wv, wg):
        blocks += [(w, j) for j in range(w.shape[1] // 128)]
    for p in range(NY):
        for b in range(3):
            w, j = blocks[3 * p + b]
            mw_src[p, b] = w[:, 128 * j : 128 * (j + 1)]
        mw_src[p, 3] = extra
    to_y(mw_src, mw_rcv, MW, True)

    ready(wo)
    for p in range(NY):
        wo_src[p] = wo[:, 128 * p : 128 * (p + 1)]
    to_y(wo_src, wo_rcv, WO, True)

    gu_src[1] = beside(gate2, up2)
    to_y(gu_src.at[1], gu_rcv.at[1], GU2, True)

    def spread(r, c):
        group = jnp.zeros_like(r)
        for i in range(1, NZ):
            group = group + jnp.where(r >= GROUP * i, 1, 0)
        return one_hot((c == r - (GROUP - KEEP) * group) & (r - GROUP * group < KEEP))

    pick = spread(iota((PAD, HID), 0), iota((PAD, HID), 1))
    pick_t = spread(iota((HID, PAD), 1), iota((HID, PAD), 0))
    lane = iota((PAD, 128), 1)

    def make_gate_up(i):
        parts = [dot(pick, gu_rcv[i, p], 1, 0) for p in range(NY)]
        for h in range(2):
            a, b = parts[2 * h], parts[2 * h + 1]
            a_w[i, 0:PAD, 128 * h : 128 * (h + 1)] = jnp.where(lane < 64, a, pltpu.roll(b, 64, 1)).astype(BF)
            a_w[i, PAD : 2 * PAD, 128 * h : 128 * (h + 1)] = jnp.where(lane < 64, pltpu.roll(a, 64, 1), b).astype(BF)

    def make_down():
        for p in range(NY):
            both = dot(dd_rcv[p], pick_t, 0, 0).astype(BF)
            d_w[0, 64 * p : 64 * (p + 1)] = both[0:64]
            d_w[1, 64 * p : 64 * (p + 1)] = both[64:128]

    arrived(gn.at[pl.ds(0, NY - 1)], GN)
    for i in range(3):
        for p in range(NY):
            row = gn[p, 8 * i : 8 * i + 1]
            col = jnp.sum(jnp.where(eye64, jnp.broadcast_to(row, (64, 64)), 0.0), axis=1, keepdims=True)
            g_col[i, 64 * p : 64 * (p + 1)] = jnp.broadcast_to(col, (64, 128))
    arrived(gu_rcv.at[0, pl.ds(0, NY - 1)], GU1)
    make_gate_up(0)

    def gathered(i, k):
        arrived(xg.at[i, pl.ds(0, PLANE - 1)], k)
        x = xg[i].astype(F32).reshape(ROWS, ROWS)
        gain = jnp.concatenate([g_col[i], g_col[i]], axis=1)
        return x * x, (x * gain).astype(BF)

    def half_ffn(i, ix, kx, krs, kag, kpr, prepare):
        squares, scaled = gathered(ix, kx)
        part = dot(a_w[i], scaled, 1, 0)
        total = jnp.sum(squares, axis=0, keepdims=True)
        coarse = total.astype(BF).astype(F32)
        row = iota((NZ, GROUP, ROWS), 1)
        gate = part[0:PAD].reshape(NZ, GROUP, ROWS)
        up = part[PAD : 2 * PAD].reshape(NZ, GROUP, ROWS)
        gate = jnp.where(row == KEEP, coarse.reshape(1, 1, ROWS), gate)
        gate = jnp.where(row == KEEP + 1, (total - coarse).reshape(1, 1, ROWS), gate)
        both = jnp.concatenate([gate, up], axis=1).astype(BF)
        rs_src[i] = both.reshape(NZ, 2 * GROUP // 8, 8, ROWS)
        to_z(rs_src.at[i], rs_rcv.at[i], krs, True)
        prepare()
        arrived(rs_rcv.at[i, pl.ds(0, NZ - 1)], krs)
        both = jnp.sum(rs_rcv[i].astype(F32), axis=0).reshape(2 * GROUP, ROWS)
        gate, up = both[0:GROUP], both[GROUP:]
        scale = lax.rsqrt((gate[KEEP : KEEP + 1] + gate[KEEP + 1 : KEEP + 2]) / D + EPS)
        hidden = silu(gate * scale) * (up * scale)
        hidden = jnp.where(iota((GROUP, ROWS), 0) < KEEP, hidden, 0.0)
        hg[i, z] = hidden.reshape(GROUP // 8, 8, ROWS).astype(BF)
        to_z(hg.at[i], hg.at[i], kag, False)
        arrived(hg.at[i, pl.ds(0, NZ - 1)], kag)
        h = hg[i].astype(F32).reshape(PAD, ROWS).astype(BF)
        return summed(dot(d_w[i], h, 1, 0), 2 * i, kpr)

    def summed(part, j, k):
        pr_src[j] = part.reshape(PLANE, 8, ROWS).astype(BF)
        to_plane(pr_src.at[j], pr_rcv.at[j], k, True)
        arrived(pr_rcv.at[j, pl.ds(0, PLANE - 1)], k)
        return jnp.sum(pr_rcv[j].astype(F32), axis=0)

    def first_prepare():
        arrived(dd_rcv.at[pl.ds(0, NY - 1)], DD)
        make_down()
        arrived(mw_rcv.at[pl.ds(0, NY - 1)], MW)
        arrived(wo_rcv.at[pl.ds(0, NY - 1)], WO)
        arrived(gu_rcv.at[1, pl.ds(0, NY - 1)], GU2)
        make_gate_up(1)

    branch = half_ffn(0, 0, X1, RS1, AG1, PR1, first_prepare)
    own1 = (own0 + 0.5 * branch).astype(BF)
    xg[1, me] = own1
    to_plane(xg.at[1], xg.at[1], X2, False)

    squares, scaled = gathered(1, X2)
    coarse = squares.astype(BF)
    fine = (squares - coarse.astype(F32)).astype(BF)
    at8 = one_hot(iota((ROWS, 128), 1) == 8)
    for b in range(4):
        w = mw_rcv[:, b].reshape(ROWS, 128)
        part = dot(scaled, w, 0, 0)
        if b < 3:
            m_src[:, :, 128 * b : 128 * (b + 1)] = part.reshape(KV, 8, 128).astype(BF)
        else:
            part = part + dot(coarse, at8, 0, 0) + dot(fine, at8, 0, 0)
            e_src[...] = part.reshape(KV, 8, 128)

    def mix_step(o, c):
        p = lax.rem(kv + o, KV)
        put(m_src.at[p], m_rcv.at[kv], MIX, (p, t))
        return c

    lax.fori_loop(1, KV, mix_step, 0)

    def ext_step(o, c):
        p = lax.rem(z + o, NZ) * NY + y
        put(e_src.at[p], e_rcv.at[z], EXT, (p, t))
        return c

    lax.fori_loop(1, NZ, ext_step, 0)
    m_rcv[kv] = m_src[kv]
    e_rcv[z] = e_src[kv]
    ready(s_buf, rate, bias, hgain)
    arrived(e_rcv.at[pl.ds(0, NZ - 1)], EXT)
    arrived(m_rcv.at[pl.ds(0, KV - 1)], MIX)

    ext = jnp.sum(e_rcv[...], axis=0)
    rowscale = lax.rsqrt(ext[:, 8:9] / D + EPS)
    quarters = [jnp.zeros((8, 384), F32) for _ in range(NY)]
    for s in range(KV):
        quarters[s % NY] = quarters[s % NY] + m_rcv[s].astype(F32)
    heads = []
    for p in range(NY):
        for b in range(3):
            heads.append(quarters[p][:, 128 * b : 128 * (b + 1)] * rowscale)

    def unit(v):
        a = silu(v)
        return a * lax.rsqrt(jnp.sum(a * a, axis=-1, keepdims=True) + EPS)

    q = [unit(heads[m]) * HEAD**-0.5 for m in range(2)]
    k = [unit(heads[2 + m]) for m in range(2)]
    q_t = [jnp.transpose(v) for v in q]
    k_t = [jnp.transpose(v) for v in k]
    kq = [jnp.sum(k[m] * q[m], axis=-1, keepdims=True) for m in range(2)]
    ext = ext * rowscale
    new = []
    for h in range(4):
        m = h // 2
        val = silu(heads[4 + h])
        gate = silu(heads[8 + h])
        pre = ext[:, h : h + 1]
        beta = 1.0 / (1.0 + jnp.exp(-pre))
        pre = ext[:, 4 + h : 5 + h] + bias[:, h : h + 1]
        soft = jnp.maximum(pre, 0.0) + jnp.log1p(jnp.exp(-jnp.abs(pre)))
        decay = jnp.exp(-jnp.exp(rate[:, h : h + 1]) * soft)
        by_k, by_q = [], []
        for r in range(8):
            s = s_buf[r, h]
            by_k.append(jnp.sum(s * k_t[m][:, r : r + 1], axis=0, keepdims=True))
            by_q.append(jnp.sum(s * q_t[m][:, r : r + 1], axis=0, keepdims=True))
        by_k = jnp.concatenate(by_k, axis=0)
        by_q = jnp.concatenate(by_q, axis=0)
        corr = beta * (val - decay * by_k)
        reading = decay * by_q + kq[m] * corr
        norm = lax.rsqrt(jnp.mean(reading * reading, axis=-1, keepdims=True) + EPS)
        n_src[h] = (reading * norm * hgain[...] * gate).astype(BF)
        new.append((decay, corr))

    def norm_step(o, c):
        p = lax.rem(kv + o, KV)
        put(n_src.at[lax.rem(p, NY)], n_rcv.at[kv], NRM, (p, t))
        return c

    lax.fori_loop(1, KV, norm_step, 0)
    n_rcv[kv] = n_src[y]
    for h in range(4):
        decay, corr = new[h]
        for r in range(8):
            col = k_t[h // 2][:, r : r + 1]
            s_buf[r, h] = s_buf[r, h] * decay[r : r + 1] + col * corr[r : r + 1]
    store = pltpu.make_async_copy(s_buf, state_out, out_sem)
    store.start()
    arrived(n_rcv.at[pl.ds(0, KV - 1)], NRM)
    normed = n_rcv[...].astype(F32).reshape(ROWS, HEAD).astype(BF)
    branch = summed(dot(wo_rcv[...].reshape(ROWS, HEAD), normed, 1, 1), 1, PR2)
    own2 = (own1.astype(F32) + branch).astype(BF)
    xg[2, me] = own2
    to_plane(xg.at[2], xg.at[2], X3, False)

    branch = half_ffn(1, 2, X3, RS2, AG2, PR3, lambda: None)
    own3 = (own2.astype(F32) + 0.5 * branch).astype(BF)
    out[...] = own3
    store.wait()

    for i, kk in enumerate((X1, X2, X3)):
        left(xg.at[i, pl.ds(0, PLANE - 1)], kk)
    for i, kk in enumerate((PR1, PR2, PR3)):
        left(pr_src.at[i, pl.ds(0, PLANE - 1)], kk)
    for i, kk in enumerate((RS1, RS2)):
        left(rs_src.at[i, pl.ds(0, NZ - 1)], kk)
    for i, kk in enumerate((AG1, AG2)):
        left(hg.at[i, pl.ds(0, NZ - 1)], kk)
    for i, kk in enumerate((GU1, GU2)):
        left(gu_src.at[i, pl.ds(0, NY - 1)], kk)
    left(dd_src.at[pl.ds(0, NY - 1)], DD)
    left(mw_src.at[pl.ds(0, NY - 1)], MW)
    left(wo_src.at[pl.ds(0, NY - 1)], WO)
    left(gn.at[pl.ds(0, NY - 1)], GN)
    left(m_src.at[pl.ds(0, KV - 1)], MIX)
    left(e_src.at[pl.ds(0, NZ - 1)], EXT)
    left(n_rcv.at[pl.ds(0, KV - 1)], NRM)


def layer(res, state, gain1, gate1, up1, down1, gain2, wq, wk, wv, wg, wbeta, wdecay, rate, bias, hgain, wo, gain3, gate2, up2, down2):
    args = (
        res.T, state, gain1[None], gain2[None], gain3[None], gate1, up1, down1.T, gate2, up2, down2.T,
        wq, wk, wv, wg, wbeta.T, wdecay.T, rate[None], bias[None], hgain[None], wo.T,
    )
    out, new_state = pl.pallas_call(
        kernel,
        out_shape=(jax.ShapeDtypeStruct((8, ROWS), BF), jax.ShapeDtypeStruct(state.shape, F32)),
        in_specs=[pl.BlockSpec(memory_space=pltpu.HBM)] * len(args),
        out_specs=(pl.BlockSpec(memory_space=pltpu.VMEM), pl.BlockSpec(memory_space=STATE_SPACE)),
        scratch_shapes=[pltpu.VMEM(a.shape, a.dtype) for a in args]
        + [
            pltpu.SemaphoreType.DMA((len(args),)),
            pltpu.SemaphoreType.DMA,
            pltpu.SemaphoreType.DMA((N_SEM,)),
            pltpu.SemaphoreType.DMA((N_SEM,)),
            pltpu.VMEM((2, NY, HID, 128), BF),
            pltpu.VMEM((2, NY, HID, 128), BF),
            pltpu.VMEM((NY, HID, 128), BF),
            pltpu.VMEM((NY, HID, 128), BF),
            pltpu.VMEM((NY, 4, 64, 128), BF),
            pltpu.VMEM((NY, 4, 64, 128), BF),
            pltpu.VMEM((NY, 64, 128), BF),
            pltpu.VMEM((NY, 64, 128), BF),
            pltpu.VMEM((NY, 24, 64), F32),
            pltpu.VMEM((2, 2 * PAD, ROWS), BF),
            pltpu.VMEM((2, ROWS, PAD), BF),
            pltpu.VMEM((3, ROWS, 128), F32),
            pltpu.VMEM((3, PLANE, 8, ROWS), BF),
            pltpu.VMEM((2, NZ, 2 * GROUP // 8, 8, ROWS), BF),
            pltpu.VMEM((2, NZ, 2 * GROUP // 8, 8, ROWS), BF),
            pltpu.VMEM((2, NZ, GROUP // 8, 8, ROWS), BF),
            pltpu.VMEM((3, PLANE, 8, ROWS), BF),
            pltpu.VMEM((3, PLANE, 8, ROWS), BF),
            pltpu.VMEM((KV, 8, 384), BF),
            pltpu.VMEM((KV, 8, 384), BF),
            pltpu.VMEM((KV, 8, 128), F32),
            pltpu.VMEM((NZ, 8, 128), F32),
            pltpu.VMEM((4, 8, HEAD), BF),
            pltpu.VMEM((KV, 8, HEAD), BF),
        ],
        compiler_params=pltpu.CompilerParams(collective_id=0, has_side_effects=True, vmem_limit_bytes=67_043_328),
    )(*args)
    return out.T, new_state


def solution(mesh):
    placed = (
        P(None, ("kv", "tp")),
        P("kv", "tp", None, None),
        P("kv"),
        P("kv", "tp"),
        P("kv", "tp"),
        P("tp", "kv"),
        P("kv"),
        P("kv", "tp"),
        P("kv", "tp"),
        P("kv", "tp"),
        P("kv", "tp"),
        P("kv", None),
        P("kv", None),
        P("tp"),
        P("tp"),
        P(),
        P("tp", "kv"),
        P("kv"),
        P("kv", "tp"),
        P("kv", "tp"),
        P("tp", "kv"),
    )
    return jax.shard_map(
        layer,
        mesh=mesh,
        in_specs=placed,
        out_specs=(P(None, ("kv", "tp")), P("kv", "tp", None, None)),
        check_vma=False,
    )
```

```python
import jax
import jax.numpy as jnp
from jax import lax
from jax.experimental import pallas as pl
from jax.experimental.pallas import tpu as pltpu
from jax.sharding import PartitionSpec as P

MESH = pl.DeviceIdType.MESH
BF, F32 = jnp.bfloat16, jnp.float32
D, EPS = 2048, 1e-6
NZ, NY, NT = 8, 4, 8
PLANE = NY * NT
KV = NZ * NY
ROWS = 256
KEEP, GROUP = 22, 24
HID = NZ * KEEP
PAD = NZ * GROUP
HEAD = 128

X1, X2, X3, RS1, RS2, AG1, AG2, PR1, PR2, PR3, MIX, NRM, GU1, DD, GN = range(15)
MW, WO, GU2, D2 = 15, 19, 23, 27
N_SEM = 31
MCOLS = 1664
FFT, FFP = 704, 768
RING_Z = (4, 3, 5, 2, 6, 1, 7)
FAR = (0, 1, 2, 1)


def dot(a, b, ca, cb):
    return lax.dot_general(a, b, (((ca,), (cb,)), ((), ())), preferred_element_type=F32)


def iota(shape, dim):
    return lax.broadcasted_iota(jnp.int32, shape, dim)


def one_hot(cond):
    return jnp.where(cond, 1.0, 0.0).astype(BF)


def silu(v):
    return v / (1.0 + jnp.exp(-v))


def kernel(
    res_h, state, gain1_h, gain2_h, gain3_h, gate1_h, up1_h, down1_h, gate2_h, up2_h, down2_h,
    wq_h, wk_h, wv_h, wg_h, wbeta_h, wdecay_h, rate_h, bias_h, hgain_h, wo_h,
    out, k_out, c_out, d_out,
    res, s_buf, gain1, gain2, gain3, gate1, up1, down1, wbeta, wdecay, rate, bias, hgain,
    in_sem, send, recv,
    gu_src, gu_rcv, dd_src, dd_rcv, gn, mw, wo, gu2, d2,
    a_w, d_w, g_col, g_row, xrow,
    xg, rs_src, rs_rcv, hg, pr1_src, pr1_rcv,
    xb, m_src, m_rcv, nb, pr2_src, pr2_rcv, rs2_src, rs2_rcv, hg2, pr3_src, pr3_rcv,
):
    kv = lax.axis_index("kv")
    t = lax.axis_index("tp")
    z, y = lax.div(kv, NY), lax.rem(kv, NY)
    x, core = lax.div(t, 2), lax.rem(t, 2)
    me = y * NT + t
    zs = [lax.rem(z + o, NZ) for o in range(NZ)]
    ys = [lax.rem(y + o, NY) for o in range(NY)]
    ts = [[lax.rem(x + o, 4) * 2 + c for c in (core, 1 - core)] for o in range(4)]

    z_peers = [(zs[o], (zs[o] * NY + y, t)) for o in RING_Z]
    y_peers = [(ys[o], (z * NY + ys[o], t)) for o in (2, 1, 3)]
    t_peers = [(ts[dx][dc], (kv, ts[dx][dc])) for dx in (2, 1, 3, 0) for dc in (0, 1) if dx or dc]
    plane = [(dy, dx, dc) for dy in range(4) for dx in range(4) for dc in range(2) if dy or dx or dc]
    plane.sort(key=lambda o: -(FAR[o[0]] + FAR[o[1]]))
    plane_peers = [(ys[dy] * NT + ts[dx][dc], (z * NY + ys[dy], ts[dx][dc])) for dy, dx, dc in plane]

    barrier = pltpu.get_barrier_semaphore()
    greet = z_peers[:3] + plane_peers[:10] + z_peers[3:5] + plane_peers[10:] + z_peers[5:]
    for _, peer in greet:
        pl.semaphore_signal(barrier, inc=1, device_id=peer, device_id_type=MESH)

    named = {}
    for i, (src, dst) in enumerate((
        (gate1_h, gate1), (up1_h, up1), (res_h, res), (gain1_h, gain1), (gain2_h, gain2), (gain3_h, gain3), (down1_h, down1),
        (wbeta_h, wbeta), (wdecay_h, wdecay),
        (wq_h, mw.at[y, :, 0:256]), (wk_h, mw.at[y, :, 256:512]), (wv_h, mw.at[y, :, 512:1024]), (wg_h, mw.at[y, :, 1024:1536]),
        (wo_h, wo.at[y]), (gate2_h, gu2.at[y, 0]), (up2_h, gu2.at[y, 1]), (down2_h, d2.at[y]),
        (rate_h, rate), (bias_h, bias), (hgain_h, hgain), (state, s_buf),
    )):
        named[id(src)] = pltpu.make_async_copy(src, dst, in_sem.at[i])
        named[id(src)].start()

    def ready(*refs):
        for ref in refs:
            named[id(ref)].wait()

    def put(src, dst, k, peer):
        pltpu.make_async_remote_copy(
            src_ref=src, dst_ref=dst, send_sem=send.at[k], recv_sem=recv.at[k], device_id=peer, device_id_type=MESH
        ).start()

    def arrived(part, k):
        pltpu.make_async_copy(part, part, recv.at[k]).wait()

    def left(part, k):
        pltpu.make_async_copy(part, part, send.at[k]).wait()

    def share(buf, own, k, peers):
        for _, peer in peers:
            put(buf.at[own], buf.at[own], k, peer)

    def deal(src, dst, own, k, peers):
        for p, peer in peers:
            put(src.at[p], dst.at[own], k, peer)
        dst[own] = src[own]

    above, below = (z * NY + ys[1], t), (z * NY + ys[3], t)

    def y_start(buf, k):
        put(buf.at[y], buf.at[y], k, above)
        put(buf.at[y], buf.at[y], k + 1, below)

    def halves(buf, p):
        n = buf.shape[1] // 2
        return buf.at[p, pl.ds(0, n)], buf.at[p, pl.ds(n, n)]

    def y_pass(buf, k):
        arrived(buf.at[ys[3]], k)
        first, second = halves(buf, ys[3])
        put(first, first, k + 2, above)
        arrived(buf.at[ys[1]], k + 1)
        first, second = halves(buf, ys[1])
        put(second, second, k + 3, below)

    def y_done(buf, k):
        first, second = halves(buf, ys[2])
        arrived(first, k + 2)
        arrived(second, k + 3)

    def y_left(buf, k):
        first, second = halves(buf, 0)
        left(buf.at[0], k)
        left(buf.at[0], k + 1)
        left(first, k + 2)
        left(second, k + 3)

    low = one_hot(iota((64, 128), 0) == iota((64, 128), 1))
    high = one_hot(iota((64, 128), 0) + 64 == iota((64, 128), 1))
    eye64 = iota((64, 64), 0) == iota((64, 64), 1)

    ready(gate1_h, up1_h)
    both = dot(gate1[...], low, 0, 0) + dot(up1[...], high, 0, 0)
    gu_src[...] = both.astype(BF).reshape(NY, HID, 128)
    ready(res_h, gain1_h, gain2_h, gain3_h)
    xg[me] = res[...]
    gn[y, 0:8] = jnp.broadcast_to(gain1[...], (8, 64))
    gn[y, 8:16] = jnp.broadcast_to(gain2[...], (8, 64))
    gn[y, 16:24] = jnp.broadcast_to(gain3[...], (8, 64))

    pl.semaphore_wait(barrier, len(greet))

    deal(gu_src, gu_rcv, y, GU1, y_peers)
    share(xg, me, X1, plane_peers)
    share(gn, y, GN, y_peers)

    ready(down1_h)
    dd_src[...] = dot(down1[...], low, 0, 0).astype(BF).reshape(NY, HID, 128)
    sel_b = one_hot((iota((32, 128), 0) == iota((32, 128), 1) + 4 * t) & (iota((32, 128), 1) < 4))
    sel_d = one_hot((iota((32, 128), 0) == iota((32, 128), 1) - 4 + 4 * t) & (iota((32, 128), 1) >= 4) & (iota((32, 128), 1) < 8))
    ready(wbeta_h, wdecay_h)
    mw[y, :, 1536:MCOLS] = (dot(wbeta[...], sel_b, 0, 0) + dot(wdecay[...], sel_d, 0, 0)).astype(BF)

    r, c = iota((PAD, HID), 0), iota((PAD, HID), 1)
    group = jnp.zeros_like(r)
    for i in range(1, NZ):
        group = group + jnp.where(r >= GROUP * i, 1, 0)
    pick = one_hot((c == r - (GROUP - KEEP) * group) & (r - GROUP * group < KEEP))
    lane = iota((PAD, 128), 1)

    def column(p, i):
        row = gn[p, 8 * i : 8 * i + 1]
        return jnp.sum(jnp.where(eye64, jnp.broadcast_to(row, (64, 64)), 0.0), axis=1, keepdims=True)

    arrived(gn.at[pl.ds(0, NY - 1)], GN)
    for p in range(NY):
        g_col[64 * p : 64 * (p + 1)] = jnp.broadcast_to(column(p, 0), (64, ROWS))
    arrived(gu_rcv.at[pl.ds(0, NY - 1)], GU1)
    parts = [dot(pick, gu_rcv[p], 1, 0) for p in range(NY)]
    for h in range(2):
        a, b = parts[2 * h], parts[2 * h + 1]
        a_w[0:PAD, 128 * h : 128 * (h + 1)] = jnp.where(lane < 64, a, pltpu.roll(b, 64, 1)).astype(BF)
        a_w[PAD : 2 * PAD, 128 * h : 128 * (h + 1)] = jnp.where(lane < 64, pltpu.roll(a, 64, 1), b).astype(BF)

    arrived(xg.at[pl.ds(0, PLANE - 1)], X1)
    x0 = xg[...].astype(F32).reshape(ROWS, ROWS)
    part = dot(a_w[...], (x0 * g_col[...]).astype(BF), 1, 0)
    total = jnp.sum(x0 * x0, axis=0, keepdims=True)
    coarse = total.astype(BF).astype(F32)
    row = iota((NZ, GROUP, ROWS), 1)
    gate = part[0:PAD].reshape(NZ, GROUP, ROWS)
    up = part[PAD : 2 * PAD].reshape(NZ, GROUP, ROWS)
    gate = jnp.where(row == KEEP, coarse.reshape(1, 1, ROWS), gate)
    gate = jnp.where(row == KEEP + 1, (total - coarse).reshape(1, 1, ROWS), gate)
    rs_src[...] = jnp.concatenate([gate, up], axis=1).astype(BF).reshape(NZ, 2 * GROUP // 8, 8, ROWS)
    deal(rs_src, rs_rcv, z, RS1, z_peers)

    for p, peer in y_peers:
        put(dd_src.at[p], dd_rcv.at[y], DD, peer)
    dd_rcv[y] = dd_src[y]
    ready(wq_h, wk_h, wv_h, wg_h)
    y_start(mw, MW)
    xrow[...] = jnp.transpose(x0).reshape(KV, 8, ROWS).astype(BF)
    lane64 = iota((64, 128), 1)
    for i in range(2):
        for h in range(2):
            spread = jnp.where(lane64 == iota((64, 128), 0), column(2 * h, i + 1), 0.0)
            spread = spread + jnp.where(lane64 == iota((64, 128), 0) + 64, column(2 * h + 1, i + 1), 0.0)
            g_row[i, :, 128 * h : 128 * (h + 1)] = jnp.broadcast_to(jnp.sum(spread, axis=0, keepdims=True), (8, 128))

    arrived(rs_rcv.at[pl.ds(0, NZ - 1)], RS1)
    both = jnp.sum(rs_rcv[...].astype(F32), axis=0).reshape(2 * GROUP, ROWS)
    gate, up = both[0:GROUP], both[GROUP:]
    scale = lax.rsqrt((gate[KEEP : KEEP + 1] + gate[KEEP + 1 : KEEP + 2]) / D + EPS)
    hidden = silu(gate * scale) * (up * scale)
    hidden = jnp.where(iota((GROUP, ROWS), 0) < KEEP, hidden, 0.0)
    hg[z] = hidden.reshape(GROUP // 8, 8, ROWS).astype(BF)
    share(hg, z, AG1, z_peers)

    arrived(dd_rcv.at[pl.ds(0, NY - 1)], DD)
    for h in range(2):
        a, b = dot(pick, dd_rcv[2 * h], 1, 0), dot(pick, dd_rcv[2 * h + 1], 1, 0)
        d_w[:, 128 * h : 128 * (h + 1)] = (a + pltpu.roll(b, 64, 1)).astype(BF)
    y_pass(mw, MW)
    arrived(hg.at[pl.ds(0, NZ - 1)], AG1)
    h = hg[...].astype(F32).reshape(PAD, ROWS).astype(BF)
    pr1_src[...] = dot(h, d_w[...], 0, 0).reshape(KV, 8, ROWS).astype(BF)
    for (dy, dx, dc), (_, peer) in zip(plane, plane_peers):
        put(pr1_src.at[ts[dx][dc] * NY + ys[dy]], pr1_rcv.at[me], PR1, peer)
    pr1_rcv[me] = pr1_src[t * NY + y]
    arrived(pr1_rcv.at[pl.ds(0, PLANE - 1)], PR1)
    branch = jnp.sum(pr1_rcv[...].astype(F32), axis=0)
    own1 = (xrow[t * NY + y].astype(F32) + 0.5 * branch).astype(BF)

    def gathered(i, own, k):
        xb[i, t] = own
        share(xb.at[i], t, k, t_peers)

    def scaled_of(i, k):
        arrived(xb.at[i, pl.ds(0, NT - 1)], k)
        v = xb[i].astype(F32).reshape(64, ROWS)
        squares = jnp.sum(v * v, axis=1, keepdims=True)
        coarse = squares.astype(BF).astype(F32)
        return v, (v * g_row[i, 0:1]).astype(BF), coarse, squares - coarse

    gathered(0, own1, X2)
    y_done(mw, MW)
    _, scaled, coarse, fine = scaled_of(0, X2)
    last = iota((64, 128), 1)
    for a, b in ((0, 512), (512, 1024), (1024, 1536), (1536, MCOLS)):
        part = dot(scaled, mw[:, :, a:b].reshape(ROWS, b - a), 1, 0)
        if a == 1536:
            part = part + jnp.where(last == 8, coarse, 0.0) + jnp.where(last == 9, fine, 0.0)
        m_src[:, :, a:b] = part.reshape(NZ, 8, b - a).astype(BF)
    deal(m_src, m_rcv, z, MIX, z_peers)
    ready(wo_h, gate2_h, up2_h, down2_h, state, rate_h, bias_h, hgain_h)
    y_start(wo, WO)
    y_start(gu2, GU2)
    arrived(m_rcv.at[pl.ds(0, NZ - 1)], MIX)

    mixed = jnp.sum(m_rcv[...].astype(F32), axis=0)
    ext = mixed[:, 1536:MCOLS]
    rowscale = lax.rsqrt((ext[:, 8:9] + ext[:, 9:10]) / D + EPS)
    heads = [mixed[:, 128 * i : 128 * (i + 1)] * rowscale for i in range(12)]

    def unit(v):
        a = silu(v)
        return a * lax.rsqrt(jnp.sum(a * a, axis=-1, keepdims=True) + EPS)

    q = [unit(heads[m]) * HEAD**-0.5 for m in range(2)]
    k = [unit(heads[2 + m]) for m in range(2)]
    q_t = [jnp.transpose(v) for v in q]
    k_t = [jnp.transpose(v) for v in k]
    kq = [jnp.sum(k[m] * q[m], axis=-1, keepdims=True) for m in range(2)]
    ext = ext * rowscale
    for h in range(4):
        m = h // 2
        val = silu(heads[4 + h])
        gate = silu(heads[8 + h])
        beta = 1.0 / (1.0 + jnp.exp(-ext[:, h : h + 1]))
        pre = ext[:, 4 + h : 5 + h] + bias[:, h : h + 1]
        soft = jnp.maximum(pre, 0.0) + jnp.log1p(jnp.exp(-jnp.abs(pre)))
        decay = jnp.exp(-jnp.exp(rate[:, h : h + 1]) * soft)
        by_k, by_q = [], []
        for i in range(8):
            s = s_buf[i, h]
            by_k.append(jnp.sum(s * k_t[m][:, i : i + 1], axis=0, keepdims=True))
            by_q.append(jnp.sum(s * q_t[m][:, i : i + 1], axis=0, keepdims=True))
        by_k = jnp.concatenate(by_k, axis=0)
        by_q = jnp.concatenate(by_q, axis=0)
        corr = beta * (val - decay * by_k)
        reading = decay * by_q + kq[m] * corr
        norm = lax.rsqrt(jnp.mean(reading * reading, axis=-1, keepdims=True) + EPS)
        nb[z, :, 128 * h : 128 * (h + 1)] = (reading * norm * hgain[...] * gate).astype(BF)
        c_out[:, h] = corr
        d_out[:, h : h + 1] = decay
    for m in range(2):
        k_out[:, m] = k[m]
    share(nb, z, NRM, z_peers)
    y_pass(wo, WO)
    y_pass(gu2, GU2)
    y_start(d2, D2)
    y_done(wo, WO)
    arrived(nb.at[pl.ds(0, NZ - 1)], NRM)
    normed = nb[...].astype(F32).reshape(64, 512).astype(BF)
    pr2_src[...] = dot(normed, wo[...].reshape(ROWS, 512), 1, 1).reshape(NT, 8, ROWS).astype(BF)
    deal(pr2_src, pr2_rcv, t, PR2, t_peers)
    arrived(pr2_rcv.at[pl.ds(0, NT - 1)], PR2)
    own2 = (own1.astype(F32) + jnp.sum(pr2_rcv[...].astype(F32), axis=0)).astype(BF)

    gathered(1, own2, X3)
    y_done(gu2, GU2)
    x3, scaled, coarse, fine = scaled_of(1, X3)
    gate = dot(scaled, gu2[:, 0].reshape(ROWS, FFT), 1, 0)
    up = dot(scaled, gu2[:, 1].reshape(ROWS, FFT), 1, 0)
    fill = jnp.where(iota((64, 64), 1) == 0, coarse, jnp.where(iota((64, 64), 1) == 1, fine, 0.0))
    rs2_src[:, :, 0:FFP] = jnp.concatenate([gate, fill], axis=1).reshape(NZ, 8, FFP).astype(BF)
    rs2_src[:, :, FFP:] = jnp.concatenate([up, jnp.zeros((64, 64), F32)], axis=1).reshape(NZ, 8, FFP).astype(BF)
    deal(rs2_src, rs2_rcv, z, RS2, z_peers)
    y_pass(d2, D2)
    x3_t = jnp.transpose(jnp.concatenate([jnp.zeros((64, ROWS), F32), x3], axis=0))
    arrived(rs2_rcv.at[pl.ds(0, NZ - 1)], RS2)
    both = jnp.sum(rs2_rcv[...].astype(F32), axis=0)
    gate, up = both[:, 0:FFP], both[:, FFP:]
    scale = lax.rsqrt((gate[:, FFT : FFT + 1] + gate[:, FFT + 1 : FFT + 2]) / D + EPS)
    hidden = silu(gate * scale) * (up * scale)
    hg2[z] = jnp.where(iota((8, FFP), 1) < FFT, hidden, 0.0).astype(BF)
    share(hg2, z, AG2, z_peers)
    y_done(d2, D2)
    arrived(hg2.at[pl.ds(0, NZ - 1)], AG2)
    h = hg2[...].astype(F32).reshape(64, FFP).astype(BF)[:, 0:FFT]
    h = jnp.concatenate([h, jnp.zeros((64, FFT), BF)], axis=0)
    part = dot(d2[...].reshape(ROWS, FFT), h, 1, 1) + x3_t
    pr3_src[...] = part.reshape(PLANE, 8, 128).astype(BF)
    deal(pr3_src, pr3_rcv, me, PR3, plane_peers)
    arrived(pr3_rcv.at[pl.ds(0, PLANE - 1)], PR3)
    final = jnp.zeros((8, ROWS), F32)
    l, b = iota((128, ROWS), 0), iota((128, ROWS), 1)
    for p in range(NY):
        total = jnp.sum(pr3_rcv[NT * p : NT * (p + 1)].astype(F32), axis=0)
        base = pltpu.roll(pr3_rcv[NT * p].astype(F32), 64, 1)
        place = one_hot((b == l + 24 * lax.shift_right_logical(l, 3) + 8 * p) & (l < 64))
        final = final + dot((base + 0.5 * total).astype(BF), place, 1, 0)
    out[...] = final.astype(BF)

    left(xg.at[pl.ds(0, PLANE - 1)], X1)
    left(pr1_src.at[pl.ds(0, PLANE - 1)], PR1)
    left(pr3_src.at[pl.ds(0, PLANE - 1)], PR3)
    left(rs_src.at[pl.ds(0, NZ - 1)], RS1)
    left(hg.at[pl.ds(0, NZ - 1)], AG1)
    left(xb.at[0, pl.ds(0, NT - 1)], X2)
    left(xb.at[1, pl.ds(0, NT - 1)], X3)
    left(pr2_src.at[pl.ds(0, NT - 1)], PR2)
    left(m_src.at[pl.ds(0, NZ - 1)], MIX)
    left(nb.at[pl.ds(0, NZ - 1)], NRM)
    left(rs2_src.at[pl.ds(0, NZ - 1)], RS2)
    left(hg2.at[pl.ds(0, NZ - 1)], AG2)
    left(gu_src.at[pl.ds(0, NY - 1)], GU1)
    left(dd_src.at[pl.ds(0, NY - 1)], DD)
    left(gn.at[pl.ds(0, NY - 1)], GN)
    y_left(mw, MW)
    y_left(wo, WO)
    y_left(gu2, GU2)
    y_left(d2, D2)


def layer(res, state, gain1, gate1, up1, down1, gain2, wq, wk, wv, wg, wbeta, wdecay, rate, bias, hgain, wo, gain3, gate2, up2, down2):
    vmem = pl.BlockSpec(memory_space=pltpu.VMEM)
    args = (
        res.T, state, gain1[None], gain2[None], gain3[None], gate1, up1, down1.T, gate2, up2, down2.T,
        wq, wk, wv, wg, wbeta.T, wdecay.T, rate[None], bias[None], hgain[None], wo.T,
    )
    held = [args[i] for i in (0, 1, 2, 3, 4, 5, 6, 7, 15, 16, 17, 18, 19)]
    out, k, corr, decay = pl.pallas_call(
        kernel,
        out_shape=(
            jax.ShapeDtypeStruct((8, ROWS), BF),
            jax.ShapeDtypeStruct((8, 2, HEAD), F32),
            jax.ShapeDtypeStruct((8, 4, HEAD), F32),
            jax.ShapeDtypeStruct((8, 4), F32),
        ),
        in_specs=[pl.BlockSpec(memory_space=pltpu.HBM)] * len(args),
        out_specs=(vmem,) * 4,
        scratch_shapes=[pltpu.VMEM(a.shape, a.dtype) for a in held]
        + [
            pltpu.SemaphoreType.DMA((len(args),)),
            pltpu.SemaphoreType.DMA((N_SEM,)),
            pltpu.SemaphoreType.DMA((N_SEM,)),
            pltpu.VMEM((NY, HID, 128), BF),
            pltpu.VMEM((NY, HID, 128), BF),
            pltpu.VMEM((NY, HID, 128), BF),
            pltpu.VMEM((NY, HID, 128), BF),
            pltpu.VMEM((NY, 24, 64), F32),
            pltpu.VMEM((NY, 64, MCOLS), BF),
            pltpu.VMEM((NY, 64, 512), BF),
            pltpu.VMEM((NY, 2, 64, FFT), BF),
            pltpu.VMEM((NY, 64, FFT), BF),
            pltpu.VMEM((2 * PAD, ROWS), BF),
            pltpu.VMEM((PAD, ROWS), BF),
            pltpu.VMEM((ROWS, ROWS), F32),
            pltpu.VMEM((2, 8, ROWS), F32),
            pltpu.VMEM((KV, 8, ROWS), BF),
            pltpu.VMEM((PLANE, 8, ROWS), BF),
            pltpu.VMEM((NZ, 2 * GROUP // 8, 8, ROWS), BF),
            pltpu.VMEM((NZ, 2 * GROUP // 8, 8, ROWS), BF),
            pltpu.VMEM((NZ, GROUP // 8, 8, ROWS), BF),
            pltpu.VMEM((PLANE, 8, ROWS), BF),
            pltpu.VMEM((PLANE, 8, ROWS), BF),
            pltpu.VMEM((2, NT, 8, ROWS), BF),
            pltpu.VMEM((NZ, 8, MCOLS), BF),
            pltpu.VMEM((NZ, 8, MCOLS), BF),
            pltpu.VMEM((NZ, 8, 512), BF),
            pltpu.VMEM((NT, 8, ROWS), BF),
            pltpu.VMEM((NT, 8, ROWS), BF),
            pltpu.VMEM((NZ, 8, 2 * FFP), BF),
            pltpu.VMEM((NZ, 8, 2 * FFP), BF),
            pltpu.VMEM((NZ, 8, FFP), BF),
            pltpu.VMEM((PLANE, 8, 128), BF),
            pltpu.VMEM((PLANE, 8, 128), BF),
        ],
        compiler_params=pltpu.CompilerParams(collective_id=0, has_side_effects=True, vmem_limit_bytes=67_043_328),
    )(*args)
    keys = jnp.repeat(k, 2, axis=1)
    return out.T, state * decay[:, :, None, None] + keys[:, :, :, None] * corr[:, :, None, :]


def solution(mesh):
    placed = (
        P(None, ("kv", "tp")),
        P("kv", "tp", None, None),
        P("kv"),
        P("kv", "tp"),
        P("kv", "tp"),
        P("tp", "kv"),
        P("kv"),
        P("kv", "tp"),
        P("kv", "tp"),
        P("kv", "tp"),
        P("kv", "tp"),
        P("kv", None),
        P("kv", None),
        P("tp"),
        P("tp"),
        P(),
        P("tp", "kv"),
        P("kv"),
        P("kv", "tp"),
        P("kv", "tp"),
        P("tp", "kv"),
    )
    return jax.shard_map(
        layer,
        mesh=mesh,
        in_specs=placed,
        out_specs=(P(None, ("kv", "tp")), P("kv", "tp", None, None)),
        check_vma=False,
    )
```

```python
import jax
import jax.numpy as jnp
from jax import lax
from jax.experimental import pallas as pl
from jax.experimental.pallas import tpu as pltpu
from jax.sharding import PartitionSpec as P

MESH = pl.DeviceIdType.MESH
BF, F32 = jnp.bfloat16, jnp.float32
D, EPS = 2048, 1e-6
NZ, NY, NT = 8, 4, 8
PLANE = NY * NT
KV = NZ * NY
ROWS = 256
KEEP, GROUP = 22, 24
HID = NZ * KEEP
PAD = NZ * GROUP
HEAD = 128

X1, X2, X3, RS1, RS2, AG1, AG2, PR1, PR2, PR3, MIX, NRM, GU1, DD, GN = range(15)
MW, WO, GU2, D2 = 15, 19, 23, 27
N_SEM = 31
MCOLS = 1664
FFT, FFP = 704, 768
RING_Z = (4, 3, 5, 2, 6, 1, 7)
FAR = (0, 1, 2, 1)


def dot(a, b, ca, cb):
    return lax.dot_general(a, b, (((ca,), (cb,)), ((), ())), preferred_element_type=F32)


def iota(shape, dim):
    return lax.broadcasted_iota(jnp.int32, shape, dim)


def one_hot(cond):
    return jnp.where(cond, 1.0, 0.0).astype(BF)


def silu(v):
    return v / (1.0 + jnp.exp(-v))


def kernel(
    res_h, state, gain1_h, gain2_h, gain3_h, gate1_h, up1_h, down1_h, gate2_h, up2_h, down2_h,
    wq_h, wk_h, wv_h, wg_h, wbeta_h, wdecay_h, rate_h, bias_h, hgain_h, wo_h,
    out, state_out,
    res, s_buf, gain1, gain2, gain3, gate1, up1, down1, wbeta, wdecay, rate, bias, hgain,
    in_sem, out_sem, send, recv,
    gu_src, gu_rcv, dd_src, dd_rcv, gn, mw, wo, gu2, d2,
    a_w, d_w, g_col, g_row, xrow,
    xg, rs_src, rs_rcv, hg, pr1_src, pr1_rcv,
    xb, m_src, m_rcv, nb, pa_src, pa_rcv, pb, rs2_src, rs2_rcv, hg2, pr3_src, pr3_rcv,
):
    kv = lax.axis_index("kv")
    t = lax.axis_index("tp")
    z, y = lax.div(kv, NY), lax.rem(kv, NY)
    x, core = lax.div(t, 2), lax.rem(t, 2)
    me = y * NT + t
    zs = [lax.rem(z + o, NZ) for o in range(NZ)]
    ys = [lax.rem(y + o, NY) for o in range(NY)]
    ts = [[lax.rem(x + o, 4) * 2 + c for c in (core, 1 - core)] for o in range(4)]

    z_peers = [(zs[o], (zs[o] * NY + y, t)) for o in RING_Z]
    y_peers = [(ys[o], (z * NY + ys[o], t)) for o in (2, 1, 3)]
    t_peers = [(ts[dx][dc], (kv, ts[dx][dc])) for dx in (2, 1, 3, 0) for dc in (0, 1) if dx or dc]
    plane = [(dy, dx, dc) for dy in range(4) for dx in range(4) for dc in range(2) if dy or dx or dc]
    plane.sort(key=lambda o: -(FAR[o[0]] + FAR[o[1]]))
    plane_peers = [(ys[dy] * NT + ts[dx][dc], (z * NY + ys[dy], ts[dx][dc])) for dy, dx, dc in plane]

    barrier = pltpu.get_barrier_semaphore()
    greet = z_peers[:3] + plane_peers[:10] + z_peers[3:5] + plane_peers[10:] + z_peers[5:]
    for _, peer in greet:
        pl.semaphore_signal(barrier, inc=1, device_id=peer, device_id_type=MESH)

    named = {}
    for i, (src, dst) in enumerate((
        (gate1_h, gate1), (up1_h, up1), (res_h, res), (gain1_h, gain1), (gain2_h, gain2), (gain3_h, gain3), (down1_h, down1),
        (wbeta_h, wbeta), (wdecay_h, wdecay),
        (wq_h, mw.at[y, :, 0:256]), (wk_h, mw.at[y, :, 256:512]), (wv_h, mw.at[y, :, 512:1024]), (wg_h, mw.at[y, :, 1024:1536]),
        (wo_h, wo.at[y]), (gate2_h, gu2.at[y, 0]), (up2_h, gu2.at[y, 1]), (down2_h, d2.at[y]),
        (rate_h, rate), (bias_h, bias), (hgain_h, hgain), (state, s_buf),
    )):
        named[id(src)] = pltpu.make_async_copy(src, dst, in_sem.at[i])
        named[id(src)].start()

    def ready(*refs):
        for ref in refs:
            named[id(ref)].wait()

    def put(src, dst, k, peer):
        pltpu.make_async_remote_copy(
            src_ref=src, dst_ref=dst, send_sem=send.at[k], recv_sem=recv.at[k], device_id=peer, device_id_type=MESH
        ).start()

    def arrived(part, k):
        pltpu.make_async_copy(part, part, recv.at[k]).wait()

    def left(part, k):
        pltpu.make_async_copy(part, part, send.at[k]).wait()

    def share(buf, own, k, peers):
        for _, peer in peers:
            put(buf.at[own], buf.at[own], k, peer)

    def deal(src, dst, own, k, peers):
        for p, peer in peers:
            put(src.at[p], dst.at[own], k, peer)
        dst[own] = src[own]

    above, below = (z * NY + ys[1], t), (z * NY + ys[3], t)

    def y_start(buf, k):
        put(buf.at[y], buf.at[y], k, above)
        put(buf.at[y], buf.at[y], k + 1, below)

    def halves(buf, p):
        n = buf.shape[1] // 2
        return buf.at[p, pl.ds(0, n)], buf.at[p, pl.ds(n, n)]

    def y_pass(buf, k):
        arrived(buf.at[ys[3]], k)
        first, second = halves(buf, ys[3])
        put(first, first, k + 2, above)
        arrived(buf.at[ys[1]], k + 1)
        first, second = halves(buf, ys[1])
        put(second, second, k + 3, below)

    def y_done(buf, k):
        first, second = halves(buf, ys[2])
        arrived(first, k + 2)
        arrived(second, k + 3)

    def y_left(buf, k):
        first, second = halves(buf, 0)
        left(buf.at[0], k)
        left(buf.at[0], k + 1)
        left(first, k + 2)
        left(second, k + 3)

    low = one_hot(iota((64, 128), 0) == iota((64, 128), 1))
    high = one_hot(iota((64, 128), 0) + 64 == iota((64, 128), 1))
    eye64 = iota((64, 64), 0) == iota((64, 64), 1)

    ready(gate1_h, up1_h)
    both = dot(gate1[...], low, 0, 0) + dot(up1[...], high, 0, 0)
    gu_src[...] = both.astype(BF).reshape(NY, HID, 128)
    ready(res_h, gain1_h, gain2_h, gain3_h)
    xg[me] = res[...]
    gn[y, 0:8] = jnp.broadcast_to(gain1[...], (8, 64))
    gn[y, 8:16] = jnp.broadcast_to(gain2[...], (8, 64))
    gn[y, 16:24] = jnp.broadcast_to(gain3[...], (8, 64))

    pl.semaphore_wait(barrier, len(greet))

    share(gn, y, GN, y_peers)
    deal(gu_src, gu_rcv, y, GU1, y_peers)
    share(xg, me, X1, plane_peers)

    ready(down1_h)
    dd_src[...] = dot(down1[...], low, 0, 0).astype(BF).reshape(NY, HID, 128)
    sel_b = one_hot((iota((32, 128), 0) == iota((32, 128), 1) + 4 * t) & (iota((32, 128), 1) < 4))
    sel_d = one_hot((iota((32, 128), 0) == iota((32, 128), 1) - 4 + 4 * t) & (iota((32, 128), 1) >= 4) & (iota((32, 128), 1) < 8))
    ready(wbeta_h, wdecay_h)
    mw[y, :, 1536:MCOLS] = (dot(wbeta[...], sel_b, 0, 0) + dot(wdecay[...], sel_d, 0, 0)).astype(BF)

    r, c = iota((PAD, HID), 0), iota((PAD, HID), 1)
    group = jnp.zeros_like(r)
    for i in range(1, NZ):
        group = group + jnp.where(r >= GROUP * i, 1, 0)
    pick = one_hot((c == r - (GROUP - KEEP) * group) & (r - GROUP * group < KEEP))
    lane = iota((PAD, 128), 1)

    def column(p, i):
        row = gn[p, 8 * i : 8 * i + 1]
        return jnp.sum(jnp.where(eye64, jnp.broadcast_to(row, (64, 64)), 0.0), axis=1, keepdims=True)

    arrived(gn.at[pl.ds(0, NY - 1)], GN)
    for p in range(NY):
        g_col[64 * p : 64 * (p + 1)] = jnp.broadcast_to(column(p, 0), (64, ROWS))
    arrived(gu_rcv.at[pl.ds(0, NY - 1)], GU1)
    parts = [dot(pick, gu_rcv[p], 1, 0) for p in range(NY)]
    for h in range(2):
        a, b = parts[2 * h], parts[2 * h + 1]
        a_w[0:PAD, 128 * h : 128 * (h + 1)] = jnp.where(lane < 64, a, pltpu.roll(b, 64, 1)).astype(BF)
        a_w[PAD : 2 * PAD, 128 * h : 128 * (h + 1)] = jnp.where(lane < 64, pltpu.roll(a, 64, 1), b).astype(BF)

    arrived(xg.at[pl.ds(0, PLANE - 1)], X1)
    x0 = xg[...].astype(F32).reshape(ROWS, ROWS)
    part = dot(a_w[...], (x0 * g_col[...]).astype(BF), 1, 0)
    total = jnp.sum(x0 * x0, axis=0, keepdims=True)
    coarse = total.astype(BF).astype(F32)
    row = iota((NZ, GROUP, ROWS), 1)
    gate = part[0:PAD].reshape(NZ, GROUP, ROWS)
    up = part[PAD : 2 * PAD].reshape(NZ, GROUP, ROWS)
    gate = jnp.where(row == KEEP, coarse.reshape(1, 1, ROWS), gate)
    gate = jnp.where(row == KEEP + 1, (total - coarse).reshape(1, 1, ROWS), gate)
    rs_src[...] = jnp.concatenate([gate, up], axis=1).astype(BF).reshape(NZ, 2 * GROUP // 8, 8, ROWS)
    deal(rs_src, rs_rcv, z, RS1, z_peers)

    for p, peer in y_peers:
        put(dd_src.at[p], dd_rcv.at[y], DD, peer)
    dd_rcv[y] = dd_src[y]
    ready(wq_h, wk_h, wv_h, wg_h)
    y_start(mw, MW)
    xrow[...] = jnp.transpose(x0).reshape(KV, 8, ROWS).astype(BF)
    lane64 = iota((64, 128), 1)
    for i in range(2):
        for h in range(2):
            spread = jnp.where(lane64 == iota((64, 128), 0), column(2 * h, i + 1), 0.0)
            spread = spread + jnp.where(lane64 == iota((64, 128), 0) + 64, column(2 * h + 1, i + 1), 0.0)
            g_row[i, :, 128 * h : 128 * (h + 1)] = jnp.broadcast_to(jnp.sum(spread, axis=0, keepdims=True), (8, 128))

    arrived(rs_rcv.at[pl.ds(0, NZ - 1)], RS1)
    both = jnp.sum(rs_rcv[...].astype(F32), axis=0).reshape(2 * GROUP, ROWS)
    gate, up = both[0:GROUP], both[GROUP:]
    scale = lax.rsqrt((gate[KEEP : KEEP + 1] + gate[KEEP + 1 : KEEP + 2]) / D + EPS)
    hidden = silu(gate * scale) * (up * scale)
    hidden = jnp.where(iota((GROUP, ROWS), 0) < KEEP, hidden, 0.0)
    hg[z] = hidden.reshape(GROUP // 8, 8, ROWS).astype(BF)
    share(hg, z, AG1, z_peers)

    arrived(dd_rcv.at[pl.ds(0, NY - 1)], DD)
    for h in range(2):
        a, b = dot(pick, dd_rcv[2 * h], 1, 0), dot(pick, dd_rcv[2 * h + 1], 1, 0)
        d_w[:, 128 * h : 128 * (h + 1)] = (a + pltpu.roll(b, 64, 1)).astype(BF)
    y_pass(mw, MW)
    arrived(hg.at[pl.ds(0, NZ - 1)], AG1)
    h = hg[...].astype(F32).reshape(PAD, ROWS).astype(BF)
    pr1_src[...] = dot(h, d_w[...], 0, 0).reshape(KV, 8, ROWS).astype(BF)
    for (dy, dx, dc), (_, peer) in zip(plane, plane_peers):
        put(pr1_src.at[ts[dx][dc] * NY + ys[dy]], pr1_rcv.at[me], PR1, peer)
    pr1_rcv[me] = pr1_src[t * NY + y]
    arrived(pr1_rcv.at[pl.ds(0, PLANE - 1)], PR1)
    branch = jnp.sum(pr1_rcv[...].astype(F32), axis=0)
    own1 = (xrow[t * NY + y].astype(F32) + 0.5 * branch).astype(BF)

    def scaled_of(v, i):
        squares = jnp.sum(v * v, axis=1, keepdims=True)
        coarse = squares.astype(BF).astype(F32)
        return (v * g_row[i, 0:1]).astype(BF), coarse, squares - coarse

    xb[t] = own1
    share(xb, t, X2, t_peers)
    y_done(mw, MW)
    arrived(xb.at[pl.ds(0, NT - 1)], X2)
    x1 = xb[...].astype(F32).reshape(64, ROWS)
    scaled, coarse, fine = scaled_of(x1, 0)
    last = iota((64, 128), 1)
    for a, b in ((0, 512), (512, 1024), (1024, 1536), (1536, MCOLS)):
        part = dot(scaled, mw[:, :, a:b].reshape(ROWS, b - a), 1, 0)
        if a == 1536:
            part = part + jnp.where(last == 8, coarse, 0.0) + jnp.where(last == 9, fine, 0.0)
        m_src[:, :, a:b] = part.reshape(NZ, 8, b - a).astype(BF)
    deal(m_src, m_rcv, z, MIX, z_peers)
    ready(wo_h, gate2_h, up2_h, down2_h, state, rate_h, bias_h, hgain_h)
    y_start(wo, WO)
    y_start(gu2, GU2)
    arrived(m_rcv.at[pl.ds(0, NZ - 1)], MIX)

    mixed = jnp.sum(m_rcv[...].astype(F32), axis=0)
    ext = mixed[:, 1536:MCOLS]
    rowscale = lax.rsqrt((ext[:, 8:9] + ext[:, 9:10]) / D + EPS)
    heads = [mixed[:, 128 * i : 128 * (i + 1)] * rowscale for i in range(12)]

    def unit(v):
        a = silu(v)
        return a * lax.rsqrt(jnp.sum(a * a, axis=-1, keepdims=True) + EPS)

    q = [unit(heads[m]) * HEAD**-0.5 for m in range(2)]
    k = [unit(heads[2 + m]) for m in range(2)]
    q_t = [jnp.transpose(v) for v in q]
    k_t = [jnp.transpose(v) for v in k]
    kq = [jnp.sum(k[m] * q[m], axis=-1, keepdims=True) for m in range(2)]
    ext = ext * rowscale
    by_k, by_q = [[] for _ in range(4)], [[] for _ in range(4)]
    for m in range(2):
        for i in range(8):
            k_col = jnp.broadcast_to(k_t[m][:, i : i + 1], (HEAD, HEAD))
            q_col = jnp.broadcast_to(q_t[m][:, i : i + 1], (HEAD, HEAD))
            for h in (2 * m, 2 * m + 1):
                s = s_buf[i, h]
                by_k[h].append(jnp.sum(s * k_col, axis=0, keepdims=True))
                by_q[h].append(jnp.sum(s * q_col, axis=0, keepdims=True))
    new = []
    for h in range(4):
        m = h // 2
        val = silu(heads[4 + h])
        gate = silu(heads[8 + h])
        beta = 1.0 / (1.0 + jnp.exp(-ext[:, h : h + 1]))
        pre = ext[:, 4 + h : 5 + h] + bias[:, h : h + 1]
        soft = jnp.maximum(pre, 0.0) + jnp.log1p(jnp.exp(-jnp.abs(pre)))
        decay = jnp.exp(-jnp.exp(rate[:, h : h + 1]) * soft)
        corr = beta * (val - decay * jnp.concatenate(by_k[h], axis=0))
        reading = decay * jnp.concatenate(by_q[h], axis=0) + kq[m] * corr
        norm = lax.rsqrt(jnp.mean(reading * reading, axis=-1, keepdims=True) + EPS)
        nb[z, :, 128 * h : 128 * (h + 1)] = (reading * norm * hgain[...] * gate).astype(BF)
        new.append((decay, corr))
    share(nb, z, NRM, z_peers)
    y_pass(wo, WO)
    y_pass(gu2, GU2)
    y_start(d2, D2)
    for i in range(8):
        for m in range(2):
            k_col = jnp.broadcast_to(k_t[m][:, i : i + 1], (HEAD, HEAD))
            for h in (2 * m, 2 * m + 1):
                decay, corr = new[h]
                s_buf[i, h] = s_buf[i, h] * decay[i : i + 1] + k_col * corr[i : i + 1]
    store = pltpu.make_async_copy(s_buf, state_out, out_sem)
    store.start()
    y_done(wo, WO)
    arrived(nb.at[pl.ds(0, NZ - 1)], NRM)
    normed = nb[...].astype(F32).reshape(64, 512).astype(BF)
    part = dot(normed, wo[...].reshape(ROWS, 512), 1, 1)
    pa_src[...] = part.reshape(2, 4, 8, ROWS).astype(BF)
    put(pa_src.at[1 - core], pa_rcv, PR2, (kv, ts[0][1]))
    mine = jnp.where(core == 0, part[0:32], part[32:64])
    arrived(pa_rcv, PR2)
    pb[t] = (mine.reshape(4, 8, ROWS) + pa_rcv[...].astype(F32)).astype(BF)
    share(pb, t, X3, t_peers)
    y_done(gu2, GU2)
    arrived(pb.at[pl.ds(0, NT - 1)], X3)
    branch = []
    for c in range(2):
        half = pb[c].astype(F32)
        for i in range(1, 4):
            half = half + pb[2 * i + c].astype(F32)
        branch.append(half.reshape(32, ROWS))

    x3 = (x1 + jnp.concatenate(branch, axis=0)).astype(BF).astype(F32)
    scaled, coarse, fine = scaled_of(x3, 1)
    gate = dot(scaled, gu2[:, 0].reshape(ROWS, FFT), 1, 0)
    up = dot(scaled, gu2[:, 1].reshape(ROWS, FFT), 1, 0)
    fill = jnp.where(iota((64, 64), 1) == 0, coarse, jnp.where(iota((64, 64), 1) == 1, fine, 0.0))
    rs2_src[:, :, 0:FFP] = jnp.concatenate([gate, fill], axis=1).reshape(NZ, 8, FFP).astype(BF)
    rs2_src[:, :, FFP:] = jnp.concatenate([up, jnp.zeros((64, 64), F32)], axis=1).reshape(NZ, 8, FFP).astype(BF)
    deal(rs2_src, rs2_rcv, z, RS2, z_peers)
    y_pass(d2, D2)
    x3_t = jnp.transpose(jnp.concatenate([jnp.zeros((64, ROWS), F32), x3], axis=0))
    arrived(rs2_rcv.at[pl.ds(0, NZ - 1)], RS2)
    both = jnp.sum(rs2_rcv[...].astype(F32), axis=0)
    gate, up = both[:, 0:FFP], both[:, FFP:]
    scale = lax.rsqrt((gate[:, FFT : FFT + 1] + gate[:, FFT + 1 : FFT + 2]) / D + EPS)
    hidden = silu(gate * scale) * (up * scale)
    hg2[z] = jnp.where(iota((8, FFP), 1) < FFT, hidden, 0.0).astype(BF)
    share(hg2, z, AG2, z_peers)
    y_done(d2, D2)
    arrived(hg2.at[pl.ds(0, NZ - 1)], AG2)
    h = hg2[...].astype(F32).reshape(64, FFP).astype(BF)[:, 0:FFT]
    h = jnp.concatenate([h, jnp.zeros((64, FFT), BF)], axis=0)
    part = dot(d2[...].reshape(ROWS, FFT), h, 1, 1) + x3_t
    pr3_src[...] = part.reshape(PLANE, 8, 128).astype(BF)
    deal(pr3_src, pr3_rcv, me, PR3, plane_peers)
    arrived(pr3_rcv.at[pl.ds(0, PLANE - 1)], PR3)
    final = jnp.zeros((8, ROWS), F32)
    l, b = iota((128, ROWS), 0), iota((128, ROWS), 1)
    for p in range(NY):
        total = jnp.sum(pr3_rcv[NT * p : NT * (p + 1)].astype(F32), axis=0)
        base = pltpu.roll(pr3_rcv[NT * p].astype(F32), 64, 1)
        place = one_hot((b == l + 24 * lax.shift_right_logical(l, 3) + 8 * p) & (l < 64))
        final = final + dot((base + 0.5 * total).astype(BF), place, 1, 0)
    out[...] = final.astype(BF)
    store.wait()

    left(xg.at[pl.ds(0, PLANE - 1)], X1)
    left(pr1_src.at[pl.ds(0, PLANE - 1)], PR1)
    left(pr3_src.at[pl.ds(0, PLANE - 1)], PR3)
    left(rs_src.at[pl.ds(0, NZ - 1)], RS1)
    left(hg.at[pl.ds(0, NZ - 1)], AG1)
    left(xb.at[pl.ds(0, NT - 1)], X2)
    left(pb.at[pl.ds(0, NT - 1)], X3)
    left(pa_rcv, PR2)
    left(m_src.at[pl.ds(0, NZ - 1)], MIX)
    left(nb.at[pl.ds(0, NZ - 1)], NRM)
    left(rs2_src.at[pl.ds(0, NZ - 1)], RS2)
    left(hg2.at[pl.ds(0, NZ - 1)], AG2)
    left(gu_src.at[pl.ds(0, NY - 1)], GU1)
    left(dd_src.at[pl.ds(0, NY - 1)], DD)
    left(gn.at[pl.ds(0, NY - 1)], GN)
    y_left(mw, MW)
    y_left(wo, WO)
    y_left(gu2, GU2)
    y_left(d2, D2)


def deliver(out_in, state_in, out, state_out, held, s_held, arrive, leave):
    pairs = [(out_in, held, out)] + [(state_in.at[i], s_held.at[i], state_out.at[i]) for i in range(8)]
    for i, (src, mid, _) in enumerate(pairs):
        pltpu.make_async_copy(src, mid, arrive.at[i]).start()
    for i, (src, mid, dst) in enumerate(pairs):
        pltpu.make_async_copy(src, mid, arrive.at[i]).wait()
        pltpu.make_async_copy(mid, dst, leave.at[i]).start()
    for i, (_, mid, dst) in enumerate(pairs):
        pltpu.make_async_copy(mid, dst, leave.at[i]).wait()


def layer(res, state, gain1, gate1, up1, down1, gain2, wq, wk, wv, wg, wbeta, wdecay, rate, bias, hgain, wo, gain3, gate2, up2, down2):
    vmem = pl.BlockSpec(memory_space=pltpu.VMEM)
    args = (
        res.T, state, gain1[None], gain2[None], gain3[None], gate1, up1, down1.T, gate2, up2, down2.T,
        wq, wk, wv, wg, wbeta.T, wdecay.T, rate[None], bias[None], hgain[None], wo.T,
    )
    held = [args[i] for i in (0, 1, 2, 3, 4, 5, 6, 7, 15, 16, 17, 18, 19)]
    hbm = pl.BlockSpec(memory_space=pltpu.HBM)
    shapes = (jax.ShapeDtypeStruct((8, ROWS), BF), jax.ShapeDtypeStruct(state.shape, F32))
    out, new_state = pl.pallas_call(
        kernel,
        out_shape=shapes,
        in_specs=[hbm] * len(args),
        out_specs=(vmem, hbm),
        scratch_shapes=[pltpu.VMEM(a.shape, a.dtype) for a in held]
        + [
            pltpu.SemaphoreType.DMA((len(args),)),
            pltpu.SemaphoreType.DMA,
            pltpu.SemaphoreType.DMA((N_SEM,)),
            pltpu.SemaphoreType.DMA((N_SEM,)),
            pltpu.VMEM((NY, HID, 128), BF),
            pltpu.VMEM((NY, HID, 128), BF),
            pltpu.VMEM((NY, HID, 128), BF),
            pltpu.VMEM((NY, HID, 128), BF),
            pltpu.VMEM((NY, 24, 64), F32),
            pltpu.VMEM((NY, 64, MCOLS), BF),
            pltpu.VMEM((NY, 64, 512), BF),
            pltpu.VMEM((NY, 2, 64, FFT), BF),
            pltpu.VMEM((NY, 64, FFT), BF),
            pltpu.VMEM((2 * PAD, ROWS), BF),
            pltpu.VMEM((PAD, ROWS), BF),
            pltpu.VMEM((ROWS, ROWS), F32),
            pltpu.VMEM((2, 8, ROWS), F32),
            pltpu.VMEM((KV, 8, ROWS), BF),
            pltpu.VMEM((PLANE, 8, ROWS), BF),
            pltpu.VMEM((NZ, 2 * GROUP // 8, 8, ROWS), BF),
            pltpu.VMEM((NZ, 2 * GROUP // 8, 8, ROWS), BF),
            pltpu.VMEM((NZ, GROUP // 8, 8, ROWS), BF),
            pltpu.VMEM((PLANE, 8, ROWS), BF),
            pltpu.VMEM((PLANE, 8, ROWS), BF),
            pltpu.VMEM((NT, 8, ROWS), BF),
            pltpu.VMEM((NZ, 8, MCOLS), BF),
            pltpu.VMEM((NZ, 8, MCOLS), BF),
            pltpu.VMEM((NZ, 8, 512), BF),
            pltpu.VMEM((2, 4, 8, ROWS), BF),
            pltpu.VMEM((4, 8, ROWS), BF),
            pltpu.VMEM((NT, 4, 8, ROWS), BF),
            pltpu.VMEM((NZ, 8, 2 * FFP), BF),
            pltpu.VMEM((NZ, 8, 2 * FFP), BF),
            pltpu.VMEM((NZ, 8, FFP), BF),
            pltpu.VMEM((PLANE, 8, 128), BF),
            pltpu.VMEM((PLANE, 8, 128), BF),
        ],
        compiler_params=pltpu.CompilerParams(collective_id=0, has_side_effects=True, vmem_limit_bytes=67_043_328),
    )(*args)
    out, new_state = pl.pallas_call(
        deliver,
        out_shape=shapes,
        in_specs=[hbm, hbm],
        out_specs=(hbm, hbm),
        scratch_shapes=[
            pltpu.VMEM(out.shape, out.dtype),
            pltpu.VMEM(state.shape, F32),
            pltpu.SemaphoreType.DMA((9,)),
            pltpu.SemaphoreType.DMA((9,)),
        ],
        compiler_params=pltpu.CompilerParams(vmem_limit_bytes=67_043_328),
    )(out, new_state)
    return out.T, new_state


def solution(mesh):
    placed = (
        P(None, ("kv", "tp")),
        P("kv", "tp", None, None),
        P("kv"),
        P("kv", "tp"),
        P("kv", "tp"),
        P("tp", "kv"),
        P("kv"),
        P("kv", "tp"),
        P("kv", "tp"),
        P("kv", "tp"),
        P("kv", "tp"),
        P("kv", None),
        P("kv", None),
        P("tp"),
        P("tp"),
        P(),
        P("tp", "kv"),
        P("kv"),
        P("kv", "tp"),
        P("kv", "tp"),
        P("tp", "kv"),
    )
    return jax.shard_map(
        layer,
        mesh=mesh,
        in_specs=placed,
        out_specs=(P(None, ("kv", "tp")), P("kv", "tp", None, None)),
        check_vma=False,
    )
```

```python
import jax
import jax.numpy as jnp
from jax import lax
from jax.experimental import pallas as pl
from jax.experimental.pallas import tpu as pltpu
from jax.sharding import PartitionSpec as P

MESH = pl.DeviceIdType.MESH
BF, F32 = jnp.bfloat16, jnp.float32
D, EPS = 2048, 1e-6
NZ, NY, NT = 8, 4, 8
PLANE = NY * NT
KV = NZ * NY
ROWS = 256
KEEP, GROUP = 22, 24
HID = NZ * KEEP
PAD = NZ * GROUP
HEAD = 128

X1, X2, X3, RS1, RS2, AG1, AG2, PR1, PR2, PR3, MIX, NRM, GU1, DD, GN = range(15)
MW, WO, GU2, D2 = 15, 19, 23, 27
N_SEM = 31
MCOLS = 1664
FFT, FFP = 704, 768
RING_Z = (4, 3, 5, 2, 6, 1, 7)
FAR = (0, 1, 2, 1)


def dot(a, b, ca, cb):
    return lax.dot_general(a, b, (((ca,), (cb,)), ((), ())), preferred_element_type=F32)


def iota(shape, dim):
    return lax.broadcasted_iota(jnp.int32, shape, dim)


def one_hot(cond):
    return jnp.where(cond, 1.0, 0.0).astype(BF)


def silu(v):
    return v / (1.0 + jnp.exp(-v))


def kernel(
    res_h, state, gain1_h, gain2_h, gain3_h, gate1_h, up1_h, down1_h, gate2_h, up2_h, down2_h,
    wq_h, wk_h, wv_h, wg_h, wbeta_h, wdecay_h, rate_h, bias_h, hgain_h, wo_h,
    out, state_out,
    res, s_buf, gain1, gain2, gain3, gate1, up1, down1, wbeta, wdecay, rate, bias, hgain,
    in_sem, send, recv,
    gu_src, gu_rcv, dd_src, dd_rcv, gn, mw, wo, gu2, d2,
    a_w, d_w, g_col, g_row, xrow,
    xg, rs_src, rs_rcv, hg, pr1_src, pr1_rcv,
    xb, m_src, m_rcv, nb, pa_src, pa_rcv, pb, rs2_src, rs2_rcv, hg2, pr3_src, pr3_rcv, place,
):
    kv = lax.axis_index("kv")
    t = lax.axis_index("tp")
    z, y = lax.div(kv, NY), lax.rem(kv, NY)
    x, core = lax.div(t, 2), lax.rem(t, 2)
    me = y * NT + t
    zs = [lax.rem(z + o, NZ) for o in range(NZ)]
    ys = [lax.rem(y + o, NY) for o in range(NY)]
    ts = [[lax.rem(x + o, 4) * 2 + c for c in (core, 1 - core)] for o in range(4)]

    z_peers = [(zs[o], (zs[o] * NY + y, t)) for o in RING_Z]
    y_peers = [(ys[o], (z * NY + ys[o], t)) for o in (2, 1, 3)]
    t_peers = [(ts[dx][dc], (kv, ts[dx][dc])) for dx in (2, 1, 3, 0) for dc in (0, 1) if dx or dc]
    plane = [(dy, dx, dc) for dy in range(4) for dx in range(4) for dc in range(2) if dy or dx or dc]
    plane.sort(key=lambda o: -(FAR[o[0]] + FAR[o[1]]))
    plane_peers = [(ys[dy] * NT + ts[dx][dc], (z * NY + ys[dy], ts[dx][dc])) for dy, dx, dc in plane]

    inputs = (
        (gate1_h, gate1), (up1_h, up1), (res_h, res), (gain1_h, gain1), (gain2_h, gain2), (gain3_h, gain3), (down1_h, down1),
        (wbeta_h, wbeta), (wdecay_h, wdecay),
        (wq_h, mw.at[y, :, 0:256]), (wk_h, mw.at[y, :, 256:512]), (wv_h, mw.at[y, :, 512:1024]), (wg_h, mw.at[y, :, 1024:1536]),
        (wo_h, wo.at[y]), (gate2_h, gu2.at[y, 0]), (up2_h, gu2.at[y, 1]), (down2_h, d2.at[y]),
        (rate_h, rate), (bias_h, bias), (hgain_h, hgain), (state, s_buf),
    )
    named = {id(src): pltpu.make_async_copy(src, dst, in_sem.at[i]) for i, (src, dst) in enumerate(inputs)}
    early = 6
    for src, _ in inputs[:early]:
        named[id(src)].start()

    barrier = pltpu.get_barrier_semaphore()
    greet = z_peers[:3] + plane_peers[:10] + z_peers[3:5] + plane_peers[10:] + z_peers[5:]
    for _, peer in greet:
        pl.semaphore_signal(barrier, inc=1, device_id=peer, device_id_type=MESH)

    def ready(*refs):
        for ref in refs:
            named[id(ref)].wait()

    def put(src, dst, k, peer):
        pltpu.make_async_remote_copy(
            src_ref=src, dst_ref=dst, send_sem=send.at[k], recv_sem=recv.at[k], device_id=peer, device_id_type=MESH
        ).start()

    def arrived(part, k):
        pltpu.make_async_copy(part, part, recv.at[k]).wait()

    def left(part, k):
        pltpu.make_async_copy(part, part, send.at[k]).wait()

    def share(buf, own, k, peers):
        for _, peer in peers:
            put(buf.at[own], buf.at[own], k, peer)

    def deal(src, dst, own, k, peers):
        for p, peer in peers:
            put(src.at[p], dst.at[own], k, peer)
        dst[own] = src[own]

    above, below = (z * NY + ys[1], t), (z * NY + ys[3], t)

    def y_start(buf, k):
        put(buf.at[y], buf.at[y], k, above)
        put(buf.at[y], buf.at[y], k + 1, below)

    def halves(buf, p):
        n = buf.shape[1] // 2
        return buf.at[p, pl.ds(0, n)], buf.at[p, pl.ds(n, n)]

    def y_pass(buf, k):
        arrived(buf.at[ys[3]], k)
        first, second = halves(buf, ys[3])
        put(first, first, k + 2, above)
        arrived(buf.at[ys[1]], k + 1)
        first, second = halves(buf, ys[1])
        put(second, second, k + 3, below)

    def y_done(buf, k):
        first, second = halves(buf, ys[2])
        arrived(first, k + 2)
        arrived(second, k + 3)

    def y_left(buf, k):
        first, second = halves(buf, 0)
        left(buf.at[0], k)
        left(buf.at[0], k + 1)
        left(first, k + 2)
        left(second, k + 3)

    low = one_hot(iota((64, 128), 0) == iota((64, 128), 1))
    high = one_hot(iota((64, 128), 0) + 64 == iota((64, 128), 1))
    eye64 = iota((64, 64), 0) == iota((64, 64), 1)

    ready(gate1_h, up1_h)
    both = dot(gate1[...], low, 0, 0) + dot(up1[...], high, 0, 0)
    gu_src[...] = both.astype(BF).reshape(NY, HID, 128)
    ready(res_h, gain1_h, gain2_h, gain3_h)
    xg[me] = res[...]
    gn[y, 0:8] = jnp.broadcast_to(gain1[...], (8, 64))
    gn[y, 8:16] = jnp.broadcast_to(gain2[...], (8, 64))
    gn[y, 16:24] = jnp.broadcast_to(gain3[...], (8, 64))

    pl.semaphore_wait(barrier, len(greet))

    share(gn, y, GN, y_peers)
    deal(gu_src, gu_rcv, y, GU1, y_peers)
    share(xg, me, X1, plane_peers)

    for src, _ in inputs[early:]:
        named[id(src)].start()
    ready(down1_h)
    dd_src[...] = dot(down1[...], low, 0, 0).astype(BF).reshape(NY, HID, 128)
    sel_b = one_hot((iota((32, 128), 0) == iota((32, 128), 1) + 4 * t) & (iota((32, 128), 1) < 4))
    sel_d = one_hot((iota((32, 128), 0) == iota((32, 128), 1) - 4 + 4 * t) & (iota((32, 128), 1) >= 4) & (iota((32, 128), 1) < 8))
    ready(wbeta_h, wdecay_h)
    mw[y, :, 1536:MCOLS] = (dot(wbeta[...], sel_b, 0, 0) + dot(wdecay[...], sel_d, 0, 0)).astype(BF)

    r, c = iota((PAD, HID), 0), iota((PAD, HID), 1)
    group = jnp.zeros_like(r)
    for i in range(1, NZ):
        group = group + jnp.where(r >= GROUP * i, 1, 0)
    pick = one_hot((c == r - (GROUP - KEEP) * group) & (r - GROUP * group < KEEP))
    lane = iota((PAD, 128), 1)

    def column(p, i):
        row = gn[p, 8 * i : 8 * i + 1]
        return jnp.sum(jnp.where(eye64, jnp.broadcast_to(row, (64, 64)), 0.0), axis=1, keepdims=True)

    arrived(gn.at[pl.ds(0, NY - 1)], GN)
    for p in range(NY):
        g_col[64 * p : 64 * (p + 1)] = jnp.broadcast_to(column(p, 0), (64, ROWS))
    arrived(gu_rcv.at[pl.ds(0, NY - 1)], GU1)
    parts = [dot(pick, gu_rcv[p], 1, 0) for p in range(NY)]
    for h in range(2):
        a, b = parts[2 * h], parts[2 * h + 1]
        a_w[0:PAD, 128 * h : 128 * (h + 1)] = jnp.where(lane < 64, a, pltpu.roll(b, 64, 1)).astype(BF)
        a_w[PAD : 2 * PAD, 128 * h : 128 * (h + 1)] = jnp.where(lane < 64, pltpu.roll(a, 64, 1), b).astype(BF)

    arrived(xg.at[pl.ds(0, PLANE - 1)], X1)
    x0 = xg[...].astype(F32).reshape(ROWS, ROWS)
    part = dot(a_w[...], (x0 * g_col[...]).astype(BF), 1, 0)
    total = jnp.sum(x0 * x0, axis=0, keepdims=True)
    coarse = total.astype(BF).astype(F32)
    row = iota((NZ, GROUP, ROWS), 1)
    gate = part[0:PAD].reshape(NZ, GROUP, ROWS)
    up = part[PAD : 2 * PAD].reshape(NZ, GROUP, ROWS)
    gate = jnp.where(row == KEEP, coarse.reshape(1, 1, ROWS), gate)
    gate = jnp.where(row == KEEP + 1, (total - coarse).reshape(1, 1, ROWS), gate)
    rs_src[...] = jnp.concatenate([gate, up], axis=1).astype(BF).reshape(NZ, 2 * GROUP // 8, 8, ROWS)
    deal(rs_src, rs_rcv, z, RS1, z_peers)

    for p, peer in y_peers:
        put(dd_src.at[p], dd_rcv.at[y], DD, peer)
    dd_rcv[y] = dd_src[y]
    ready(wq_h, wk_h, wv_h, wg_h)
    y_start(mw, MW)
    xrow[...] = jnp.transpose(x0).reshape(KV, 8, ROWS).astype(BF)
    lane64 = iota((64, 128), 1)
    for i in range(2):
        for h in range(2):
            spread = jnp.where(lane64 == iota((64, 128), 0), column(2 * h, i + 1), 0.0)
            spread = spread + jnp.where(lane64 == iota((64, 128), 0) + 64, column(2 * h + 1, i + 1), 0.0)
            g_row[i, :, 128 * h : 128 * (h + 1)] = jnp.broadcast_to(jnp.sum(spread, axis=0, keepdims=True), (8, 128))

    arrived(rs_rcv.at[pl.ds(0, NZ - 1)], RS1)
    both = jnp.sum(rs_rcv[...].astype(F32), axis=0).reshape(2 * GROUP, ROWS)
    gate, up = both[0:GROUP], both[GROUP:]
    scale = lax.rsqrt((gate[KEEP : KEEP + 1] + gate[KEEP + 1 : KEEP + 2]) / D + EPS)
    hidden = silu(gate * scale) * (up * scale)
    hidden = jnp.where(iota((GROUP, ROWS), 0) < KEEP, hidden, 0.0)
    hg[z] = hidden.reshape(GROUP // 8, 8, ROWS).astype(BF)
    share(hg, z, AG1, z_peers)

    arrived(dd_rcv.at[pl.ds(0, NY - 1)], DD)
    for h in range(2):
        a, b = dot(pick, dd_rcv[2 * h], 1, 0), dot(pick, dd_rcv[2 * h + 1], 1, 0)
        d_w[:, 128 * h : 128 * (h + 1)] = (a + pltpu.roll(b, 64, 1)).astype(BF)
    y_pass(mw, MW)
    arrived(hg.at[pl.ds(0, NZ - 1)], AG1)
    h = hg[...].astype(F32).reshape(PAD, ROWS).astype(BF)
    pr1_src[...] = dot(h, d_w[...], 0, 0).reshape(KV, 8, ROWS).astype(BF)
    for (dy, dx, dc), (_, peer) in zip(plane, plane_peers):
        put(pr1_src.at[ts[dx][dc] * NY + ys[dy]], pr1_rcv.at[me], PR1, peer)
    pr1_rcv[me] = pr1_src[t * NY + y]
    arrived(pr1_rcv.at[pl.ds(0, PLANE - 1)], PR1)
    branch = jnp.sum(pr1_rcv[...].astype(F32), axis=0)
    own1 = (xrow[t * NY + y].astype(F32) + 0.5 * branch).astype(BF)

    def scaled_of(v, i):
        squares = jnp.sum(v * v, axis=1, keepdims=True)
        coarse = squares.astype(BF).astype(F32)
        return (v * g_row[i, 0:1]).astype(BF), coarse, squares - coarse

    xb[t] = own1
    share(xb, t, X2, t_peers)
    y_done(mw, MW)
    arrived(xb.at[pl.ds(0, NT - 1)], X2)
    x1 = xb[...].astype(F32).reshape(64, ROWS)
    scaled, coarse, fine = scaled_of(x1, 0)
    last = iota((64, 128), 1)
    for a, b in ((0, 512), (512, 1024), (1024, 1536), (1536, MCOLS)):
        part = dot(scaled, mw[:, :, a:b].reshape(ROWS, b - a), 1, 0)
        if a == 1536:
            part = part + jnp.where(last == 8, coarse, 0.0) + jnp.where(last == 9, fine, 0.0)
        m_src[:, :, a:b] = part.reshape(NZ, 8, b - a).astype(BF)
    deal(m_src, m_rcv, z, MIX, z_peers)
    ready(wo_h, gate2_h, up2_h, down2_h, state, rate_h, bias_h, hgain_h)
    y_start(wo, WO)
    y_start(gu2, GU2)
    arrived(m_rcv.at[pl.ds(0, NZ - 1)], MIX)

    mixed = jnp.sum(m_rcv[...].astype(F32), axis=0)
    ext = mixed[:, 1536:MCOLS]
    rowscale = lax.rsqrt((ext[:, 8:9] + ext[:, 9:10]) / D + EPS)
    heads = [mixed[:, 128 * i : 128 * (i + 1)] * rowscale for i in range(12)]

    def unit(v):
        a = silu(v)
        return a * lax.rsqrt(jnp.sum(a * a, axis=-1, keepdims=True) + EPS)

    q = [unit(heads[m]) * HEAD**-0.5 for m in range(2)]
    k = [unit(heads[2 + m]) for m in range(2)]
    q_t = [jnp.transpose(v) for v in q]
    k_t = [jnp.transpose(v) for v in k]
    kq = [jnp.sum(k[m] * q[m], axis=-1, keepdims=True) for m in range(2)]
    ext = ext * rowscale
    by_k, by_q = [[] for _ in range(4)], [[] for _ in range(4)]
    for m in range(2):
        for i in range(8):
            k_col = jnp.broadcast_to(k_t[m][:, i : i + 1], (HEAD, HEAD))
            q_col = jnp.broadcast_to(q_t[m][:, i : i + 1], (HEAD, HEAD))
            for h in (2 * m, 2 * m + 1):
                s = s_buf[i, h]
                by_k[h].append(jnp.sum(s * k_col, axis=0, keepdims=True))
                by_q[h].append(jnp.sum(s * q_col, axis=0, keepdims=True))
    new = []
    for h in range(4):
        m = h // 2
        val = silu(heads[4 + h])
        gate = silu(heads[8 + h])
        beta = 1.0 / (1.0 + jnp.exp(-ext[:, h : h + 1]))
        pre = ext[:, 4 + h : 5 + h] + bias[:, h : h + 1]
        soft = jnp.maximum(pre, 0.0) + jnp.log1p(jnp.exp(-jnp.abs(pre)))
        decay = jnp.exp(-jnp.exp(rate[:, h : h + 1]) * soft)
        corr = beta * (val - decay * jnp.concatenate(by_k[h], axis=0))
        reading = decay * jnp.concatenate(by_q[h], axis=0) + kq[m] * corr
        norm = lax.rsqrt(jnp.mean(reading * reading, axis=-1, keepdims=True) + EPS)
        nb[z, :, 128 * h : 128 * (h + 1)] = (reading * norm * hgain[...] * gate).astype(BF)
        new.append((decay, corr))
    share(nb, z, NRM, z_peers)
    y_pass(wo, WO)
    y_pass(gu2, GU2)
    y_start(d2, D2)
    for i in range(8):
        for m in range(2):
            k_col = jnp.broadcast_to(k_t[m][:, i : i + 1], (HEAD, HEAD))
            for h in (2 * m, 2 * m + 1):
                decay, corr = new[h]
                state_out[i, h] = s_buf[i, h] * decay[i : i + 1] + k_col * corr[i : i + 1]
    y_done(wo, WO)
    arrived(nb.at[pl.ds(0, NZ - 1)], NRM)
    normed = nb[...].astype(F32).reshape(64, 512).astype(BF)
    part = dot(normed, wo[...].reshape(ROWS, 512), 1, 1)
    pa_src[...] = part.reshape(2, 4, 8, ROWS).astype(BF)
    put(pa_src.at[1 - core], pa_rcv, PR2, (kv, ts[0][1]))
    mine = jnp.where(core == 0, part[0:32], part[32:64])
    arrived(pa_rcv, PR2)
    pb[t] = (mine.reshape(4, 8, ROWS) + pa_rcv[...].astype(F32)).astype(BF)
    share(pb, t, X3, t_peers)
    y_done(gu2, GU2)
    arrived(pb.at[pl.ds(0, NT - 1)], X3)
    branch = []
    for c in range(2):
        half = pb[c].astype(F32)
        for i in range(1, 4):
            half = half + pb[2 * i + c].astype(F32)
        branch.append(half.reshape(32, ROWS))

    x3 = (x1 + jnp.concatenate(branch, axis=0)).astype(BF).astype(F32)
    scaled, coarse, fine = scaled_of(x3, 1)
    gate = dot(scaled, gu2[:, 0].reshape(ROWS, FFT), 1, 0)
    up = dot(scaled, gu2[:, 1].reshape(ROWS, FFT), 1, 0)
    fill = jnp.where(iota((64, 64), 1) == 0, coarse, jnp.where(iota((64, 64), 1) == 1, fine, 0.0))
    rs2_src[:, :, 0:FFP] = jnp.concatenate([gate, fill], axis=1).reshape(NZ, 8, FFP).astype(BF)
    rs2_src[:, :, FFP:] = jnp.concatenate([up, jnp.zeros((64, 64), F32)], axis=1).reshape(NZ, 8, FFP).astype(BF)
    deal(rs2_src, rs2_rcv, z, RS2, z_peers)
    y_pass(d2, D2)
    x3_t = jnp.transpose(jnp.concatenate([jnp.zeros((64, ROWS), F32), x3], axis=0))
    arrived(rs2_rcv.at[pl.ds(0, NZ - 1)], RS2)
    both = jnp.sum(rs2_rcv[...].astype(F32), axis=0)
    gate, up = both[:, 0:FFP], both[:, FFP:]
    scale = lax.rsqrt((gate[:, FFT : FFT + 1] + gate[:, FFT + 1 : FFT + 2]) / D + EPS)
    hidden = silu(gate * scale) * (up * scale)
    hg2[z] = jnp.where(iota((8, FFP), 1) < FFT, hidden, 0.0).astype(BF)
    share(hg2, z, AG2, z_peers)
    l, b = iota((128, ROWS), 0), iota((128, ROWS), 1)
    for p in range(NY):
        place[128 * p : 128 * (p + 1)] = one_hot((b == l + 24 * lax.shift_right_logical(l, 3) + 8 * p) & (l < 64))
    y_done(d2, D2)
    arrived(hg2.at[pl.ds(0, NZ - 1)], AG2)
    h = hg2[...].astype(F32).reshape(64, FFP).astype(BF)[:, 0:FFT]
    h = jnp.concatenate([h, jnp.zeros((64, FFT), BF)], axis=0)
    part = dot(d2[...].reshape(ROWS, FFT), h, 1, 1) + x3_t
    pr3_src[...] = part.reshape(PLANE, 8, 128).astype(BF)
    deal(pr3_src, pr3_rcv, me, PR3, plane_peers)
    arrived(pr3_rcv.at[pl.ds(0, PLANE - 1)], PR3)
    pieces = []
    for p in range(NY):
        total = jnp.sum(pr3_rcv[NT * p : NT * (p + 1)].astype(F32), axis=0)
        base = pltpu.roll(pr3_rcv[NT * p].astype(F32), 64, 1)
        pieces.append((base + 0.5 * total).astype(BF))
    final = dot(jnp.concatenate(pieces, axis=1), place[...], 1, 0)
    out[...] = final.astype(BF)

    left(xg.at[pl.ds(0, PLANE - 1)], X1)
    left(pr1_src.at[pl.ds(0, PLANE - 1)], PR1)
    left(pr3_src.at[pl.ds(0, PLANE - 1)], PR3)
    left(rs_src.at[pl.ds(0, NZ - 1)], RS1)
    left(hg.at[pl.ds(0, NZ - 1)], AG1)
    left(xb.at[pl.ds(0, NT - 1)], X2)
    left(pb.at[pl.ds(0, NT - 1)], X3)
    left(pa_rcv, PR2)
    left(m_src.at[pl.ds(0, NZ - 1)], MIX)
    left(nb.at[pl.ds(0, NZ - 1)], NRM)
    left(rs2_src.at[pl.ds(0, NZ - 1)], RS2)
    left(hg2.at[pl.ds(0, NZ - 1)], AG2)
    left(gu_src.at[pl.ds(0, NY - 1)], GU1)
    left(dd_src.at[pl.ds(0, NY - 1)], DD)
    left(gn.at[pl.ds(0, NY - 1)], GN)
    y_left(mw, MW)
    y_left(wo, WO)
    y_left(gu2, GU2)
    y_left(d2, D2)


def deliver(out_in, state_in, out, state_out, sems):
    copies = [pltpu.make_async_copy(out_in, out, sems.at[0]), pltpu.make_async_copy(state_in, state_out, sems.at[1])]
    for copy in copies:
        copy.start()
    for copy in copies:
        copy.wait()


def layer(res, state, gain1, gate1, up1, down1, gain2, wq, wk, wv, wg, wbeta, wdecay, rate, bias, hgain, wo, gain3, gate2, up2, down2):
    vmem = pl.BlockSpec(memory_space=pltpu.VMEM)
    args = (
        res.T, state, gain1[None], gain2[None], gain3[None], gate1, up1, down1.T, gate2, up2, down2.T,
        wq, wk, wv, wg, wbeta.T, wdecay.T, rate[None], bias[None], hgain[None], wo.T,
    )
    args = tuple(pltpu.with_memory_space_constraint(a, pltpu.HBM) for a in args)
    held = [args[i] for i in (0, 1, 2, 3, 4, 5, 6, 7, 15, 16, 17, 18, 19)]
    hbm = pl.BlockSpec(memory_space=pltpu.HBM)
    shapes = (jax.ShapeDtypeStruct((8, ROWS), BF), jax.ShapeDtypeStruct(state.shape, F32))
    out, new_state = pl.pallas_call(
        kernel,
        out_shape=(pltpu.VMEM((8, ROWS), BF), pltpu.VMEM(state.shape, F32)),
        in_specs=[hbm] * len(args),
        out_specs=(vmem, vmem),
        scratch_shapes=[pltpu.VMEM(a.shape, a.dtype) for a in held]
        + [
            pltpu.SemaphoreType.DMA((len(args),)),
            pltpu.SemaphoreType.DMA((N_SEM,)),
            pltpu.SemaphoreType.DMA((N_SEM,)),
            pltpu.VMEM((NY, HID, 128), BF),
            pltpu.VMEM((NY, HID, 128), BF),
            pltpu.VMEM((NY, HID, 128), BF),
            pltpu.VMEM((NY, HID, 128), BF),
            pltpu.VMEM((NY, 24, 64), F32),
            pltpu.VMEM((NY, 64, MCOLS), BF),
            pltpu.VMEM((NY, 64, 512), BF),
            pltpu.VMEM((NY, 2, 64, FFT), BF),
            pltpu.VMEM((NY, 64, FFT), BF),
            pltpu.VMEM((2 * PAD, ROWS), BF),
            pltpu.VMEM((PAD, ROWS), BF),
            pltpu.VMEM((ROWS, ROWS), F32),
            pltpu.VMEM((2, 8, ROWS), F32),
            pltpu.VMEM((KV, 8, ROWS), BF),
            pltpu.VMEM((PLANE, 8, ROWS), BF),
            pltpu.VMEM((NZ, 2 * GROUP // 8, 8, ROWS), BF),
            pltpu.VMEM((NZ, 2 * GROUP // 8, 8, ROWS), BF),
            pltpu.VMEM((NZ, GROUP // 8, 8, ROWS), BF),
            pltpu.VMEM((PLANE, 8, ROWS), BF),
            pltpu.VMEM((PLANE, 8, ROWS), BF),
            pltpu.VMEM((NT, 8, ROWS), BF),
            pltpu.VMEM((NZ, 8, MCOLS), BF),
            pltpu.VMEM((NZ, 8, MCOLS), BF),
            pltpu.VMEM((NZ, 8, 512), BF),
            pltpu.VMEM((2, 4, 8, ROWS), BF),
            pltpu.VMEM((4, 8, ROWS), BF),
            pltpu.VMEM((NT, 4, 8, ROWS), BF),
            pltpu.VMEM((NZ, 8, 2 * FFP), BF),
            pltpu.VMEM((NZ, 8, 2 * FFP), BF),
            pltpu.VMEM((NZ, 8, FFP), BF),
            pltpu.VMEM((PLANE, 8, 128), BF),
            pltpu.VMEM((PLANE, 8, 128), BF),
            pltpu.VMEM((NY * 128, ROWS), BF),
        ],
        compiler_params=pltpu.CompilerParams(collective_id=0, has_side_effects=True, vmem_limit_bytes=40 << 20),
    )(*args)
    out, new_state = pl.pallas_call(
        deliver,
        out_shape=shapes,
        in_specs=[vmem, vmem],
        out_specs=(hbm, hbm),
        scratch_shapes=[pltpu.SemaphoreType.DMA((2,))],
        compiler_params=pltpu.CompilerParams(vmem_limit_bytes=40 << 20),
    )(out, new_state)
    return out.T, new_state


def solution(mesh):
    placed = (
        P(None, ("kv", "tp")),
        P("kv", "tp", None, None),
        P("kv"),
        P("kv", "tp"),
        P("kv", "tp"),
        P("tp", "kv"),
        P("kv"),
        P("kv", "tp"),
        P("kv", "tp"),
        P("kv", "tp"),
        P("kv", "tp"),
        P("kv", None),
        P("kv", None),
        P("tp"),
        P("tp"),
        P(),
        P("tp", "kv"),
        P("kv"),
        P("kv", "tp"),
        P("kv", "tp"),
        P("tp", "kv"),
    )
    return jax.shard_map(
        layer,
        mesh=mesh,
        in_specs=placed,
        out_specs=(P(None, ("kv", "tp")), P("kv", "tp", None, None)),
        check_vma=False,
    )
```

```python
import jax
import jax.numpy as jnp
from jax import lax
from jax.experimental import pallas as pl
from jax.experimental.pallas import tpu as pltpu
from jax.sharding import PartitionSpec as P

MESH = pl.DeviceIdType.MESH
BF, F32 = jnp.bfloat16, jnp.float32
D, EPS = 2048, 1e-6
NZ, NY, NT = 8, 4, 8
PLANE = NY * NT
KV = NZ * NY
ROWS = 256
HID, PITCH = 176, 192
HEAD = 128

X1, X2, X3, RS1, RS2, AG1, AG2, PR1, PR2, PR3, MIX, NRM, GU1, GN = range(14)
D1, MW, WO, GU2, D2 = 14, 18, 22, 26, 30
N_SEM = 34
MCOLS = 1664
FFT, FFP = 704, 768
RING_Z = (4, 3, 5, 2, 6, 1, 7)
FAR, FAR_Z = (0, 1, 2, 1), (0, 1, 2, 3, 4, 3, 2, 1)


def dot(a, b, ca, cb):
    return lax.dot_general(a, b, (((ca,), (cb,)), ((), ())), preferred_element_type=F32)


def iota(shape, dim):
    return lax.broadcasted_iota(jnp.int32, shape, dim)


def one_hot(cond):
    return jnp.where(cond, 1.0, 0.0).astype(BF)


def silu(v):
    return v / (1.0 + jnp.exp(-v))


def kernel(
    res_h, state, gain1_h, gain2_h, gain3_h, gate1_h, up1_h, down1_h, gate2_h, up2_h, down2_h,
    wq_h, wk_h, wv_h, wg_h, wbeta_h, wdecay_h, rate_h, bias_h, hgain_h, wo_h,
    out, state_out,
    res, s_buf, gain1, gain2, gain3, gate1, up1, down1, wbeta, wdecay, rate, bias, hgain,
    in_sem, send, recv,
    gu_src, gu_rcv, gn, d1, mw, wo, gu2, d2,
    g_row, xrow, xg, f_src, f_rcv, hg, pa_src, pa_rcv, pb,
    m_src, m_rcv, nb, rs2_src, rs2_rcv, pr3_src, pr3_rcv, place,
):
    kv = lax.axis_index("kv")
    t = lax.axis_index("tp")
    z, y = lax.div(kv, NY), lax.rem(kv, NY)
    x, core = lax.div(t, 2), lax.rem(t, 2)
    me = y * NT + t
    zs = [lax.rem(z + o, NZ) for o in range(NZ)]
    ys = [lax.rem(y + o, NY) for o in range(NY)]
    ts = [[lax.rem(x + o, 4) * 2 + c for c in (core, 1 - core)] for o in range(4)]

    z_peers = [(zs[o], (zs[o] * NY + y, t)) for o in RING_Z]
    y_peers = [(ys[o], (z * NY + ys[o], t)) for o in (2, 1, 3)]
    t_peers = [(ts[dx][dc], (kv, ts[dx][dc])) for dx in (2, 1, 3, 0) for dc in (0, 1) if dx or dc]
    kv_peers = [(dz, dy) for dz in range(NZ) for dy in range(NY) if dz or dy]
    kv_peers.sort(key=lambda o: -(FAR_Z[o[0]] + FAR[o[1]]))
    kv_peers = [(zs[dz] * NY + ys[dy], (zs[dz] * NY + ys[dy], t)) for dz, dy in kv_peers]
    plane = [(dy, dx, dc) for dy in range(4) for dx in range(4) for dc in range(2) if dy or dx or dc]
    plane.sort(key=lambda o: -(FAR[o[0]] + FAR[o[1]]))
    plane_peers = [(ys[dy] * NT + ts[dx][dc], (z * NY + ys[dy], ts[dx][dc])) for dy, dx, dc in plane]

    inputs = (
        (gate1_h, gate1), (up1_h, up1), (res_h, res), (gain1_h, gain1), (gain2_h, gain2), (gain3_h, gain3), (down1_h, down1),
        (wbeta_h, wbeta), (wdecay_h, wdecay),
        (wq_h, mw.at[y, :, 0:256]), (wk_h, mw.at[y, :, 256:512]), (wv_h, mw.at[y, :, 512:1024]), (wg_h, mw.at[y, :, 1024:1536]),
        (wo_h, wo.at[y]), (gate2_h, gu2.at[y, 0]), (up2_h, gu2.at[y, 1]), (down2_h, d2.at[y]),
        (rate_h, rate), (bias_h, bias), (hgain_h, hgain), (state, s_buf),
    )
    named = {id(src): pltpu.make_async_copy(src, dst, in_sem.at[i]) for i, (src, dst) in enumerate(inputs)}
    early = 6
    for src, _ in inputs[:early]:
        named[id(src)].start()

    barrier = pltpu.get_barrier_semaphore()
    greet = z_peers[:3] + plane_peers[:10] + z_peers[3:5] + plane_peers[10:] + z_peers[5:]
    for _, peer in greet:
        pl.semaphore_signal(barrier, inc=1, device_id=peer, device_id_type=MESH)

    def ready(*refs):
        for ref in refs:
            named[id(ref)].wait()

    def put(src, dst, k, peer):
        pltpu.make_async_remote_copy(
            src_ref=src, dst_ref=dst, send_sem=send.at[k], recv_sem=recv.at[k], device_id=peer, device_id_type=MESH
        ).start()

    def arrived(part, k):
        pltpu.make_async_copy(part, part, recv.at[k]).wait()

    def left(part, k):
        pltpu.make_async_copy(part, part, send.at[k]).wait()

    def share(buf, own, k, peers):
        for _, peer in peers:
            put(buf.at[own], buf.at[own], k, peer)

    def deal(src, dst, own, k, peers):
        for p, peer in peers:
            put(src.at[p], dst.at[own], k, peer)
        dst[own] = src[own]

    above, below = (z * NY + ys[1], t), (z * NY + ys[3], t)

    def y_start(buf, k):
        put(buf.at[y], buf.at[y], k, above)
        put(buf.at[y], buf.at[y], k + 1, below)

    def halves(buf, p):
        n = buf.shape[1] // 2
        return buf.at[p, pl.ds(0, n)], buf.at[p, pl.ds(n, n)]

    def y_pass(buf, k):
        arrived(buf.at[ys[3]], k)
        first, second = halves(buf, ys[3])
        put(first, first, k + 2, above)
        arrived(buf.at[ys[1]], k + 1)
        first, second = halves(buf, ys[1])
        put(second, second, k + 3, below)

    def y_done(buf, k):
        first, second = halves(buf, ys[2])
        arrived(first, k + 2)
        arrived(second, k + 3)

    def y_left(buf, k):
        first, second = halves(buf, 0)
        left(buf.at[0], k)
        left(buf.at[0], k + 1)
        left(first, k + 2)
        left(second, k + 3)

    lane = iota((64, FFP), 1)
    pos = lane - PITCH * sum(jnp.where(lane >= PITCH * p, 1, 0) for p in range(1, NY))

    def spread(v):
        v = jnp.concatenate([v.astype(F32), jnp.zeros((64, FFP - FFT), F32)], axis=1)
        w = v
        for p in range(1, NY):
            w = jnp.where(lane >= PITCH * p, pltpu.roll(v, (PITCH - HID) * p, 1), w)
        return jnp.where(pos < HID, w, 0.0)

    ready(gate1_h, up1_h)
    gate, up = spread(gate1[...]), spread(up1[...])
    first = iota((64, 2 * PITCH), 1) < PITCH
    for h in range(2):
        a = gate[:, 2 * PITCH * h : 2 * PITCH * (h + 1)]
        b = pltpu.roll(up[:, 2 * PITCH * h : 2 * PITCH * (h + 1)], PITCH, 1)
        gu_src[2 * h] = jnp.where(first, a, b).astype(BF)
        gu_src[2 * h + 1] = jnp.where(first, b, a).astype(BF)
    ready(res_h, gain1_h, gain2_h, gain3_h)
    xg[me] = res[...]
    gn[y, 0:8] = jnp.broadcast_to(gain1[...], (8, 64))
    gn[y, 8:16] = jnp.broadcast_to(gain2[...], (8, 64))
    gn[y, 16:24] = jnp.broadcast_to(gain3[...], (8, 64))

    pl.semaphore_wait(barrier, len(greet))

    share(gn, y, GN, y_peers)
    deal(gu_src, gu_rcv, y, GU1, y_peers)
    share(xg, me, X1, plane_peers)

    for src, _ in inputs[early:]:
        named[id(src)].start()
    ready(down1_h)
    d1[y] = spread(down1[...]).astype(BF)
    sel_b = one_hot((iota((32, 128), 0) == iota((32, 128), 1) + 4 * t) & (iota((32, 128), 1) < 4))
    sel_d = one_hot((iota((32, 128), 0) == iota((32, 128), 1) - 4 + 4 * t) & (iota((32, 128), 1) >= 4) & (iota((32, 128), 1) < 8))
    ready(wbeta_h, wdecay_h)
    mw[y, :, 1536:MCOLS] = (dot(wbeta[...], sel_b, 0, 0) + dot(wdecay[...], sel_d, 0, 0)).astype(BF)

    eye64 = iota((64, 64), 0) == iota((64, 64), 1)
    lane64 = iota((64, 128), 1)

    def column(p, i):
        row = gn[p, 8 * i : 8 * i + 1]
        return jnp.sum(jnp.where(eye64, jnp.broadcast_to(row, (64, 64)), 0.0), axis=1, keepdims=True)

    arrived(gn.at[pl.ds(0, NY - 1)], GN)
    for i in range(3):
        for h in range(2):
            wide = jnp.where(lane64 == iota((64, 128), 0), column(2 * h, i), 0.0)
            wide = wide + jnp.where(lane64 == iota((64, 128), 0) + 64, column(2 * h + 1, i), 0.0)
            g_row[i, :, 128 * h : 128 * (h + 1)] = jnp.broadcast_to(jnp.sum(wide, axis=0, keepdims=True), (8, 128))

    def scaled_of(v, i):
        squares = jnp.sum(v * v, axis=1, keepdims=True)
        coarse = squares.astype(BF).astype(F32)
        return (v * g_row[i, 0:1]).astype(BF), coarse, squares - coarse

    arrived(xg.at[pl.ds(0, PLANE - 1)], X1)
    x0 = jnp.transpose(xg[...].astype(F32).reshape(ROWS, ROWS))
    scaled, coarse, fine = scaled_of(x0, 0)
    arrived(gu_rcv.at[pl.ds(0, NY - 1)], GU1)
    part = dot(scaled, gu_rcv[...].reshape(ROWS, 2 * PITCH), 1, 0)
    at = iota((ROWS, 2 * PITCH), 1)
    part = part + jnp.where(at == HID, coarse, 0.0) + jnp.where(at == HID + 1, fine, 0.0)
    f_src[...] = part.reshape(KV, 8, 2 * PITCH).astype(BF)
    deal(f_src, f_rcv, kv, RS1, kv_peers)
    y_start(d1, D1)
    ready(wq_h, wk_h, wv_h, wg_h)
    y_start(mw, MW)
    xrow[...] = x0.reshape(NZ, NY, 8, ROWS).astype(BF)
    arrived(f_rcv.at[pl.ds(0, KV - 1)], RS1)
    quarters = jnp.sum(f_rcv[...].astype(F32).reshape(NZ, NY, 8, 2 * PITCH), axis=0)
    scale = lax.rsqrt((quarters[0, :, HID : HID + 1] + quarters[0, :, HID + 1 : HID + 2]) / D + EPS)
    at = iota((8, 2 * PITCH), 1)
    pos = at - PITCH * jnp.where(at >= PITCH, 1, 0)
    for h in range(2):
        a, b = quarters[2 * h], quarters[2 * h + 1]
        gate = jnp.where(at < PITCH, a, b) * scale
        up = pltpu.roll(jnp.where(at < PITCH, b, a), PITCH, 1) * scale
        hg[0, z, :, 2 * PITCH * h : 2 * PITCH * (h + 1)] = jnp.where(pos < HID, silu(gate) * up, 0.0).astype(BF)
    share(hg.at[0], z, AG1, z_peers)
    y_pass(d1, D1)
    y_pass(mw, MW)
    y_done(d1, D1)

    def gathered_hidden(i, k):
        arrived(hg.at[i, pl.ds(0, NZ - 1)], k)
        return hg[i].astype(F32).reshape(64, FFP).astype(BF)

    def swap(part, i, k):
        pa_src[i] = part.reshape(2, 4, 8, ROWS).astype(BF)
        put(pa_src.at[i, 1 - core], pa_rcv.at[i], k, (kv, ts[0][1]))
        mine = jnp.where(core == 0, part[0:32], part[32:64])
        arrived(pa_rcv.at[i], k)
        pb[i, t] = (mine.reshape(4, 8, ROWS) + pa_rcv[i].astype(F32)).astype(BF)

    def everyones(i, k):
        arrived(pb.at[i, pl.ds(0, NT - 1)], k)
        branch = []
        for c in range(2):
            half = pb[i, c].astype(F32)
            for j in range(1, 4):
                half = half + pb[i, 2 * j + c].astype(F32)
            branch.append(half.reshape(32, ROWS))
        return jnp.concatenate(branch, axis=0)

    h = gathered_hidden(0, AG1)
    swap(dot(h, d1[...].reshape(ROWS, FFP), 1, 1), 0, PR1)
    share(pb.at[0], t, X2, t_peers)
    y_done(mw, MW)
    x1 = xrow[:, y].astype(F32).reshape(64, ROWS)
    x1 = (x1 + 0.5 * everyones(0, X2)).astype(BF).astype(F32)
    scaled, coarse, fine = scaled_of(x1, 1)
    last = iota((64, 128), 1)
    for a, b in ((0, 512), (512, 1024), (1024, 1536), (1536, MCOLS)):
        part = dot(scaled, mw[:, :, a:b].reshape(ROWS, b - a), 1, 0)
        if a == 1536:
            part = part + jnp.where(last == 8, coarse, 0.0) + jnp.where(last == 9, fine, 0.0)
        m_src[:, :, a:b] = part.reshape(NZ, 8, b - a).astype(BF)
    deal(m_src, m_rcv, z, MIX, z_peers)
    ready(wo_h, gate2_h, up2_h, down2_h, state, rate_h, bias_h, hgain_h)
    y_start(wo, WO)
    y_start(gu2, GU2)
    arrived(m_rcv.at[pl.ds(0, NZ - 1)], MIX)

    mixed = jnp.sum(m_rcv[...].astype(F32), axis=0)
    ext = mixed[:, 1536:MCOLS]
    rowscale = lax.rsqrt((ext[:, 8:9] + ext[:, 9:10]) / D + EPS)
    heads = [mixed[:, 128 * i : 128 * (i + 1)] * rowscale for i in range(12)]

    def factor(v):
        return lax.rsqrt(jnp.sum(v * v, axis=-1, keepdims=True) + EPS)

    q = [silu(heads[m]) for m in range(2)]
    k = [silu(heads[2 + m]) for m in range(2)]
    q_t = [jnp.transpose(v) for v in q]
    k_t = [jnp.transpose(v) for v in k]
    q_f = [factor(v) * HEAD**-0.5 for v in q]
    k_f = [factor(v) for v in k]
    kq = [jnp.sum(k[m] * q[m], axis=-1, keepdims=True) * k_f[m] * q_f[m] for m in range(2)]
    ext = ext * rowscale
    by_k, by_q = [[] for _ in range(4)], [[] for _ in range(4)]
    for m in range(2):
        for i in range(8):
            k_col = jnp.broadcast_to(k_t[m][:, i : i + 1], (HEAD, HEAD))
            q_col = jnp.broadcast_to(q_t[m][:, i : i + 1], (HEAD, HEAD))
            for h in (2 * m, 2 * m + 1):
                s = s_buf[i, h]
                by_k[h].append(jnp.sum(s * k_col, axis=0, keepdims=True))
                by_q[h].append(jnp.sum(s * q_col, axis=0, keepdims=True))
    new = []
    for h in range(4):
        m = h // 2
        val = silu(heads[4 + h])
        gate = silu(heads[8 + h])
        beta = 1.0 / (1.0 + jnp.exp(-ext[:, h : h + 1]))
        pre = ext[:, 4 + h : 5 + h] + bias[:, h : h + 1]
        soft = jnp.maximum(pre, 0.0) + jnp.log1p(jnp.exp(-jnp.abs(pre)))
        decay = jnp.exp(-jnp.exp(rate[:, h : h + 1]) * soft)
        corr = beta * (val - decay * k_f[m] * jnp.concatenate(by_k[h], axis=0))
        reading = decay * q_f[m] * jnp.concatenate(by_q[h], axis=0) + kq[m] * corr
        norm = lax.rsqrt(jnp.mean(reading * reading, axis=-1, keepdims=True) + EPS)
        nb[z, :, 128 * h : 128 * (h + 1)] = (reading * norm * hgain[...] * gate).astype(BF)
        new.append((decay, corr * k_f[m]))
    share(nb, z, NRM, z_peers)
    y_pass(wo, WO)
    y_pass(gu2, GU2)
    y_start(d2, D2)
    for i in range(8):
        for m in range(2):
            k_col = jnp.broadcast_to(k_t[m][:, i : i + 1], (HEAD, HEAD))
            for h in (2 * m, 2 * m + 1):
                decay, corr = new[h]
                state_out[i, h] = s_buf[i, h] * decay[i : i + 1] + k_col * corr[i : i + 1]
    y_done(wo, WO)
    arrived(nb.at[pl.ds(0, NZ - 1)], NRM)
    normed = nb[...].astype(F32).reshape(64, 512).astype(BF)
    part = dot(normed, wo[...].reshape(ROWS, 512), 1, 1)
    swap(part, 1, PR2)
    share(pb.at[1], t, X3, t_peers)
    y_done(gu2, GU2)

    x3 = (x1 + everyones(1, X3)).astype(BF).astype(F32)
    scaled, coarse, fine = scaled_of(x3, 2)
    gate = dot(scaled, gu2[:, 0].reshape(ROWS, FFT), 1, 0)
    up = dot(scaled, gu2[:, 1].reshape(ROWS, FFT), 1, 0)
    fill = jnp.where(iota((64, 64), 1) == 0, coarse, jnp.where(iota((64, 64), 1) == 1, fine, 0.0))
    rs2_src[:, :, 0:FFP] = jnp.concatenate([gate, fill], axis=1).reshape(NZ, 8, FFP).astype(BF)
    rs2_src[:, :, FFP:] = jnp.concatenate([up, jnp.zeros((64, 64), F32)], axis=1).reshape(NZ, 8, FFP).astype(BF)
    deal(rs2_src, rs2_rcv, z, RS2, z_peers)
    y_pass(d2, D2)
    x3_t = jnp.transpose(jnp.concatenate([jnp.zeros((64, ROWS), F32), x3], axis=0))
    arrived(rs2_rcv.at[pl.ds(0, NZ - 1)], RS2)
    both = jnp.sum(rs2_rcv[...].astype(F32), axis=0)
    gate, up = both[:, 0:FFP], both[:, FFP:]
    scale = lax.rsqrt((gate[:, FFT : FFT + 1] + gate[:, FFT + 1 : FFT + 2]) / D + EPS)
    hidden = silu(gate * scale) * (up * scale)
    hg[1, z] = jnp.where(iota((8, FFP), 1) < FFT, hidden, 0.0).astype(BF)
    share(hg.at[1], z, AG2, z_peers)
    l, b = iota((128, ROWS), 0), iota((128, ROWS), 1)
    for p in range(NY):
        place[128 * p : 128 * (p + 1)] = one_hot((b == l + 24 * lax.shift_right_logical(l, 3) + 8 * p) & (l < 64))
    y_done(d2, D2)
    h = gathered_hidden(1, AG2)[:, 0:FFT]
    h = jnp.concatenate([h, jnp.zeros((64, FFT), BF)], axis=0)
    part = dot(d2[...].reshape(ROWS, FFT), h, 1, 1) + x3_t
    pr3_src[...] = part.reshape(PLANE, 8, 128).astype(BF)
    deal(pr3_src, pr3_rcv, me, PR3, plane_peers)
    arrived(pr3_rcv.at[pl.ds(0, PLANE - 1)], PR3)
    pieces = []
    for p in range(NY):
        total = jnp.sum(pr3_rcv[NT * p : NT * (p + 1)].astype(F32), axis=0)
        base = pltpu.roll(pr3_rcv[NT * p].astype(F32), 64, 1)
        pieces.append((base + 0.5 * total).astype(BF))
    final = dot(jnp.concatenate(pieces, axis=1), place[...], 1, 0)
    out[...] = final.astype(BF)

    left(xg.at[pl.ds(0, PLANE - 1)], X1)
    left(f_src.at[pl.ds(0, KV - 1)], RS1)
    left(pr3_src.at[pl.ds(0, PLANE - 1)], PR3)
    for i, (ag, pr, xx) in enumerate(((AG1, PR1, X2), (AG2, PR2, X3))):
        left(hg.at[i, pl.ds(0, NZ - 1)], ag)
        left(pa_rcv.at[i], pr)
        left(pb.at[i, pl.ds(0, NT - 1)], xx)
    left(m_src.at[pl.ds(0, NZ - 1)], MIX)
    left(nb.at[pl.ds(0, NZ - 1)], NRM)
    left(rs2_src.at[pl.ds(0, NZ - 1)], RS2)
    left(gu_src.at[pl.ds(0, NY - 1)], GU1)
    left(gn.at[pl.ds(0, NY - 1)], GN)
    y_left(d1, D1)
    y_left(mw, MW)
    y_left(wo, WO)
    y_left(gu2, GU2)
    y_left(d2, D2)


def deliver(out_in, state_in, out, state_out, sems):
    copies = [pltpu.make_async_copy(out_in, out, sems.at[0]), pltpu.make_async_copy(state_in, state_out, sems.at[1])]
    for copy in copies:
        copy.start()
    for copy in copies:
        copy.wait()


def layer(res, state, gain1, gate1, up1, down1, gain2, wq, wk, wv, wg, wbeta, wdecay, rate, bias, hgain, wo, gain3, gate2, up2, down2):
    vmem = pl.BlockSpec(memory_space=pltpu.VMEM)
    args = (
        res.T, state, gain1[None], gain2[None], gain3[None], gate1, up1, down1.T, gate2, up2, down2.T,
        wq, wk, wv, wg, wbeta.T, wdecay.T, rate[None], bias[None], hgain[None], wo.T,
    )
    args = tuple(pltpu.with_memory_space_constraint(a, pltpu.HBM) for a in args)
    held = [args[i] for i in (0, 1, 2, 3, 4, 5, 6, 7, 15, 16, 17, 18, 19)]
    hbm = pl.BlockSpec(memory_space=pltpu.HBM)
    shapes = (jax.ShapeDtypeStruct((8, ROWS), BF), jax.ShapeDtypeStruct(state.shape, F32))
    out, new_state = pl.pallas_call(
        kernel,
        out_shape=(pltpu.VMEM((8, ROWS), BF), pltpu.VMEM(state.shape, F32)),
        in_specs=[hbm] * len(args),
        out_specs=(vmem, vmem),
        scratch_shapes=[pltpu.VMEM(a.shape, a.dtype) for a in held]
        + [
            pltpu.SemaphoreType.DMA((len(args),)),
            pltpu.SemaphoreType.DMA((N_SEM,)),
            pltpu.SemaphoreType.DMA((N_SEM,)),
            pltpu.VMEM((NY, 64, 2 * PITCH), BF),
            pltpu.VMEM((NY, 64, 2 * PITCH), BF),
            pltpu.VMEM((NY, 24, 64), F32),
            pltpu.VMEM((NY, 64, FFP), BF),
            pltpu.VMEM((NY, 64, MCOLS), BF),
            pltpu.VMEM((NY, 64, 512), BF),
            pltpu.VMEM((NY, 2, 64, FFT), BF),
            pltpu.VMEM((NY, 64, FFT), BF),
            pltpu.VMEM((3, 8, ROWS), F32),
            pltpu.VMEM((NZ, NY, 8, ROWS), BF),
            pltpu.VMEM((PLANE, 8, ROWS), BF),
            pltpu.VMEM((KV, 8, 2 * PITCH), BF),
            pltpu.VMEM((KV, 8, 2 * PITCH), BF),
            pltpu.VMEM((2, NZ, 8, FFP), BF),
            pltpu.VMEM((2, 2, 4, 8, ROWS), BF),
            pltpu.VMEM((2, 4, 8, ROWS), BF),
            pltpu.VMEM((2, NT, 4, 8, ROWS), BF),
            pltpu.VMEM((NZ, 8, MCOLS), BF),
            pltpu.VMEM((NZ, 8, MCOLS), BF),
            pltpu.VMEM((NZ, 8, 512), BF),
            pltpu.VMEM((NZ, 8, 2 * FFP), BF),
            pltpu.VMEM((NZ, 8, 2 * FFP), BF),
            pltpu.VMEM((PLANE, 8, 128), BF),
            pltpu.VMEM((PLANE, 8, 128), BF),
            pltpu.VMEM((NY * 128, ROWS), BF),
        ],
        compiler_params=pltpu.CompilerParams(collective_id=0, has_side_effects=True, vmem_limit_bytes=40 << 20),
    )(*args)
    out, new_state = pl.pallas_call(
        deliver,
        out_shape=shapes,
        in_specs=[vmem, vmem],
        out_specs=(hbm, hbm),
        scratch_shapes=[pltpu.SemaphoreType.DMA((2,))],
        compiler_params=pltpu.CompilerParams(vmem_limit_bytes=40 << 20),
    )(out, new_state)
    return out.T, new_state


def solution(mesh):
    placed = (
        P(None, ("kv", "tp")),
        P("kv", "tp", None, None),
        P("kv"),
        P("kv", "tp"),
        P("kv", "tp"),
        P("tp", "kv"),
        P("kv"),
        P("kv", "tp"),
        P("kv", "tp"),
        P("kv", "tp"),
        P("kv", "tp"),
        P("kv", None),
        P("kv", None),
        P("tp"),
        P("tp"),
        P(),
        P("tp", "kv"),
        P("kv"),
        P("kv", "tp"),
        P("kv", "tp"),
        P("tp", "kv"),
    )
    return jax.shard_map(
        layer,
        mesh=mesh,
        in_specs=placed,
        out_specs=(P(None, ("kv", "tp")), P("kv", "tp", None, None)),
        check_vma=False,
    )
```

```python
import jax
import jax.numpy as jnp
from jax import lax
from jax.experimental import pallas as pl
from jax.experimental.pallas import tpu as pltpu
from jax.sharding import PartitionSpec as P

MESH = pl.DeviceIdType.MESH
BF, F32 = jnp.bfloat16, jnp.float32
D, EPS = 2048, 1e-6
NZ, NY, NT = 8, 4, 8
PLANE = NY * NT
KV = NZ * NY
ROWS = 256
HID, PITCH = 176, 192
HEAD = 128

X1, X2, X3, RS1, RS2, AG1, AG2, PR1, PR2, PR3, MIX, VG, NRM, GU1, GN = range(15)
D1, MW, WO, GU2, D2 = 15, 19, 23, 27, 31
N_SEM = 35
MCOLS = 1664
QK = 640
FFT, FFP = 704, 768
RING_Z = (4, 3, 5, 2, 6, 1, 7)
FAR, FAR_Z = (0, 1, 2, 1), (0, 1, 2, 3, 4, 3, 2, 1)


def dot(a, b, ca, cb):
    return lax.dot_general(a, b, (((ca,), (cb,)), ((), ())), preferred_element_type=F32)


def iota(shape, dim):
    return lax.broadcasted_iota(jnp.int32, shape, dim)


def one_hot(cond):
    return jnp.where(cond, 1.0, 0.0).astype(BF)


def silu(v):
    return v / (1.0 + jnp.exp(-v))


def kernel(
    res_h, state, gain1_h, gain2_h, gain3_h, gate1_h, up1_h, down1_h, gate2_h, up2_h, down2_h,
    wq_h, wk_h, wv_h, wg_h, wbeta_h, wdecay_h, rate_h, bias_h, hgain_h, wo_h,
    out, state_out,
    res, s_buf, gain1, gain2, gain3, gate1, up1, down1, wbeta, wdecay, rate, bias, hgain,
    in_sem, send, recv,
    gu_src, gu_rcv, gn, d1, mw, wo, gu2, d2,
    g_row, xrow, xg, f_src, f_rcv, hg, pa_src, pa_rcv, pb,
    m_src, m_rcv, v_src, v_rcv, nb, rs2_src, rs2_rcv, pr3_src, pr3_rcv, place,
):
    kv = lax.axis_index("kv")
    t = lax.axis_index("tp")
    z, y = lax.div(kv, NY), lax.rem(kv, NY)
    x, core = lax.div(t, 2), lax.rem(t, 2)
    me = y * NT + t
    zs = [lax.rem(z + o, NZ) for o in range(NZ)]
    ys = [lax.rem(y + o, NY) for o in range(NY)]
    ts = [[lax.rem(x + o, 4) * 2 + c for c in (core, 1 - core)] for o in range(4)]

    z_peers = [(zs[o], (zs[o] * NY + y, t)) for o in RING_Z]
    y_peers = [(ys[o], (z * NY + ys[o], t)) for o in (2, 1, 3)]
    t_peers = [(ts[dx][dc], (kv, ts[dx][dc])) for dx in (2, 1, 3, 0) for dc in (0, 1) if dx or dc]
    kv_peers = [(dz, dy) for dz in range(NZ) for dy in range(NY) if dz or dy]
    kv_peers.sort(key=lambda o: -(FAR_Z[o[0]] + FAR[o[1]]))
    kv_peers = [(zs[dz] * NY + ys[dy], (zs[dz] * NY + ys[dy], t)) for dz, dy in kv_peers]
    plane = [(dy, dx, dc) for dy in range(4) for dx in range(4) for dc in range(2) if dy or dx or dc]
    plane.sort(key=lambda o: -(FAR[o[0]] + FAR[o[1]]))
    plane_peers = [(ys[dy] * NT + ts[dx][dc], (z * NY + ys[dy], ts[dx][dc])) for dy, dx, dc in plane]

    inputs = (
        (gate1_h, gate1), (up1_h, up1), (res_h, res), (gain1_h, gain1), (gain2_h, gain2), (gain3_h, gain3), (down1_h, down1),
        (wbeta_h, wbeta), (wdecay_h, wdecay),
        (wq_h, mw.at[y, :, 0:256]), (wk_h, mw.at[y, :, 256:512]), (wv_h, mw.at[y, :, 640:1152]), (wg_h, mw.at[y, :, 1152:MCOLS]),
        (wo_h, wo.at[y]), (gate2_h, gu2.at[y, 0]), (up2_h, gu2.at[y, 1]), (down2_h, d2.at[y]),
        (rate_h, rate), (bias_h, bias), (hgain_h, hgain), (state, s_buf),
    )
    named = {id(src): pltpu.make_async_copy(src, dst, in_sem.at[i]) for i, (src, dst) in enumerate(inputs)}
    early = 6
    for src, _ in inputs[:early]:
        named[id(src)].start()

    barrier = pltpu.get_barrier_semaphore()
    greet = z_peers[:3] + plane_peers[:10] + z_peers[3:5] + plane_peers[10:] + z_peers[5:]
    for _, peer in greet:
        pl.semaphore_signal(barrier, inc=1, device_id=peer, device_id_type=MESH)

    def ready(*refs):
        for ref in refs:
            named[id(ref)].wait()

    def put(src, dst, k, peer):
        pltpu.make_async_remote_copy(
            src_ref=src, dst_ref=dst, send_sem=send.at[k], recv_sem=recv.at[k], device_id=peer, device_id_type=MESH
        ).start()

    def arrived(part, k):
        pltpu.make_async_copy(part, part, recv.at[k]).wait()

    def left(part, k):
        pltpu.make_async_copy(part, part, send.at[k]).wait()

    def share(buf, own, k, peers):
        for _, peer in peers:
            put(buf.at[own], buf.at[own], k, peer)

    def deal(src, dst, own, k, peers):
        for p, peer in peers:
            put(src.at[p], dst.at[own], k, peer)
        dst[own] = src[own]

    above, below = (z * NY + ys[1], t), (z * NY + ys[3], t)

    def y_start(buf, k):
        put(buf.at[y], buf.at[y], k, above)
        put(buf.at[y], buf.at[y], k + 1, below)

    def halves(buf, p):
        n = buf.shape[1] // 2
        return buf.at[p, pl.ds(0, n)], buf.at[p, pl.ds(n, n)]

    def y_pass(buf, k):
        arrived(buf.at[ys[3]], k)
        first, second = halves(buf, ys[3])
        put(first, first, k + 2, above)
        arrived(buf.at[ys[1]], k + 1)
        first, second = halves(buf, ys[1])
        put(second, second, k + 3, below)

    def y_done(buf, k):
        first, second = halves(buf, ys[2])
        arrived(first, k + 2)
        arrived(second, k + 3)

    def y_left(buf, k):
        first, second = halves(buf, 0)
        left(buf.at[0], k)
        left(buf.at[0], k + 1)
        left(first, k + 2)
        left(second, k + 3)

    lane = iota((64, FFP), 1)
    pos = lane - PITCH * sum(jnp.where(lane >= PITCH * p, 1, 0) for p in range(1, NY))

    def spread(v):
        v = jnp.concatenate([v.astype(F32), jnp.zeros((64, FFP - FFT), F32)], axis=1)
        w = v
        for p in range(1, NY):
            w = jnp.where(lane >= PITCH * p, pltpu.roll(v, (PITCH - HID) * p, 1), w)
        return jnp.where(pos < HID, w, 0.0)

    ready(gate1_h, up1_h)
    gate, up = spread(gate1[...]), spread(up1[...])
    first = iota((64, 2 * PITCH), 1) < PITCH
    for h in range(2):
        a = gate[:, 2 * PITCH * h : 2 * PITCH * (h + 1)]
        b = pltpu.roll(up[:, 2 * PITCH * h : 2 * PITCH * (h + 1)], PITCH, 1)
        gu_src[2 * h] = jnp.where(first, a, b).astype(BF)
        gu_src[2 * h + 1] = jnp.where(first, b, a).astype(BF)
    ready(res_h, gain1_h, gain2_h, gain3_h)
    xg[me] = res[...]
    gn[y, 0:1] = gain1[...]
    gn[y, 1:2] = gain2[...]
    gn[y, 2:3] = gain3[...]

    pl.semaphore_wait(barrier, len(greet))

    share(gn, y, GN, y_peers)
    share(xg, me, X1, plane_peers[:18])
    deal(gu_src, gu_rcv, y, GU1, y_peers)
    share(xg, me, X1, plane_peers[18:])

    for src, _ in inputs[early:]:
        named[id(src)].start()
    ready(down1_h)
    d1[y] = spread(down1[...]).astype(BF)
    sel_b = one_hot((iota((32, 128), 0) == iota((32, 128), 1) + 4 * t) & (iota((32, 128), 1) < 4))
    sel_d = one_hot((iota((32, 128), 0) == iota((32, 128), 1) - 4 + 4 * t) & (iota((32, 128), 1) >= 4) & (iota((32, 128), 1) < 8))
    ready(wbeta_h, wdecay_h)
    mw[y, :, 512:QK] = (dot(wbeta[...], sel_b, 0, 0) + dot(wdecay[...], sel_d, 0, 0)).astype(BF)

    eye64 = iota((64, 64), 0) == iota((64, 64), 1)
    lane64 = iota((64, 128), 1)

    def column(p, i):
        row = gn[p, i : i + 1]
        return jnp.sum(jnp.where(eye64, jnp.broadcast_to(row, (64, 64)), 0.0), axis=1, keepdims=True)

    arrived(gn.at[pl.ds(0, NY - 1)], GN)
    for i in range(3):
        for h in range(2):
            wide = jnp.where(lane64 == iota((64, 128), 0), column(2 * h, i), 0.0)
            wide = wide + jnp.where(lane64 == iota((64, 128), 0) + 64, column(2 * h + 1, i), 0.0)
            g_row[i, :, 128 * h : 128 * (h + 1)] = jnp.broadcast_to(jnp.sum(wide, axis=0, keepdims=True), (8, 128))

    def scaled_of(v, i):
        squares = jnp.sum(v * v, axis=1, keepdims=True)
        coarse = squares.astype(BF).astype(F32)
        return (v * g_row[i, 0:1]).astype(BF), coarse, squares - coarse

    arrived(xg.at[pl.ds(0, PLANE - 1)], X1)
    x0 = jnp.transpose(xg[...].astype(F32).reshape(ROWS, ROWS))
    scaled, coarse, fine = scaled_of(x0, 0)
    arrived(gu_rcv.at[pl.ds(0, NY - 1)], GU1)
    part = dot(scaled, gu_rcv[...].reshape(ROWS, 2 * PITCH), 1, 0)
    at = iota((ROWS, 2 * PITCH), 1)
    part = part + jnp.where(at == HID, coarse, 0.0) + jnp.where(at == HID + 1, fine, 0.0)
    f_src[...] = part.reshape(KV, 8, 2 * PITCH).astype(BF)
    deal(f_src, f_rcv, kv, RS1, kv_peers)
    y_start(d1, D1)
    ready(wq_h, wk_h, wv_h, wg_h)
    y_start(mw, MW)
    xrow[...] = x0.reshape(NZ, NY, 8, ROWS).astype(BF)
    y_pass(d1, D1)
    arrived(f_rcv.at[pl.ds(0, KV - 1)], RS1)
    quarters = jnp.sum(f_rcv[...].astype(F32).reshape(NZ, NY, 8, 2 * PITCH), axis=0)
    scale = lax.rsqrt((quarters[0, :, HID : HID + 1] + quarters[0, :, HID + 1 : HID + 2]) / D + EPS)
    at = iota((8, 2 * PITCH), 1)
    pos = at - PITCH * jnp.where(at >= PITCH, 1, 0)
    for h in range(2):
        a, b = quarters[2 * h], quarters[2 * h + 1]
        gate = jnp.where(at < PITCH, a, b) * scale
        up = pltpu.roll(jnp.where(at < PITCH, b, a), PITCH, 1) * scale
        hg[0, z, :, 2 * PITCH * h : 2 * PITCH * (h + 1)] = jnp.where(pos < HID, silu(gate) * up, 0.0).astype(BF)
    share(hg.at[0], z, AG1, z_peers)
    y_pass(mw, MW)
    y_done(d1, D1)

    def gathered_hidden(i, k):
        arrived(hg.at[i, pl.ds(0, NZ - 1)], k)
        return hg[i].astype(F32).reshape(64, FFP).astype(BF)

    def swap(part, i, k):
        pa_src[i] = part.reshape(2, 4, 8, ROWS).astype(BF)
        put(pa_src.at[i, 1 - core], pa_rcv.at[i], k, (kv, ts[0][1]))
        mine = jnp.where(core == 0, part[0:32], part[32:64])
        arrived(pa_rcv.at[i], k)
        pb[i, t] = (mine.reshape(4, 8, ROWS) + pa_rcv[i].astype(F32)).astype(BF)

    def everyones(i, k):
        arrived(pb.at[i, pl.ds(0, NT - 1)], k)
        branch = []
        for c in range(2):
            half = pb[i, c].astype(F32)
            for j in range(1, 4):
                half = half + pb[i, 2 * j + c].astype(F32)
            branch.append(half.reshape(32, ROWS))
        return jnp.concatenate(branch, axis=0)

    h = gathered_hidden(0, AG1)
    swap(dot(h, d1[...].reshape(ROWS, FFP), 1, 1), 0, PR1)
    share(pb.at[0], t, X2, t_peers)
    y_done(mw, MW)
    x1 = xrow[:, y].astype(F32).reshape(64, ROWS)
    x1 = (x1 + 0.5 * everyones(0, X2)).astype(BF).astype(F32)
    scaled, coarse, fine = scaled_of(x1, 1)
    last = iota((64, 128), 1)
    part = dot(scaled, mw[:, :, 0:512].reshape(ROWS, 512), 1, 0)
    m_src[:, :, 0:512] = part.reshape(NZ, 8, 512).astype(BF)
    part = dot(scaled, mw[:, :, 512:QK].reshape(ROWS, 128), 1, 0)
    part = part + jnp.where(last == 8, coarse, 0.0) + jnp.where(last == 9, fine, 0.0)
    m_src[:, :, 512:QK] = part.reshape(NZ, 8, 128).astype(BF)
    deal(m_src, m_rcv, z, MIX, z_peers)
    part = dot(scaled, mw[:, :, QK:MCOLS].reshape(ROWS, 1024), 1, 0)
    v_src[...] = part.reshape(NZ, 8, 1024).astype(BF)
    deal(v_src, v_rcv, z, VG, z_peers)
    ready(wo_h, gate2_h, up2_h, down2_h, state, rate_h, bias_h, hgain_h)
    y_start(wo, WO)
    y_start(gu2, GU2)
    arrived(m_rcv.at[pl.ds(0, NZ - 1)], MIX)

    mixed = jnp.sum(m_rcv[...].astype(F32), axis=0)
    ext = mixed[:, 512:QK]
    rowscale = lax.rsqrt((ext[:, 8:9] + ext[:, 9:10]) / D + EPS)
    heads = [mixed[:, 128 * i : 128 * (i + 1)] * rowscale for i in range(4)]

    def factor(v):
        return lax.rsqrt(jnp.sum(v * v, axis=-1, keepdims=True) + EPS)

    q = [silu(heads[m]) for m in range(2)]
    k = [silu(heads[2 + m]) for m in range(2)]
    q_t = [jnp.transpose(v) for v in q]
    k_t = [jnp.transpose(v) for v in k]
    q_f = [factor(v) * HEAD**-0.5 for v in q]
    k_f = [factor(v) for v in k]
    kq = [jnp.sum(k[m] * q[m], axis=-1, keepdims=True) * k_f[m] * q_f[m] for m in range(2)]
    ext = ext * rowscale
    by_k, by_q = [[] for _ in range(4)], [[] for _ in range(4)]
    for m in range(2):
        for i in range(8):
            k_col = jnp.broadcast_to(k_t[m][:, i : i + 1], (HEAD, HEAD))
            q_col = jnp.broadcast_to(q_t[m][:, i : i + 1], (HEAD, HEAD))
            for h in (2 * m, 2 * m + 1):
                s = s_buf[i, h]
                by_k[h].append(jnp.sum(s * k_col, axis=0, keepdims=True))
                by_q[h].append(jnp.sum(s * q_col, axis=0, keepdims=True))
    gates = []
    for h in range(4):
        beta = 1.0 / (1.0 + jnp.exp(-ext[:, h : h + 1]))
        pre = ext[:, 4 + h : 5 + h] + bias[:, h : h + 1]
        soft = jnp.maximum(pre, 0.0) + jnp.log1p(jnp.exp(-jnp.abs(pre)))
        decay = jnp.exp(-jnp.exp(rate[:, h : h + 1]) * soft)
        by_k[h] = decay * k_f[h // 2] * jnp.concatenate(by_k[h], axis=0)
        by_q[h] = decay * q_f[h // 2] * jnp.concatenate(by_q[h], axis=0)
        gates.append((beta, decay))
    arrived(v_rcv.at[pl.ds(0, NZ - 1)], VG)
    mixed = jnp.sum(v_rcv[...].astype(F32), axis=0)
    heads = [mixed[:, 128 * i : 128 * (i + 1)] * rowscale for i in range(8)]
    new = []
    for h in range(4):
        m = h // 2
        beta, decay = gates[h]
        val = silu(heads[h])
        gate = silu(heads[4 + h])
        corr = beta * (val - by_k[h])
        reading = by_q[h] + kq[m] * corr
        norm = lax.rsqrt(jnp.mean(reading * reading, axis=-1, keepdims=True) + EPS)
        nb[z, :, 128 * h : 128 * (h + 1)] = (reading * norm * hgain[...] * gate).astype(BF)
        new.append((decay, corr * k_f[m]))
    share(nb, z, NRM, z_peers)
    y_pass(wo, WO)
    y_pass(gu2, GU2)
    y_start(d2, D2)
    for i in range(8):
        for m in range(2):
            k_col = jnp.broadcast_to(k_t[m][:, i : i + 1], (HEAD, HEAD))
            for h in (2 * m, 2 * m + 1):
                decay, corr = new[h]
                state_out[i, h] = s_buf[i, h] * decay[i : i + 1] + k_col * corr[i : i + 1]
    y_done(wo, WO)
    arrived(nb.at[pl.ds(0, NZ - 1)], NRM)
    normed = nb[...].astype(F32).reshape(64, 512).astype(BF)
    part = dot(normed, wo[...].reshape(ROWS, 512), 1, 1)
    swap(part, 1, PR2)
    share(pb.at[1], t, X3, t_peers)
    y_done(gu2, GU2)

    x3 = (x1 + everyones(1, X3)).astype(BF).astype(F32)
    scaled, coarse, fine = scaled_of(x3, 2)
    gate = dot(scaled, gu2[:, 0].reshape(ROWS, FFT), 1, 0)
    up = dot(scaled, gu2[:, 1].reshape(ROWS, FFT), 1, 0)
    fill = jnp.where(iota((64, 64), 1) == 0, coarse, jnp.where(iota((64, 64), 1) == 1, fine, 0.0))
    rs2_src[:, :, 0:FFP] = jnp.concatenate([gate, fill], axis=1).reshape(NZ, 8, FFP).astype(BF)
    rs2_src[:, :, FFP:] = jnp.concatenate([up, jnp.zeros((64, 64), F32)], axis=1).reshape(NZ, 8, FFP).astype(BF)
    deal(rs2_src, rs2_rcv, z, RS2, z_peers)
    y_pass(d2, D2)
    x3_t = jnp.transpose(jnp.concatenate([jnp.zeros((64, ROWS), F32), x3], axis=0))
    arrived(rs2_rcv.at[pl.ds(0, NZ - 1)], RS2)
    both = jnp.sum(rs2_rcv[...].astype(F32), axis=0)
    gate, up = both[:, 0:FFP], both[:, FFP:]
    scale = lax.rsqrt((gate[:, FFT : FFT + 1] + gate[:, FFT + 1 : FFT + 2]) / D + EPS)
    hidden = silu(gate * scale) * (up * scale)
    hg[1, z] = jnp.where(iota((8, FFP), 1) < FFT, hidden, 0.0).astype(BF)
    share(hg.at[1], z, AG2, z_peers)
    l, b = iota((128, ROWS), 0), iota((128, ROWS), 1)
    for p in range(NY):
        place[128 * p : 128 * (p + 1)] = one_hot((b == l + 24 * lax.shift_right_logical(l, 3) + 8 * p) & (l < 64))
    y_done(d2, D2)
    h = gathered_hidden(1, AG2)[:, 0:FFT]
    h = jnp.concatenate([h, jnp.zeros((64, FFT), BF)], axis=0)
    part = dot(d2[...].reshape(ROWS, FFT), h, 1, 1) + x3_t
    pr3_src[...] = part.reshape(PLANE, 8, 128).astype(BF)
    deal(pr3_src, pr3_rcv, me, PR3, plane_peers)
    left(xg.at[pl.ds(0, PLANE - 1)], X1)
    left(f_src.at[pl.ds(0, KV - 1)], RS1)
    for i, (ag, pr, xx) in enumerate(((AG1, PR1, X2), (AG2, PR2, X3))):
        left(hg.at[i, pl.ds(0, NZ - 1)], ag)
        left(pa_rcv.at[i], pr)
        left(pb.at[i, pl.ds(0, NT - 1)], xx)
    left(m_src.at[pl.ds(0, NZ - 1)], MIX)
    left(v_src.at[pl.ds(0, NZ - 1)], VG)
    left(nb.at[pl.ds(0, NZ - 1)], NRM)
    left(rs2_src.at[pl.ds(0, NZ - 1)], RS2)
    left(gu_src.at[pl.ds(0, NY - 1)], GU1)
    left(gn.at[pl.ds(0, NY - 1)], GN)
    y_left(d1, D1)
    y_left(mw, MW)
    y_left(wo, WO)
    y_left(gu2, GU2)
    y_left(d2, D2)
    arrived(pr3_rcv.at[pl.ds(0, PLANE - 1)], PR3)
    pieces = []
    for p in range(NY):
        total = jnp.sum(pr3_rcv[NT * p : NT * (p + 1)].astype(F32), axis=0)
        base = pltpu.roll(pr3_rcv[NT * p].astype(F32), 64, 1)
        pieces.append((base + 0.5 * total).astype(BF))
    final = dot(jnp.concatenate(pieces, axis=1), place[...], 1, 0)
    out[...] = final.astype(BF)
    left(pr3_src.at[pl.ds(0, PLANE - 1)], PR3)


def deliver(out_in, state_in, out, state_out, sems):
    copies = [pltpu.make_async_copy(state_in.at[i], state_out.at[i], sems.at[i]) for i in range(8)]
    copies.append(pltpu.make_async_copy(out_in, out, sems.at[8]))
    for copy in copies:
        copy.start()
    for copy in copies:
        copy.wait()


def layer(res, state, gain1, gate1, up1, down1, gain2, wq, wk, wv, wg, wbeta, wdecay, rate, bias, hgain, wo, gain3, gate2, up2, down2):
    vmem = pl.BlockSpec(memory_space=pltpu.VMEM)
    args = (
        res.T, state, gain1[None], gain2[None], gain3[None], gate1, up1, down1.T, gate2, up2, down2.T,
        wq, wk, wv, wg, wbeta.T, wdecay.T, rate[None], bias[None], hgain[None], wo.T,
    )
    args = tuple(pltpu.with_memory_space_constraint(a, pltpu.HBM) for a in args)
    held = [args[i] for i in (0, 1, 2, 3, 4, 5, 6, 7, 15, 16, 17, 18, 19)]
    hbm = pl.BlockSpec(memory_space=pltpu.HBM)
    shapes = (jax.ShapeDtypeStruct((8, ROWS), BF), jax.ShapeDtypeStruct(state.shape, F32))
    out, new_state = pl.pallas_call(
        kernel,
        out_shape=(pltpu.VMEM((8, ROWS), BF), pltpu.VMEM(state.shape, F32)),
        in_specs=[hbm] * len(args),
        out_specs=(vmem, vmem),
        scratch_shapes=[pltpu.VMEM(a.shape, a.dtype) for a in held]
        + [
            pltpu.SemaphoreType.DMA((len(args),)),
            pltpu.SemaphoreType.DMA((N_SEM,)),
            pltpu.SemaphoreType.DMA((N_SEM,)),
            pltpu.VMEM((NY, 64, 2 * PITCH), BF),
            pltpu.VMEM((NY, 64, 2 * PITCH), BF),
            pltpu.VMEM((NY, 8, 64), F32),
            pltpu.VMEM((NY, 64, FFP), BF),
            pltpu.VMEM((NY, 64, MCOLS), BF),
            pltpu.VMEM((NY, 64, 512), BF),
            pltpu.VMEM((NY, 2, 64, FFT), BF),
            pltpu.VMEM((NY, 64, FFT), BF),
            pltpu.VMEM((3, 8, ROWS), F32),
            pltpu.VMEM((NZ, NY, 8, ROWS), BF),
            pltpu.VMEM((PLANE, 8, ROWS), BF),
            pltpu.VMEM((KV, 8, 2 * PITCH), BF),
            pltpu.VMEM((KV, 8, 2 * PITCH), BF),
            pltpu.VMEM((2, NZ, 8, FFP), BF),
            pltpu.VMEM((2, 2, 4, 8, ROWS), BF),
            pltpu.VMEM((2, 4, 8, ROWS), BF),
            pltpu.VMEM((2, NT, 4, 8, ROWS), BF),
            pltpu.VMEM((NZ, 8, QK), BF),
            pltpu.VMEM((NZ, 8, QK), BF),
            pltpu.VMEM((NZ, 8, 1024), BF),
            pltpu.VMEM((NZ, 8, 1024), BF),
            pltpu.VMEM((NZ, 8, 512), BF),
            pltpu.VMEM((NZ, 8, 2 * FFP), BF),
            pltpu.VMEM((NZ, 8, 2 * FFP), BF),
            pltpu.VMEM((PLANE, 8, 128), BF),
            pltpu.VMEM((PLANE, 8, 128), BF),
            pltpu.VMEM((NY * 128, ROWS), BF),
        ],
        compiler_params=pltpu.CompilerParams(collective_id=0, has_side_effects=True, vmem_limit_bytes=40 << 20),
    )(*args)
    out, new_state = pl.pallas_call(
        deliver,
        out_shape=shapes,
        in_specs=[vmem, vmem],
        out_specs=(hbm, hbm),
        scratch_shapes=[pltpu.SemaphoreType.DMA((9,))],
        compiler_params=pltpu.CompilerParams(vmem_limit_bytes=40 << 20),
    )(out, new_state)
    return out.T, new_state


def solution(mesh):
    placed = (
        P(None, ("kv", "tp")),
        P("kv", "tp", None, None),
        P("kv"),
        P("kv", "tp"),
        P("kv", "tp"),
        P("tp", "kv"),
        P("kv"),
        P("kv", "tp"),
        P("kv", "tp"),
        P("kv", "tp"),
        P("kv", "tp"),
        P("kv", None),
        P("kv", None),
        P("tp"),
        P("tp"),
        P(),
        P("tp", "kv"),
        P("kv"),
        P("kv", "tp"),
        P("kv", "tp"),
        P("tp", "kv"),
    )
    return jax.shard_map(
        layer,
        mesh=mesh,
        in_specs=placed,
        out_specs=(P(None, ("kv", "tp")), P("kv", "tp", None, None)),
        check_vma=False,
    )
```

```python
import jax
import jax.numpy as jnp
from jax import lax
from jax.experimental import pallas as pl
from jax.experimental.pallas import tpu as pltpu
from jax.sharding import PartitionSpec as P

MESH = pl.DeviceIdType.MESH
BF, F32 = jnp.bfloat16, jnp.float32
D, EPS = 2048, 1e-6
NZ, NY, NT = 8, 4, 8
PLANE = NY * NT
KV = NZ * NY
ROWS = 256
HID, PITCH = 176, 192
HEAD = 128

X1, X2, X3, RS1, RS2, AG1, AG2, PR1, PR2, PR3, MIX, VG, NRM, GU1, GN, SQ = range(16)
D1, MW, WO, GU2, D2, MV = 16, 20, 24, 28, 32, 36
N_SEM = 40
QK, VGC = 640, 1024
FFT, FFP = 704, 768
RING_Z = (4, 3, 5, 2, 6, 1, 7)
FAR, FAR_Z = (0, 1, 2, 1), (0, 1, 2, 3, 4, 3, 2, 1)


def dot(a, b, ca, cb):
    return lax.dot_general(a, b, (((ca,), (cb,)), ((), ())), preferred_element_type=F32)


def iota(shape, dim):
    return lax.broadcasted_iota(jnp.int32, shape, dim)


def one_hot(cond):
    return jnp.where(cond, 1.0, 0.0).astype(BF)


def silu(v):
    return v / (1.0 + jnp.exp(-v))


def kernel(
    res_h, state, gain1_h, gain2_h, gain3_h, gate1_h, up1_h, down1_h, gate2_h, up2_h, down2_h,
    wq_h, wk_h, wv_h, wg_h, wbeta_h, wdecay_h, rate_h, bias_h, hgain_h, wo_h,
    out, state_out,
    res, s_buf, gain1, gain2, gain3, gate1, up1, down1, gate2, up2, wbeta, wdecay, rate, bias, hgain,
    in_sem, send, recv,
    gu_src, gu_rcv, gn, d1, mw, mv, wo, gu2, d2,
    g_row, xrow, xg, f_src, f_rcv, hg, pa_src, pa_rcv, pb,
    m_src, m_rcv, v_src, v_rcv, nb, sq_src, sq_rcv, rs2_src, rs2_rcv, pr3_src, pr3_rcv,
):
    kv = lax.axis_index("kv")
    t = lax.axis_index("tp")
    z, y = lax.div(kv, NY), lax.rem(kv, NY)
    x, core = lax.div(t, 2), lax.rem(t, 2)
    me = y * NT + t
    zs = [lax.rem(z + o, NZ) for o in range(NZ)]
    ys = [lax.rem(y + o, NY) for o in range(NY)]
    ts = [[lax.rem(x + o, 4) * 2 + c for c in (core, 1 - core)] for o in range(4)]

    z_peers = [(zs[o], (zs[o] * NY + y, t)) for o in RING_Z]
    y_peers = [(ys[o], (z * NY + ys[o], t)) for o in (2, 1, 3)]
    t_peers = [(ts[dx][dc], (kv, ts[dx][dc])) for dx in (2, 1, 3, 0) for dc in (0, 1) if dx or dc]
    kv_peers = [(dz, dy) for dz in range(NZ) for dy in range(NY) if dz or dy]
    kv_peers.sort(key=lambda o: -(FAR_Z[o[0]] + FAR[o[1]]))
    kv_peers = [(zs[dz] * NY + ys[dy], (zs[dz] * NY + ys[dy], t)) for dz, dy in kv_peers]
    plane = [(dy, dx, dc) for dy in range(4) for dx in range(4) for dc in range(2) if dy or dx or dc]
    plane.sort(key=lambda o: -(FAR[o[0]] + FAR[o[1]]))
    plane_peers = [(ys[dy] * NT + ts[dx][dc], (z * NY + ys[dy], ts[dx][dc])) for dy, dx, dc in plane]

    inputs = (
        (gate1_h, gate1), (up1_h, up1), (res_h, res), (gain1_h, gain1), (gain2_h, gain2), (gain3_h, gain3), (down1_h, down1),
        (wbeta_h, wbeta), (wdecay_h, wdecay),
        (wq_h, mw.at[y, :, 0:256]), (wk_h, mw.at[y, :, 256:512]), (wv_h, mv.at[y, :, 0:512]), (wg_h, mv.at[y, :, 512:VGC]),
        (wo_h, wo.at[y]), (gate2_h, gate2), (up2_h, up2), (down2_h, d2.at[y]),
        (rate_h, rate), (bias_h, bias), (hgain_h, hgain), (state, s_buf),
    )
    named = {id(src): pltpu.make_async_copy(src, dst, in_sem.at[i]) for i, (src, dst) in enumerate(inputs)}
    early = 6
    for src, _ in inputs[:early]:
        named[id(src)].start()

    barrier = pltpu.get_barrier_semaphore()
    greet = z_peers[:3] + plane_peers[:10] + z_peers[3:5] + plane_peers[10:] + z_peers[5:]
    for _, peer in greet:
        pl.semaphore_signal(barrier, inc=1, device_id=peer, device_id_type=MESH)

    def ready(*refs):
        for ref in refs:
            named[id(ref)].wait()

    def put(src, dst, k, peer):
        pltpu.make_async_remote_copy(
            src_ref=src, dst_ref=dst, send_sem=send.at[k], recv_sem=recv.at[k], device_id=peer, device_id_type=MESH
        ).start()

    def arrived(part, k):
        pltpu.make_async_copy(part, part, recv.at[k]).wait()

    def left(part, k):
        pltpu.make_async_copy(part, part, send.at[k]).wait()

    def share(buf, own, k, peers):
        for _, peer in peers:
            put(buf.at[own], buf.at[own], k, peer)

    def deal(src, dst, own, k, peers):
        for p, peer in peers:
            put(src.at[p], dst.at[own], k, peer)
        dst[own] = src[own]

    above, below = (z * NY + ys[1], t), (z * NY + ys[3], t)

    def y_start(buf, k):
        put(buf.at[y], buf.at[y], k, above)
        put(buf.at[y], buf.at[y], k + 1, below)

    def halves(buf, p):
        n = buf.shape[1] // 2
        return buf.at[p, pl.ds(0, n)], buf.at[p, pl.ds(n, n)]

    def y_pass(buf, k):
        arrived(buf.at[ys[3]], k)
        first, second = halves(buf, ys[3])
        put(first, first, k + 2, above)
        arrived(buf.at[ys[1]], k + 1)
        first, second = halves(buf, ys[1])
        put(second, second, k + 3, below)

    def y_done(buf, k):
        first, second = halves(buf, ys[2])
        arrived(first, k + 2)
        arrived(second, k + 3)

    def y_left(buf, k):
        first, second = halves(buf, 0)
        left(buf.at[0], k)
        left(buf.at[0], k + 1)
        left(first, k + 2)
        left(second, k + 3)

    lane = iota((64, FFP), 1)
    pos = lane - PITCH * sum(jnp.where(lane >= PITCH * p, 1, 0) for p in range(1, NY))

    def spread(v):
        v = jnp.concatenate([v.astype(F32), jnp.zeros((64, FFP - FFT), F32)], axis=1)
        w = v
        for p in range(1, NY):
            w = jnp.where(lane >= PITCH * p, pltpu.roll(v, (PITCH - HID) * p, 1), w)
        return jnp.where(pos < HID, w, 0.0)

    ready(gate1_h, up1_h)
    gate, up = spread(gate1[...]), spread(up1[...])
    first = iota((64, 2 * PITCH), 1) < PITCH
    for h in range(2):
        a = gate[:, 2 * PITCH * h : 2 * PITCH * (h + 1)]
        b = pltpu.roll(up[:, 2 * PITCH * h : 2 * PITCH * (h + 1)], PITCH, 1)
        gu_src[2 * h] = jnp.where(first, a, b).astype(BF)
        gu_src[2 * h + 1] = jnp.where(first, b, a).astype(BF)
    ready(res_h, gain1_h, gain2_h, gain3_h)
    xg[me] = res[...]
    gn[y, 0:1] = gain1[...]
    gn[y, 1:2] = gain2[...]
    gn[y, 2:3] = gain3[...]

    pl.semaphore_wait(barrier, len(greet))

    share(gn, y, GN, y_peers)
    share(xg, me, X1, plane_peers[:18])
    deal(gu_src, gu_rcv, y, GU1, y_peers)
    share(xg, me, X1, plane_peers[18:])

    for src, _ in inputs[early:]:
        named[id(src)].start()
    ready(down1_h)
    d1[y] = spread(down1[...]).astype(BF)
    sel_b = one_hot((iota((32, 128), 0) == iota((32, 128), 1) + 4 * t) & (iota((32, 128), 1) < 4))
    sel_d = one_hot((iota((32, 128), 0) == iota((32, 128), 1) - 4 + 4 * t) & (iota((32, 128), 1) >= 4) & (iota((32, 128), 1) < 8))
    ready(wbeta_h, wdecay_h)
    mw[y, :, 512:QK] = (dot(wbeta[...], sel_b, 0, 0) + dot(wdecay[...], sel_d, 0, 0)).astype(BF)

    eye64 = iota((64, 64), 0) == iota((64, 64), 1)
    lane64 = iota((64, 128), 1)

    def column(p, i):
        row = gn[p, i : i + 1]
        return jnp.sum(jnp.where(eye64, jnp.broadcast_to(row, (64, 64)), 0.0), axis=1, keepdims=True)

    arrived(gn.at[pl.ds(0, NY - 1)], GN)
    for i in range(3):
        for h in range(2):
            wide = jnp.where(lane64 == iota((64, 128), 0), column(2 * h, i), 0.0)
            wide = wide + jnp.where(lane64 == iota((64, 128), 0) + 64, column(2 * h + 1, i), 0.0)
            g_row[i, :, 128 * h : 128 * (h + 1)] = jnp.broadcast_to(jnp.sum(wide, axis=0, keepdims=True), (8, 128))

    def scaled_of(v, i):
        squares = jnp.sum(v * v, axis=1, keepdims=True)
        coarse = squares.astype(BF).astype(F32)
        return (v * g_row[i, 0:1]).astype(BF), coarse, squares - coarse

    arrived(xg.at[pl.ds(0, PLANE - 1)], X1)
    x0 = jnp.transpose(xg[...].astype(F32).reshape(ROWS, ROWS))
    scaled, coarse, fine = scaled_of(x0, 0)
    arrived(gu_rcv.at[pl.ds(0, NY - 1)], GU1)
    part = dot(scaled, gu_rcv[...].reshape(ROWS, 2 * PITCH), 1, 0)
    at = iota((ROWS, 2 * PITCH), 1)
    part = part + jnp.where(at == HID, coarse, 0.0) + jnp.where(at == HID + 1, fine, 0.0)
    f_src[...] = part.reshape(KV, 8, 2 * PITCH).astype(BF)
    deal(f_src, f_rcv, kv, RS1, kv_peers)
    y_start(d1, D1)
    ready(wq_h, wk_h)
    y_start(mw, MW)
    xrow[...] = x0.reshape(NZ, NY, 8, ROWS).astype(BF)
    y_pass(d1, D1)
    ready(wv_h, wg_h)
    y_start(mv, MV)
    arrived(f_rcv.at[pl.ds(0, KV - 1)], RS1)
    quarters = jnp.sum(f_rcv[...].astype(F32).reshape(NZ, NY, 8, 2 * PITCH), axis=0)
    scale = lax.rsqrt((quarters[0, :, HID : HID + 1] + quarters[0, :, HID + 1 : HID + 2]) / D + EPS)
    at = iota((8, 2 * PITCH), 1)
    pos = at - PITCH * jnp.where(at >= PITCH, 1, 0)
    for h in range(2):
        a, b = quarters[2 * h], quarters[2 * h + 1]
        gate = jnp.where(at < PITCH, a, b) * scale
        up = pltpu.roll(jnp.where(at < PITCH, b, a), PITCH, 1) * scale
        hg[0, z, :, 2 * PITCH * h : 2 * PITCH * (h + 1)] = jnp.where(pos < HID, silu(gate) * up, 0.0).astype(BF)
    share(hg.at[0], z, AG1, z_peers)
    y_pass(mw, MW)
    y_done(d1, D1)

    def gathered_hidden(i, k):
        arrived(hg.at[i, pl.ds(0, NZ - 1)], k)
        return hg[i].astype(F32).reshape(64, FFP).astype(BF)

    def swap(part, i, k, between):
        pa_src[i] = part.reshape(2, 4, 8, ROWS).astype(BF)
        put(pa_src.at[i, 1 - core], pa_rcv.at[i], k, (kv, ts[0][1]))
        mine = jnp.where(core == 0, part[0:32], part[32:64])
        between()
        arrived(pa_rcv.at[i], k)
        pb[i, t] = (mine.reshape(4, 8, ROWS) + pa_rcv[i].astype(F32)).astype(BF)

    def everyones(i, k):
        arrived(pb.at[i, pl.ds(0, NT - 1)], k)
        branch = []
        for c in range(2):
            half = pb[i, c].astype(F32)
            for j in range(1, 4):
                half = half + pb[i, 2 * j + c].astype(F32)
            branch.append(half.reshape(32, ROWS))
        return jnp.concatenate(branch, axis=0)

    h = gathered_hidden(0, AG1)
    swap(dot(h, d1[...].reshape(ROWS, FFP), 1, 1), 0, PR1, lambda: y_pass(mv, MV))
    share(pb.at[0], t, X2, t_peers)
    y_done(mw, MW)
    x1 = xrow[:, y].astype(F32).reshape(64, ROWS)
    x1 = (x1 + 0.5 * everyones(0, X2)).astype(BF).astype(F32)
    scaled, coarse, fine = scaled_of(x1, 1)
    last = iota((64, 128), 1)
    part = dot(scaled, mw[:, :, 0:512].reshape(ROWS, 512), 1, 0)
    m_src[:, :, 0:512] = part.reshape(NZ, 8, 512).astype(BF)
    part = dot(scaled, mw[:, :, 512:QK].reshape(ROWS, 128), 1, 0)
    part = part + jnp.where(last == 8, coarse, 0.0) + jnp.where(last == 9, fine, 0.0)
    m_src[:, :, 512:QK] = part.reshape(NZ, 8, 128).astype(BF)
    deal(m_src, m_rcv, z, MIX, z_peers)
    y_done(mv, MV)
    part = dot(scaled, mv[...].reshape(ROWS, VGC), 1, 0)
    v_src[...] = part.reshape(NZ, 8, 1024).astype(BF)
    deal(v_src, v_rcv, z, VG, z_peers)
    ready(wo_h, gate2_h, up2_h, down2_h, state, rate_h, bias_h, hgain_h)
    y_start(wo, WO)
    gu2[y] = jnp.concatenate([gate2[...].astype(F32), up2[...].astype(F32)], axis=1).astype(BF)
    y_start(gu2, GU2)
    arrived(m_rcv.at[pl.ds(0, NZ - 1)], MIX)

    mixed = jnp.sum(m_rcv[...].astype(F32), axis=0)
    ext = mixed[:, 512:QK]
    rowscale = lax.rsqrt((ext[:, 8:9] + ext[:, 9:10]) / D + EPS)
    heads = [mixed[:, 128 * i : 128 * (i + 1)] * rowscale for i in range(4)]

    def factor(v):
        return lax.rsqrt(jnp.sum(v * v, axis=-1, keepdims=True) + EPS)

    q = [silu(heads[m]) for m in range(2)]
    k = [silu(heads[2 + m]) for m in range(2)]
    q_t = [jnp.transpose(v) for v in q]
    k_t = [jnp.transpose(v) for v in k]
    q_f = [factor(v) * HEAD**-0.5 for v in q]
    k_f = [factor(v) for v in k]
    kq = [jnp.sum(k[m] * q[m], axis=-1, keepdims=True) * k_f[m] * q_f[m] for m in range(2)]
    ext = ext * rowscale
    by_k, by_q = [[] for _ in range(4)], [[] for _ in range(4)]
    for m in range(2):
        for i in range(8):
            k_col = jnp.broadcast_to(k_t[m][:, i : i + 1], (HEAD, HEAD))
            q_col = jnp.broadcast_to(q_t[m][:, i : i + 1], (HEAD, HEAD))
            for h in (2 * m, 2 * m + 1):
                s = s_buf[i, h]
                by_k[h].append(jnp.sum(s * k_col, axis=0, keepdims=True))
                by_q[h].append(jnp.sum(s * q_col, axis=0, keepdims=True))
    gates = []
    for h in range(4):
        beta = 1.0 / (1.0 + jnp.exp(-ext[:, h : h + 1]))
        pre = ext[:, 4 + h : 5 + h] + bias[:, h : h + 1]
        soft = jnp.maximum(pre, 0.0) + jnp.log1p(jnp.exp(-jnp.abs(pre)))
        decay = jnp.exp(-jnp.exp(rate[:, h : h + 1]) * soft)
        by_k[h] = decay * k_f[h // 2] * jnp.concatenate(by_k[h], axis=0)
        by_q[h] = decay * q_f[h // 2] * jnp.concatenate(by_q[h], axis=0)
        gates.append((beta, decay))
    arrived(v_rcv.at[pl.ds(0, NZ - 1)], VG)
    mixed = jnp.sum(v_rcv[...].astype(F32), axis=0)
    heads = [mixed[:, 128 * i : 128 * (i + 1)] * rowscale for i in range(8)]
    new = []
    for h in range(4):
        m = h // 2
        beta, decay = gates[h]
        val = silu(heads[h])
        gate = silu(heads[4 + h])
        corr = beta * (val - by_k[h])
        reading = by_q[h] + kq[m] * corr
        norm = lax.rsqrt(jnp.mean(reading * reading, axis=-1, keepdims=True) + EPS)
        nb[z, :, 128 * h : 128 * (h + 1)] = (reading * norm * hgain[...] * gate).astype(BF)
        new.append((decay, corr * k_f[m]))
    share(nb, z, NRM, z_peers)
    y_pass(wo, WO)
    y_pass(gu2, GU2)
    y_start(d2, D2)
    for i in range(8):
        for m in range(2):
            k_col = jnp.broadcast_to(k_t[m][:, i : i + 1], (HEAD, HEAD))
            for h in (2 * m, 2 * m + 1):
                decay, corr = new[h]
                state_out[i, h] = s_buf[i, h] * decay[i : i + 1] + k_col * corr[i : i + 1]
    y_done(wo, WO)
    arrived(nb.at[pl.ds(0, NZ - 1)], NRM)
    normed = nb[...].astype(F32).reshape(64, 512).astype(BF)
    part = dot(normed, wo[...].reshape(ROWS, 512), 1, 1)
    swap(part, 1, PR2, lambda: None)
    share(pb.at[1], t, X3, t_peers)
    y_done(gu2, GU2)

    x3 = (x1 + everyones(1, X3)).astype(BF).astype(F32)
    scaled, coarse, fine = scaled_of(x3, 2)
    squares = jnp.where(last == 0, coarse, jnp.where(last == 1, fine, 0.0))
    sq_src[...] = squares.reshape(NZ, 8, 128).astype(BF)
    deal(sq_src, sq_rcv, z, SQ, z_peers)
    part = dot(scaled, gu2[...].reshape(ROWS, 2 * FFT), 1, 0)
    rs2_src[...] = part.reshape(NZ, 8, 2 * FFT).astype(BF)
    deal(rs2_src, rs2_rcv, z, RS2, z_peers)
    y_pass(d2, D2)
    x3_t = jnp.transpose(jnp.concatenate([jnp.zeros((64, ROWS), F32), x3], axis=0))
    arrived(sq_rcv.at[pl.ds(0, NZ - 1)], SQ)
    squares = jnp.sum(sq_rcv[...].astype(F32), axis=0)
    scale = lax.rsqrt((squares[:, 0:1] + squares[:, 1:2]) / D + EPS)
    arrived(rs2_rcv.at[pl.ds(0, NZ - 1)], RS2)
    both = jnp.sum(rs2_rcv[...].astype(F32), axis=0) * scale
    hidden = silu(both[:, 0:FFT]) * both[:, FFT:]
    hg[1, z] = jnp.concatenate([hidden, jnp.zeros((8, FFP - FFT), F32)], axis=1).astype(BF)
    share(hg.at[1], z, AG2, z_peers)
    y_done(d2, D2)
    h = gathered_hidden(1, AG2)[:, 0:FFT]
    h = jnp.concatenate([h, jnp.zeros((64, FFT), BF)], axis=0)
    part = dot(d2[...].reshape(ROWS, FFT), h, 1, 1) + x3_t
    pr3_src[...] = part.reshape(PLANE, 8, 128).astype(BF)
    deal(pr3_src, pr3_rcv, me, PR3, plane_peers)
    left(xg.at[pl.ds(0, PLANE - 1)], X1)
    left(f_src.at[pl.ds(0, KV - 1)], RS1)
    for i, (ag, pr, xx) in enumerate(((AG1, PR1, X2), (AG2, PR2, X3))):
        left(hg.at[i, pl.ds(0, NZ - 1)], ag)
        left(pa_rcv.at[i], pr)
        left(pb.at[i, pl.ds(0, NT - 1)], xx)
    left(m_src.at[pl.ds(0, NZ - 1)], MIX)
    left(v_src.at[pl.ds(0, NZ - 1)], VG)
    left(nb.at[pl.ds(0, NZ - 1)], NRM)
    left(rs2_src.at[pl.ds(0, NZ - 1)], RS2)
    left(gu_src.at[pl.ds(0, NY - 1)], GU1)
    left(gn.at[pl.ds(0, NY - 1)], GN)
    y_left(d1, D1)
    y_left(mw, MW)
    y_left(mv, MV)
    left(sq_src.at[pl.ds(0, NZ - 1)], SQ)
    y_left(wo, WO)
    y_left(gu2, GU2)
    y_left(d2, D2)
    arrived(pr3_rcv.at[pl.ds(0, PLANE - 1)], PR3)
    for p in range(NY):
        total = jnp.sum(pr3_rcv[NT * p : NT * (p + 1)].astype(F32), axis=0)
        base = pltpu.roll(pr3_rcv[NT * p].astype(F32), 64, 1)
        out[:, 128 * p : 128 * (p + 1)] = (base + 0.5 * total).astype(BF)
    left(pr3_src.at[pl.ds(0, PLANE - 1)], PR3)


def deliver(out_in, state_in, out, state_out, placed, sems):
    copies = [pltpu.make_async_copy(state_in.at[i], state_out.at[i], sems.at[i]) for i in range(8)]
    for copy in copies:
        copy.start()
    line, b = iota((128, ROWS), 0), iota((128, ROWS), 1)
    final = jnp.zeros((8, ROWS), F32)
    for p in range(NY):
        place = one_hot((b == line + 24 * lax.shift_right_logical(line, 3) + 8 * p) & (line < 64))
        final = final + dot(out_in[:, 128 * p : 128 * (p + 1)], place, 1, 0)
    placed[...] = final.astype(BF)
    copies.append(pltpu.make_async_copy(placed, out, sems.at[8]))
    copies[-1].start()
    for copy in copies:
        copy.wait()


def layer(res, state, gain1, gate1, up1, down1, gain2, wq, wk, wv, wg, wbeta, wdecay, rate, bias, hgain, wo, gain3, gate2, up2, down2):
    vmem = pl.BlockSpec(memory_space=pltpu.VMEM)
    args = (
        res.T, state, gain1[None], gain2[None], gain3[None], gate1, up1, down1.T, gate2, up2, down2.T,
        wq, wk, wv, wg, wbeta.T, wdecay.T, rate[None], bias[None], hgain[None], wo.T,
    )
    args = tuple(pltpu.with_memory_space_constraint(a, pltpu.HBM) for a in args)
    held = [args[i] for i in (0, 1, 2, 3, 4, 5, 6, 7, 8, 9, 15, 16, 17, 18, 19)]
    hbm = pl.BlockSpec(memory_space=pltpu.HBM)
    shapes = (jax.ShapeDtypeStruct((8, ROWS), BF), jax.ShapeDtypeStruct(state.shape, F32))
    out, new_state = pl.pallas_call(
        kernel,
        out_shape=(pltpu.VMEM((8, NY * 128), BF), pltpu.VMEM(state.shape, F32)),
        in_specs=[hbm] * len(args),
        out_specs=(vmem, vmem),
        scratch_shapes=[pltpu.VMEM(a.shape, a.dtype) for a in held]
        + [
            pltpu.SemaphoreType.DMA((len(args),)),
            pltpu.SemaphoreType.DMA((N_SEM,)),
            pltpu.SemaphoreType.DMA((N_SEM,)),
            pltpu.VMEM((NY, 64, 2 * PITCH), BF),
            pltpu.VMEM((NY, 64, 2 * PITCH), BF),
            pltpu.VMEM((NY, 8, 64), F32),
            pltpu.VMEM((NY, 64, FFP), BF),
            pltpu.VMEM((NY, 64, QK), BF),
            pltpu.VMEM((NY, 64, VGC), BF),
            pltpu.VMEM((NY, 64, 512), BF),
            pltpu.VMEM((NY, 64, 2 * FFT), BF),
            pltpu.VMEM((NY, 64, FFT), BF),
            pltpu.VMEM((3, 8, ROWS), F32),
            pltpu.VMEM((NZ, NY, 8, ROWS), BF),
            pltpu.VMEM((PLANE, 8, ROWS), BF),
            pltpu.VMEM((KV, 8, 2 * PITCH), BF),
            pltpu.VMEM((KV, 8, 2 * PITCH), BF),
            pltpu.VMEM((2, NZ, 8, FFP), BF),
            pltpu.VMEM((2, 2, 4, 8, ROWS), BF),
            pltpu.VMEM((2, 4, 8, ROWS), BF),
            pltpu.VMEM((2, NT, 4, 8, ROWS), BF),
            pltpu.VMEM((NZ, 8, QK), BF),
            pltpu.VMEM((NZ, 8, QK), BF),
            pltpu.VMEM((NZ, 8, 1024), BF),
            pltpu.VMEM((NZ, 8, 1024), BF),
            pltpu.VMEM((NZ, 8, 512), BF),
            pltpu.VMEM((NZ, 8, 128), BF),
            pltpu.VMEM((NZ, 8, 128), BF),
            pltpu.VMEM((NZ, 8, 2 * FFT), BF),
            pltpu.VMEM((NZ, 8, 2 * FFT), BF),
            pltpu.VMEM((PLANE, 8, 128), BF),
            pltpu.VMEM((PLANE, 8, 128), BF),
        ],
        compiler_params=pltpu.CompilerParams(collective_id=0, has_side_effects=True, vmem_limit_bytes=40 << 20),
    )(*args)
    out, new_state = pl.pallas_call(
        deliver,
        out_shape=shapes,
        in_specs=[vmem, vmem],
        out_specs=(hbm, hbm),
        scratch_shapes=[pltpu.VMEM((8, ROWS), BF), pltpu.SemaphoreType.DMA((9,))],
        compiler_params=pltpu.CompilerParams(vmem_limit_bytes=40 << 20),
    )(out, new_state)
    return out.T, new_state


def solution(mesh):
    placed = (
        P(None, ("kv", "tp")),
        P("kv", "tp", None, None),
        P("kv"),
        P("kv", "tp"),
        P("kv", "tp"),
        P("tp", "kv"),
        P("kv"),
        P("kv", "tp"),
        P("kv", "tp"),
        P("kv", "tp"),
        P("kv", "tp"),
        P("kv", None),
        P("kv", None),
        P("tp"),
        P("tp"),
        P(),
        P("tp", "kv"),
        P("kv"),
        P("kv", "tp"),
        P("kv", "tp"),
        P("tp", "kv"),
    )
    return jax.shard_map(
        layer,
        mesh=mesh,
        in_specs=placed,
        out_specs=(P(None, ("kv", "tp")), P("kv", "tp", None, None)),
        check_vma=False,
    )
```

```python
import jax
import jax.numpy as jnp
from jax import lax
from jax.experimental import pallas as pl
from jax.experimental.pallas import tpu as pltpu
from jax.sharding import PartitionSpec as P

MESH = pl.DeviceIdType.MESH
BF, F32 = jnp.bfloat16, jnp.float32
D, EPS = 2048, 1e-6
NZ, NY, NT = 8, 4, 8
PLANE = NY * NT
KV = NZ * NY
ROWS = 256
HID, PITCH = 176, 192
HEAD = 128

X1, X2, X3, RS1, RS2, AG1, AG2, PR1, PR2, PR3, MIX, VG, NRM, GU1, GN, SQ = range(16)
D1, MW, WO, GU2, D2, MV = range(16, 28, 2)
TILES, GAINS, DOWN2 = range(3)
I_W1, I_RES, I_GAIN, I_DOWN, I_BD, I_QK, I_VG, I_WO, I_W2, I_D2, I_RB, I_HEAD, I_STATE = range(13)
QK, VGC = 640, 1024
FFT, FFP = 704, 768
SENT = 31 * 2 + 3 * 24 + 31 * 3 + 14 * 6 + 2 * 8 + 14 * 8 + 7 * (5 + 8 + 4 + 1 + 11) + 31 + 3 * 8 * (6 + 5 + 8 + 4 + 11)
RING_Z = (4, 3, 5, 2, 6, 1, 7)
FAR, FAR_Z = (0, 1, 2, 1), (0, 1, 2, 3, 4, 3, 2, 1)


def dot(a, b, ca, cb):
    return lax.dot_general(a, b, (((ca,), (cb,)), ((), ())), preferred_element_type=F32)


def iota(shape, dim):
    return lax.broadcasted_iota(jnp.int32, shape, dim)


def one_hot(cond):
    return jnp.where(cond, 1.0, 0.0).astype(BF)


def silu(v):
    return v / (1.0 + jnp.exp(-v))


def kernel(
    res_h, state, gain1_h, gain2_h, gain3_h, gate1_h, up1_h, down1_h, gate2_h, up2_h, down2_h,
    wq_h, wk_h, wv_h, wg_h, wbeta_h, wdecay_h, rate_h, bias_h, hgain_h, wo_h,
    out, state_out,
    res, s_buf, gains, w1, w2, bd, rb, hgain,
    in_sem, send, recv, tiles,
    gu_src, gu_rcv, gn, d1, mw, mv, wo, gu2, d2,
    g_row, xrow, xg, f_src, f_rcv, hg, pa_src, pa_rcv, pb,
    m_src, m_rcv, v_src, v_rcv, nb, sq_src, sq_rcv, rs2_src, rs2_rcv, pr3_src, pr3_rcv,
):
    kv = lax.axis_index("kv")
    t = lax.axis_index("tp")
    z, y = lax.div(kv, NY), lax.rem(kv, NY)
    x, core = lax.div(t, 2), lax.rem(t, 2)
    me = y * NT + t
    zs = [lax.rem(z + o, NZ) for o in range(NZ)]
    ys = [lax.rem(y + o, NY) for o in range(NY)]
    ts = [[lax.rem(x + o, 4) * 2 + c for c in (core, 1 - core)] for o in range(4)]

    z_peers = [(zs[o], (zs[o] * NY + y, t)) for o in RING_Z]
    y_peers = [(ys[o], (z * NY + ys[o], t)) for o in (2, 1, 3)]
    t_peers = [(ts[dx][dc], (kv, ts[dx][dc])) for dx in (2, 1, 3, 0) for dc in (0, 1) if dx or dc]
    kv_peers = [(dz, dy) for dz in range(NZ) for dy in range(NY) if dz or dy]
    kv_peers.sort(key=lambda o: -(FAR_Z[o[0]] + FAR[o[1]]))
    kv_peers = [(zs[dz] * NY + ys[dy], (zs[dz] * NY + ys[dy], t)) for dz, dy in kv_peers]
    plane = [(dy, dx, dc) for dy in range(4) for dx in range(4) for dc in range(2) if dy or dx or dc]
    plane.sort(key=lambda o: -(FAR[o[0]] + FAR[o[1]]))
    plane_peers = [(ys[dy] * NT + ts[dx][dc], (z * NY + ys[dy], ts[dx][dc])) for dy, dx, dc in plane]

    inputs = (
        (I_W1, w1.at[pl.ds(0, 2)], (gate1_h, w1.at[0]), (up1_h, w1.at[1])),
        (I_RES, res, (res_h, res)),
        (I_GAIN, gains, (gain1_h, gains.at[0]), (gain2_h, gains.at[1]), (gain3_h, gains.at[2])),
        (I_DOWN, w1.at[2], (down1_h, w1.at[2])),
        (I_BD, bd, (wbeta_h, bd.at[0]), (wdecay_h, bd.at[1])),
        (I_QK, mw.at[y, :, 0:512], (wq_h, mw.at[y, :, 0:256]), (wk_h, mw.at[y, :, 256:512])),
        (I_VG, mv.at[y], (wv_h, mv.at[y, :, 0:512]), (wg_h, mv.at[y, :, 512:VGC])),
        (I_WO, wo.at[y], (wo_h, wo.at[y])),
        (I_W2, w2, (gate2_h, w2.at[0]), (up2_h, w2.at[1])),
        (I_D2, d2.at[y], (down2_h, d2.at[y])),
        (I_RB, rb, (rate_h, rb.at[0]), (bias_h, rb.at[1])),
        (I_HEAD, hgain, (hgain_h, hgain)),
        (I_STATE, s_buf, (state, s_buf)),
    )

    def fetch(groups):
        for i, _, *copies in groups:
            for src, dst in copies:
                pltpu.make_async_copy(src, dst, in_sem.at[i]).start()

    def ready(*groups):
        for i in groups:
            whole = inputs[i][1]
            pltpu.make_async_copy(whole, whole, in_sem.at[i]).wait()

    fetch(inputs[:3])

    barrier = pltpu.get_barrier_semaphore()
    greet = z_peers[:3] + plane_peers[:10] + z_peers[3:5] + plane_peers[10:] + z_peers[5:]
    for _, peer in greet:
        pl.semaphore_signal(barrier, inc=1, device_id=peer, device_id_type=MESH)

    counted = []

    def put(src, dst, k, peer, by=TILES):
        if by == TILES:
            counted.append(src.size * src.dtype.itemsize)
        pltpu.make_async_remote_copy(
            src_ref=src, dst_ref=dst, send_sem=send.at[by], recv_sem=recv.at[k], device_id=peer, device_id_type=MESH
        ).start()

    def arrived(part, k):
        pltpu.make_async_copy(part, part, recv.at[k]).wait()

    def left(part, k):
        pltpu.make_async_copy(part, part, send.at[k]).wait()

    def share(buf, own, k, peers, by=TILES):
        for _, peer in peers:
            put(buf.at[own], buf.at[own], k, peer, by)

    def deal(src, dst, own, k, peers):
        for p, peer in peers:
            put(src.at[p], dst.at[own], k, peer)
        dst[own] = src[own]

    above, below = (z * NY + ys[1], t), (z * NY + ys[3], t)

    def y_start(buf, k, by=TILES):
        put(buf.at[y], buf.at[y], k, above, by)
        put(buf.at[y], buf.at[y], k, below, by)

    def halves(buf, p):
        n = buf.shape[1] // 2
        return buf.at[p, pl.ds(0, n)], buf.at[p, pl.ds(n, n)]

    def y_pass(buf, k, by=TILES):
        arrived(buf.at[pl.ds(0, 2)], k)
        first, _ = halves(buf, ys[3])
        put(first, first, k + 1, above, by)
        _, second = halves(buf, ys[1])
        put(second, second, k + 1, below, by)

    def y_done(buf, k):
        arrived(buf.at[0], k + 1)

    lane = iota((64, FFP), 1)
    pos = lane - PITCH * sum(jnp.where(lane >= PITCH * p, 1, 0) for p in range(1, NY))

    def spread(v):
        v = jnp.concatenate([v.astype(F32), jnp.zeros((64, FFP - FFT), F32)], axis=1)
        w = v
        for p in range(1, NY):
            w = jnp.where(lane >= PITCH * p, pltpu.roll(v, (PITCH - HID) * p, 1), w)
        return jnp.where(pos < HID, w, 0.0)

    ready(I_W1)
    gate, up = spread(w1[0]), spread(w1[1])
    first = iota((64, 2 * PITCH), 1) < PITCH
    for h in range(2):
        a = gate[:, 2 * PITCH * h : 2 * PITCH * (h + 1)]
        b = pltpu.roll(up[:, 2 * PITCH * h : 2 * PITCH * (h + 1)], PITCH, 1)
        gu_src[2 * h] = jnp.where(first, a, b).astype(BF)
        gu_src[2 * h + 1] = jnp.where(first, b, a).astype(BF)
    ready(I_RES, I_GAIN)
    xg[me] = res[...]
    gn[y, 0:1] = gains[0]
    gn[y, 1:2] = gains[1]
    gn[y, 2:3] = gains[2]

    pl.semaphore_wait(barrier, len(greet))

    share(gn, y, GN, y_peers, GAINS)
    share(xg, me, X1, plane_peers[:18])
    deal(gu_src, gu_rcv, y, GU1, y_peers)
    share(xg, me, X1, plane_peers[18:])

    fetch(inputs[3:])
    ready(I_DOWN)
    d1[y] = spread(w1[2]).astype(BF)
    sel_b = one_hot((iota((32, 128), 0) == iota((32, 128), 1) + 4 * t) & (iota((32, 128), 1) < 4))
    sel_d = one_hot((iota((32, 128), 0) == iota((32, 128), 1) - 4 + 4 * t) & (iota((32, 128), 1) >= 4) & (iota((32, 128), 1) < 8))
    ready(I_BD)
    mw[y, :, 512:QK] = (dot(bd[0], sel_b, 0, 0) + dot(bd[1], sel_d, 0, 0)).astype(BF)

    eye64 = iota((64, 64), 0) == iota((64, 64), 1)
    lane64 = iota((64, 128), 1)

    def column(p, i):
        row = gn[p, i : i + 1]
        return jnp.sum(jnp.where(eye64, jnp.broadcast_to(row, (64, 64)), 0.0), axis=1, keepdims=True)

    arrived(gn.at[pl.ds(0, NY - 1)], GN)
    for i in range(3):
        for h in range(2):
            wide = jnp.where(lane64 == iota((64, 128), 0), column(2 * h, i), 0.0)
            wide = wide + jnp.where(lane64 == iota((64, 128), 0) + 64, column(2 * h + 1, i), 0.0)
            g_row[i, :, 128 * h : 128 * (h + 1)] = jnp.broadcast_to(jnp.sum(wide, axis=0, keepdims=True), (8, 128))

    def scaled_of(v, i):
        squares = jnp.sum(v * v, axis=1, keepdims=True)
        coarse = squares.astype(BF).astype(F32)
        return (v * g_row[i, 0:1]).astype(BF), coarse, squares - coarse

    arrived(xg.at[pl.ds(0, PLANE - 1)], X1)
    x0 = jnp.transpose(xg[...].astype(F32).reshape(ROWS, ROWS))
    scaled, coarse, fine = scaled_of(x0, 0)
    arrived(gu_rcv.at[pl.ds(0, NY - 1)], GU1)
    part = dot(scaled, gu_rcv[...].reshape(ROWS, 2 * PITCH), 1, 0)
    at = iota((ROWS, 2 * PITCH), 1)
    part = part + jnp.where(at == HID, coarse, 0.0) + jnp.where(at == HID + 1, fine, 0.0)
    f_src[...] = part.reshape(KV, 8, 2 * PITCH).astype(BF)
    deal(f_src, f_rcv, kv, RS1, kv_peers)
    y_start(d1, D1)
    ready(I_QK)
    y_start(mw, MW)
    xrow[...] = x0.reshape(NZ, NY, 8, ROWS).astype(BF)
    y_pass(d1, D1)
    ready(I_VG)
    y_start(mv, MV)
    arrived(f_rcv.at[pl.ds(0, KV - 1)], RS1)
    quarters = jnp.sum(f_rcv[...].astype(F32).reshape(NZ, NY, 8, 2 * PITCH), axis=0)
    scale = lax.rsqrt((quarters[0, :, HID : HID + 1] + quarters[0, :, HID + 1 : HID + 2]) / D + EPS)
    at = iota((8, 2 * PITCH), 1)
    pos = at - PITCH * jnp.where(at >= PITCH, 1, 0)
    for h in range(2):
        a, b = quarters[2 * h], quarters[2 * h + 1]
        gate = jnp.where(at < PITCH, a, b) * scale
        up = pltpu.roll(jnp.where(at < PITCH, b, a), PITCH, 1) * scale
        hg[0, z, :, 2 * PITCH * h : 2 * PITCH * (h + 1)] = jnp.where(pos < HID, silu(gate) * up, 0.0).astype(BF)
    share(hg.at[0], z, AG1, z_peers)
    y_pass(mw, MW)
    y_done(d1, D1)

    def gathered_hidden(i, k):
        arrived(hg.at[i, pl.ds(0, NZ - 1)], k)
        return hg[i].astype(F32).reshape(64, FFP).astype(BF)

    def swap(part, i, k, between):
        pa_src[i] = part.reshape(2, 4, 8, ROWS).astype(BF)
        put(pa_src.at[i, 1 - core], pa_rcv.at[i], k, (kv, ts[0][1]))
        mine = jnp.where(core == 0, part[0:32], part[32:64])
        between()
        arrived(pa_rcv.at[i], k)
        pb[i, t] = (mine.reshape(4, 8, ROWS) + pa_rcv[i].astype(F32)).astype(BF)

    def everyones(i, k):
        arrived(pb.at[i, pl.ds(0, NT - 1)], k)
        branch = []
        for c in range(2):
            half = pb[i, c].astype(F32)
            for j in range(1, 4):
                half = half + pb[i, 2 * j + c].astype(F32)
            branch.append(half.reshape(32, ROWS))
        return jnp.concatenate(branch, axis=0)

    h = gathered_hidden(0, AG1)
    swap(dot(h, d1[...].reshape(ROWS, FFP), 1, 1), 0, PR1, lambda: y_pass(mv, MV))
    share(pb.at[0], t, X2, t_peers)
    y_done(mw, MW)
    x1 = xrow[:, y].astype(F32).reshape(64, ROWS)
    x1 = (x1 + 0.5 * everyones(0, X2)).astype(BF).astype(F32)
    scaled, coarse, fine = scaled_of(x1, 1)
    last = iota((64, 128), 1)
    part = dot(scaled, mw[:, :, 0:512].reshape(ROWS, 512), 1, 0)
    m_src[:, :, 0:512] = part.reshape(NZ, 8, 512).astype(BF)
    part = dot(scaled, mw[:, :, 512:QK].reshape(ROWS, 128), 1, 0)
    part = part + jnp.where(last == 8, coarse, 0.0) + jnp.where(last == 9, fine, 0.0)
    m_src[:, :, 512:QK] = part.reshape(NZ, 8, 128).astype(BF)
    deal(m_src, m_rcv, z, MIX, z_peers)
    y_done(mv, MV)
    part = dot(scaled, mv[...].reshape(ROWS, VGC), 1, 0)
    v_src[...] = part.reshape(NZ, 8, 1024).astype(BF)
    deal(v_src, v_rcv, z, VG, z_peers)
    ready(I_WO, I_W2, I_D2, I_RB, I_HEAD, I_STATE)
    y_start(wo, WO)
    gu2[y] = jnp.concatenate([w2[0].astype(F32), w2[1].astype(F32)], axis=1).astype(BF)
    y_start(gu2, GU2)
    arrived(m_rcv.at[pl.ds(0, NZ - 1)], MIX)

    mixed = jnp.sum(m_rcv[...].astype(F32), axis=0)
    ext = mixed[:, 512:QK]
    rowscale = lax.rsqrt((ext[:, 8:9] + ext[:, 9:10]) / D + EPS)
    heads = [mixed[:, 128 * i : 128 * (i + 1)] * rowscale for i in range(4)]

    def factor(v):
        return lax.rsqrt(jnp.sum(v * v, axis=-1, keepdims=True) + EPS)

    q = [silu(heads[m]) for m in range(2)]
    k = [silu(heads[2 + m]) for m in range(2)]
    q_t = [jnp.transpose(v) for v in q]
    k_t = [jnp.transpose(v) for v in k]
    q_f = [factor(v) * HEAD**-0.5 for v in q]
    k_f = [factor(v) for v in k]
    kq = [jnp.sum(k[m] * q[m], axis=-1, keepdims=True) * k_f[m] * q_f[m] for m in range(2)]
    ext = ext * rowscale
    by_k, by_q = [[] for _ in range(4)], [[] for _ in range(4)]
    for m in range(2):
        for i in range(8):
            k_col = jnp.broadcast_to(k_t[m][:, i : i + 1], (HEAD, HEAD))
            q_col = jnp.broadcast_to(q_t[m][:, i : i + 1], (HEAD, HEAD))
            for h in (2 * m, 2 * m + 1):
                s = s_buf[i, h]
                by_k[h].append(jnp.sum(s * k_col, axis=0, keepdims=True))
                by_q[h].append(jnp.sum(s * q_col, axis=0, keepdims=True))
    gates = []
    for h in range(4):
        beta = 1.0 / (1.0 + jnp.exp(-ext[:, h : h + 1]))
        pre = ext[:, 4 + h : 5 + h] + rb[1, :, h : h + 1]
        soft = jnp.maximum(pre, 0.0) + jnp.log1p(jnp.exp(-jnp.abs(pre)))
        decay = jnp.exp(-jnp.exp(rb[0, :, h : h + 1]) * soft)
        by_k[h] = decay * k_f[h // 2] * jnp.concatenate(by_k[h], axis=0)
        by_q[h] = decay * q_f[h // 2] * jnp.concatenate(by_q[h], axis=0)
        gates.append((beta, decay))
    arrived(v_rcv.at[pl.ds(0, NZ - 1)], VG)
    mixed = jnp.sum(v_rcv[...].astype(F32), axis=0)
    heads = [mixed[:, 128 * i : 128 * (i + 1)] * rowscale for i in range(8)]
    new = []
    for h in range(4):
        m = h // 2
        beta, decay = gates[h]
        val = silu(heads[h])
        gate = silu(heads[4 + h])
        corr = beta * (val - by_k[h])
        reading = by_q[h] + kq[m] * corr
        norm = lax.rsqrt(jnp.mean(reading * reading, axis=-1, keepdims=True) + EPS)
        nb[z, :, 128 * h : 128 * (h + 1)] = (reading * norm * hgain[...] * gate).astype(BF)
        new.append((decay, corr * k_f[m]))
    share(nb, z, NRM, z_peers)
    y_pass(wo, WO)
    y_pass(gu2, GU2)
    y_start(d2, D2, DOWN2)
    for i in range(8):
        for m in range(2):
            k_col = jnp.broadcast_to(k_t[m][:, i : i + 1], (HEAD, HEAD))
            for h in (2 * m, 2 * m + 1):
                decay, corr = new[h]
                state_out[i, h] = s_buf[i, h] * decay[i : i + 1] + k_col * corr[i : i + 1]
    y_done(wo, WO)
    arrived(nb.at[pl.ds(0, NZ - 1)], NRM)
    normed = nb[...].astype(F32).reshape(64, 512).astype(BF)
    part = dot(normed, wo[...].reshape(ROWS, 512), 1, 1)
    swap(part, 1, PR2, lambda: None)
    share(pb.at[1], t, X3, t_peers)
    y_done(gu2, GU2)

    x3 = (x1 + everyones(1, X3)).astype(BF).astype(F32)
    scaled, coarse, fine = scaled_of(x3, 2)
    squares = jnp.where(last == 0, coarse, jnp.where(last == 1, fine, 0.0))
    sq_src[...] = squares.reshape(NZ, 8, 128).astype(BF)
    deal(sq_src, sq_rcv, z, SQ, z_peers)
    part = dot(scaled, gu2[...].reshape(ROWS, 2 * FFT), 1, 0)
    rs2_src[...] = part.reshape(NZ, 8, 2 * FFT).astype(BF)
    deal(rs2_src, rs2_rcv, z, RS2, z_peers)
    y_pass(d2, D2, DOWN2)
    x3_t = jnp.transpose(jnp.concatenate([jnp.zeros((64, ROWS), F32), x3], axis=0))
    arrived(sq_rcv.at[pl.ds(0, NZ - 1)], SQ)
    squares = jnp.sum(sq_rcv[...].astype(F32), axis=0)
    scale = lax.rsqrt((squares[:, 0:1] + squares[:, 1:2]) / D + EPS)
    arrived(rs2_rcv.at[pl.ds(0, NZ - 1)], RS2)
    both = jnp.sum(rs2_rcv[...].astype(F32), axis=0) * scale
    hidden = silu(both[:, 0:FFT]) * both[:, FFT:]
    hg[1, z] = jnp.concatenate([hidden, jnp.zeros((8, FFP - FFT), F32)], axis=1).astype(BF)
    share(hg.at[1], z, AG2, z_peers)
    y_done(d2, D2)
    h = gathered_hidden(1, AG2)[:, 0:FFT]
    h = jnp.concatenate([h, jnp.zeros((64, FFT), BF)], axis=0)
    part = dot(d2[...].reshape(ROWS, FFT), h, 1, 1) + x3_t
    pr3_src[...] = part.reshape(PLANE, 8, 128).astype(BF)
    deal(pr3_src, pr3_rcv, me, PR3, plane_peers)
    arrived(pr3_rcv.at[pl.ds(0, PLANE - 1)], PR3)
    for p in range(NY):
        total = jnp.sum(pr3_rcv[NT * p : NT * (p + 1)].astype(F32), axis=0)
        base = pltpu.roll(pr3_rcv[NT * p].astype(F32), 64, 1)
        out[:, 128 * p : 128 * (p + 1)] = (base + 0.5 * total).astype(BF)
    assert sum(counted) == SENT * 2048, sum(counted) / 2048
    left(tiles, TILES)
    left(gn.at[pl.ds(0, NY - 1)], GAINS)
    left(d2.at[pl.ds(0, NY - 1)], DOWN2)


def deliver(out_in, state_in, out, state_out, placed, sems):
    copies = [pltpu.make_async_copy(state_in, state_out, sems.at[0])]
    copies[0].start()
    line, b = iota((128, ROWS), 0), iota((128, ROWS), 1)
    final = jnp.zeros((8, ROWS), F32)
    for p in range(NY):
        place = one_hot((b == line + 24 * lax.shift_right_logical(line, 3) + 8 * p) & (line < 64))
        final = final + dot(out_in[:, 128 * p : 128 * (p + 1)], place, 1, 0)
    placed[...] = final.astype(BF)
    copies.append(pltpu.make_async_copy(placed, out, sems.at[1]))
    copies[-1].start()
    for copy in copies:
        copy.wait()


def layer(res, state, gain1, gate1, up1, down1, gain2, wq, wk, wv, wg, wbeta, wdecay, rate, bias, hgain, wo, gain3, gate2, up2, down2):
    vmem = pl.BlockSpec(memory_space=pltpu.VMEM)
    args = (
        res.T, state, gain1[None], gain2[None], gain3[None], gate1, up1, down1.T, gate2, up2, down2.T,
        wq, wk, wv, wg, wbeta.T, wdecay.T, rate[None], bias[None], hgain[None], wo.T,
    )
    args = tuple(pltpu.with_memory_space_constraint(a, pltpu.HBM) for a in args)
    hbm = pl.BlockSpec(memory_space=pltpu.HBM)
    shapes = (jax.ShapeDtypeStruct((8, ROWS), BF), jax.ShapeDtypeStruct(state.shape, F32))
    out, new_state = pl.pallas_call(
        kernel,
        out_shape=(pltpu.VMEM((8, NY * 128), BF), pltpu.VMEM(state.shape, F32)),
        in_specs=[hbm] * len(args),
        out_specs=(vmem, vmem),
        scratch_shapes=[
            pltpu.VMEM((8, ROWS), BF),
            pltpu.VMEM(state.shape, F32),
            pltpu.VMEM((3, 1, 64), F32),
            pltpu.VMEM((3, 64, FFT), BF),
            pltpu.VMEM((2, 64, FFT), BF),
            pltpu.VMEM((2, 32, 64), BF),
            pltpu.VMEM((2, 1, 4), F32),
            pltpu.VMEM((1, HEAD), F32),
            pltpu.SemaphoreType.DMA((13,)),
            pltpu.SemaphoreType.DMA((3,)),
            pltpu.SemaphoreType.DMA((28,)),
            pltpu.VMEM((SENT, 8, 128), BF),
            pltpu.VMEM((NY, 64, 2 * PITCH), BF),
            pltpu.VMEM((NY, 64, 2 * PITCH), BF),
            pltpu.VMEM((NY, 8, 64), F32),
            pltpu.VMEM((NY, 64, FFP), BF),
            pltpu.VMEM((NY, 64, QK), BF),
            pltpu.VMEM((NY, 64, VGC), BF),
            pltpu.VMEM((NY, 64, 512), BF),
            pltpu.VMEM((NY, 64, 2 * FFT), BF),
            pltpu.VMEM((NY, 64, FFT), BF),
            pltpu.VMEM((3, 8, ROWS), F32),
            pltpu.VMEM((NZ, NY, 8, ROWS), BF),
            pltpu.VMEM((PLANE, 8, ROWS), BF),
            pltpu.VMEM((KV, 8, 2 * PITCH), BF),
            pltpu.VMEM((KV, 8, 2 * PITCH), BF),
            pltpu.VMEM((2, NZ, 8, FFP), BF),
            pltpu.VMEM((2, 2, 4, 8, ROWS), BF),
            pltpu.VMEM((2, 4, 8, ROWS), BF),
            pltpu.VMEM((2, NT, 4, 8, ROWS), BF),
            pltpu.VMEM((NZ, 8, QK), BF),
            pltpu.VMEM((NZ, 8, QK), BF),
            pltpu.VMEM((NZ, 8, 1024), BF),
            pltpu.VMEM((NZ, 8, 1024), BF),
            pltpu.VMEM((NZ, 8, 512), BF),
            pltpu.VMEM((NZ, 8, 128), BF),
            pltpu.VMEM((NZ, 8, 128), BF),
            pltpu.VMEM((NZ, 8, 2 * FFT), BF),
            pltpu.VMEM((NZ, 8, 2 * FFT), BF),
            pltpu.VMEM((PLANE, 8, 128), BF),
            pltpu.VMEM((PLANE, 8, 128), BF),
        ],
        compiler_params=pltpu.CompilerParams(collective_id=0, has_side_effects=True, vmem_limit_bytes=40 << 20),
    )(*args)
    out, new_state = pl.pallas_call(
        deliver,
        out_shape=shapes,
        in_specs=[vmem, vmem],
        out_specs=(hbm, hbm),
        scratch_shapes=[pltpu.VMEM((8, ROWS), BF), pltpu.SemaphoreType.DMA((2,))],
        compiler_params=pltpu.CompilerParams(vmem_limit_bytes=40 << 20),
    )(out, new_state)
    return out.T, new_state


def solution(mesh):
    placed = (
        P(None, ("kv", "tp")),
        P("kv", "tp", None, None),
        P("kv"),
        P("kv", "tp"),
        P("kv", "tp"),
        P("tp", "kv"),
        P("kv"),
        P("kv", "tp"),
        P("kv", "tp"),
        P("kv", "tp"),
        P("kv", "tp"),
        P("kv", None),
        P("kv", None),
        P("tp"),
        P("tp"),
        P(),
        P("tp", "kv"),
        P("kv"),
        P("kv", "tp"),
        P("kv", "tp"),
        P("tp", "kv"),
    )
    return jax.shard_map(
        layer,
        mesh=mesh,
        in_specs=placed,
        out_specs=(P(None, ("kv", "tp")), P("kv", "tp", None, None)),
        check_vma=False,
    )
```

```python
import jax
import jax.numpy as jnp
from jax import lax
from jax.experimental import pallas as pl
from jax.experimental.pallas import tpu as pltpu
from jax.sharding import PartitionSpec as P

MESH = pl.DeviceIdType.MESH
BF, F32 = jnp.bfloat16, jnp.float32
D, EPS = 2048, 1e-6
NZ, NY, NT = 8, 4, 8
PLANE = NY * NT
KV = NZ * NY
ROWS = 256
HID, PITCH = 176, 192
HEAD = 128

X1, X2, X3, RS1, RS2, AG1, AG2, PR1, PR2, PR3, MIX, VG, NRM, GU1, GN, SQ = range(16)
D1, MW, WO, GU2, D2, MV = range(16, 28, 2)
TILES, GAINS, DOWN2 = range(3)
I_W1, I_RES, I_GAIN, I_DOWN, I_BD, I_QK, I_VG, I_WO, I_W2, I_D2, I_RB, I_HEAD, I_STATE = range(13)
QK, VGC = 640, 1024
FFT, FFP = 704, 768
SENT = 31 * 2 + 3 * 24 + 31 * 3 + 14 * 6 + 2 * 8 + 14 * 8 + 7 * (5 + 8 + 4 + 1 + 11) + 31 + 3 * 8 * (6 + 5 + 8 + 4 + 11)
RING_Z = (4, 3, 5, 2, 6, 1, 7)
FAR, FAR_Z = (0, 1, 2, 1), (0, 1, 2, 3, 4, 3, 2, 1)


def dot(a, b, ca, cb):
    return lax.dot_general(a, b, (((ca,), (cb,)), ((), ())), preferred_element_type=F32)


def iota(shape, dim):
    return lax.broadcasted_iota(jnp.int32, shape, dim)


def one_hot(cond):
    return jnp.where(cond, 1.0, 0.0).astype(BF)


def silu(v):
    return v / (1.0 + jnp.exp(-v))


def kernel(
    res_h, state, gain1_h, gain2_h, gain3_h, gate1_h, up1_h, down1_h, gate2_h, up2_h, down2_h,
    wq_h, wk_h, wv_h, wg_h, wbeta_h, wdecay_h, rate_h, bias_h, hgain_h, wo_h,
    out, state_out,
    res, s_buf, gains, w1, w2, bd, rb, hgain,
    in_sem, send, recv, tiles,
    gu_src, gu_rcv, gn, d1, mw, mv, wo, gu2, d2,
    g_row, xrow, xg, f_src, f_rcv, hg, pa_src, pa_rcv, pb,
    m_src, m_rcv, v_src, v_rcv, nb, sq_src, sq_rcv, rs2_src, rs2_rcv, pr3_src, pr3_rcv,
):
    kv = lax.axis_index("kv")
    t = lax.axis_index("tp")
    z, y = lax.div(kv, NY), lax.rem(kv, NY)
    x, core = lax.div(t, 2), lax.rem(t, 2)
    me = y * NT + t
    zs = [lax.rem(z + o, NZ) for o in range(NZ)]
    ys = [lax.rem(y + o, NY) for o in range(NY)]
    ts = [[lax.rem(x + o, 4) * 2 + c for c in (core, 1 - core)] for o in range(4)]

    z_peers = [(zs[o], (zs[o] * NY + y, t)) for o in RING_Z]
    y_peers = [(ys[o], (z * NY + ys[o], t)) for o in (2, 1, 3)]
    t_peers = [(ts[dx][dc], (kv, ts[dx][dc])) for dx in (2, 1, 3, 0) for dc in (0, 1) if dx or dc]
    kv_peers = [(dz, dy) for dz in range(NZ) for dy in range(NY) if dz or dy]
    kv_peers.sort(key=lambda o: -(FAR_Z[o[0]] + FAR[o[1]]))
    kv_peers = [(zs[dz] * NY + ys[dy], (zs[dz] * NY + ys[dy], t)) for dz, dy in kv_peers]
    plane = [(dy, dx, dc) for dy in range(4) for dx in range(4) for dc in range(2) if dy or dx or dc]
    plane.sort(key=lambda o: -(FAR[o[0]] + FAR[o[1]]))
    plane_peers = [(ys[dy] * NT + ts[dx][dc], (z * NY + ys[dy], ts[dx][dc])) for dy, dx, dc in plane]

    inputs = (
        (I_W1, w1.at[pl.ds(0, 2)], (gate1_h, w1.at[0]), (up1_h, w1.at[1])),
        (I_RES, res, (res_h, res)),
        (I_GAIN, gains, (gain1_h, gains.at[0]), (gain2_h, gains.at[1]), (gain3_h, gains.at[2])),
        (I_DOWN, w1.at[2], (down1_h, w1.at[2])),
        (I_BD, bd, (wbeta_h, bd.at[0]), (wdecay_h, bd.at[1])),
        (I_QK, mw.at[y, :, 0:512], (wq_h, mw.at[y, :, 0:256]), (wk_h, mw.at[y, :, 256:512])),
        (I_VG, mv.at[y], (wv_h, mv.at[y, :, 0:512]), (wg_h, mv.at[y, :, 512:VGC])),
        (I_WO, wo.at[y], (wo_h, wo.at[y])),
        (I_W2, w2, (gate2_h, w2.at[0]), (up2_h, w2.at[1])),
        (I_D2, d2.at[y], (down2_h, d2.at[y])),
        (I_RB, rb, (rate_h, rb.at[0]), (bias_h, rb.at[1])),
        (I_HEAD, hgain, (hgain_h, hgain)),
        (I_STATE, s_buf, (state, s_buf)),
    )

    def fetch(groups):
        for i, _, *copies in groups:
            for src, dst in copies:
                pltpu.make_async_copy(src, dst, in_sem.at[i]).start()

    def ready(*groups):
        for i in groups:
            whole = inputs[i][1]
            pltpu.make_async_copy(whole, whole, in_sem.at[i]).wait()

    fetch(inputs[:3])

    barrier = pltpu.get_barrier_semaphore()
    greet = z_peers[:3] + plane_peers[:10] + z_peers[3:5] + plane_peers[10:] + z_peers[5:]
    for _, peer in greet:
        pl.semaphore_signal(barrier, inc=1, device_id=peer, device_id_type=MESH)

    counted = []

    def put(src, dst, k, peer, by=TILES):
        if by == TILES:
            counted.append(src.size * src.dtype.itemsize)
        pltpu.make_async_remote_copy(
            src_ref=src, dst_ref=dst, send_sem=send.at[by], recv_sem=recv.at[k], device_id=peer, device_id_type=MESH
        ).start()

    def arrived(part, k):
        pltpu.make_async_copy(part, part, recv.at[k]).wait()

    def left(part, k):
        pltpu.make_async_copy(part, part, send.at[k]).wait()

    def share(buf, own, k, peers, by=TILES):
        for _, peer in peers:
            put(buf.at[own], buf.at[own], k, peer, by)

    def deal(src, dst, own, k, peers):
        for p, peer in peers:
            put(src.at[p], dst.at[own], k, peer)
        dst[own] = src[own]

    above, below = (z * NY + ys[1], t), (z * NY + ys[3], t)

    def y_start(buf, k, by=TILES):
        put(buf.at[y], buf.at[y], k, above, by)
        put(buf.at[y], buf.at[y], k, below, by)

    def halves(buf, p):
        n = buf.shape[1] // 2
        return buf.at[p, pl.ds(0, n)], buf.at[p, pl.ds(n, n)]

    def y_pass(buf, k, by=TILES):
        arrived(buf.at[pl.ds(0, 2)], k)
        first, _ = halves(buf, ys[3])
        put(first, first, k + 1, above, by)
        _, second = halves(buf, ys[1])
        put(second, second, k + 1, below, by)

    def y_done(buf, k):
        arrived(buf.at[0], k + 1)

    lane = iota((64, FFP), 1)
    pos = lane - PITCH * sum(jnp.where(lane >= PITCH * p, 1, 0) for p in range(1, NY))

    def spread(v):
        v = jnp.concatenate([v.astype(F32), jnp.zeros((64, FFP - FFT), F32)], axis=1)
        w = v
        for p in range(1, NY):
            w = jnp.where(lane >= PITCH * p, pltpu.roll(v, (PITCH - HID) * p, 1), w)
        return jnp.where(pos < HID, w, 0.0)

    ready(I_W1)
    gate, up = spread(w1[0]), spread(w1[1])
    first = iota((64, 2 * PITCH), 1) < PITCH
    for h in range(2):
        a = gate[:, 2 * PITCH * h : 2 * PITCH * (h + 1)]
        b = pltpu.roll(up[:, 2 * PITCH * h : 2 * PITCH * (h + 1)], PITCH, 1)
        gu_src[2 * h] = jnp.where(first, a, b).astype(BF)
        gu_src[2 * h + 1] = jnp.where(first, b, a).astype(BF)
    ready(I_RES, I_GAIN)
    xg[me] = res[...]
    gn[y, 0:1] = gains[0]
    gn[y, 1:2] = gains[1]
    gn[y, 2:3] = gains[2]

    pl.semaphore_wait(barrier, len(greet))

    share(gn, y, GN, y_peers, GAINS)
    share(xg, me, X1, plane_peers)
    deal(gu_src, gu_rcv, y, GU1, y_peers)

    fetch(inputs[3:])
    ready(I_DOWN)
    d1[y] = spread(w1[2]).astype(BF)
    sel_b = one_hot((iota((32, 128), 0) == iota((32, 128), 1) + 4 * t) & (iota((32, 128), 1) < 4))
    sel_d = one_hot((iota((32, 128), 0) == iota((32, 128), 1) - 4 + 4 * t) & (iota((32, 128), 1) >= 4) & (iota((32, 128), 1) < 8))
    ready(I_BD)
    mw[y, :, 512:QK] = (dot(bd[0], sel_b, 0, 0) + dot(bd[1], sel_d, 0, 0)).astype(BF)

    eye64 = iota((64, 64), 0) == iota((64, 64), 1)
    lane64 = iota((64, 128), 1)

    def column(p, i):
        row = gn[p, i : i + 1]
        return jnp.sum(jnp.where(eye64, jnp.broadcast_to(row, (64, 64)), 0.0), axis=1, keepdims=True)

    arrived(gn.at[pl.ds(0, NY - 1)], GN)
    for i in range(3):
        for h in range(2):
            wide = jnp.where(lane64 == iota((64, 128), 0), column(2 * h, i), 0.0)
            wide = wide + jnp.where(lane64 == iota((64, 128), 0) + 64, column(2 * h + 1, i), 0.0)
            g_row[i, :, 128 * h : 128 * (h + 1)] = jnp.broadcast_to(jnp.sum(wide, axis=0, keepdims=True), (8, 128))

    def scaled_of(v, i):
        squares = jnp.sum(v * v, axis=1, keepdims=True)
        coarse = squares.astype(BF).astype(F32)
        return (v * g_row[i, 0:1]).astype(BF), coarse, squares - coarse

    arrived(xg.at[pl.ds(0, PLANE - 1)], X1)
    x0 = jnp.transpose(xg[...].astype(F32).reshape(ROWS, ROWS))
    scaled, coarse, fine = scaled_of(x0, 0)
    arrived(gu_rcv.at[pl.ds(0, NY - 1)], GU1)
    part = dot(scaled, gu_rcv[...].reshape(ROWS, 2 * PITCH), 1, 0)
    at = iota((ROWS, 2 * PITCH), 1)
    part = part + jnp.where(at == HID, coarse, 0.0) + jnp.where(at == HID + 1, fine, 0.0)
    f_src[...] = part.reshape(KV, 8, 2 * PITCH).astype(BF)
    deal(f_src, f_rcv, kv, RS1, kv_peers)
    y_start(d1, D1)
    ready(I_QK)
    y_start(mw, MW)
    xrow[...] = x0.reshape(NZ, NY, 8, ROWS).astype(BF)
    y_pass(d1, D1)
    ready(I_VG)
    y_start(mv, MV)
    arrived(f_rcv.at[pl.ds(0, KV - 1)], RS1)
    quarters = jnp.sum(f_rcv[...].astype(F32).reshape(NZ, NY, 8, 2 * PITCH), axis=0)
    scale = lax.rsqrt((quarters[0, :, HID : HID + 1] + quarters[0, :, HID + 1 : HID + 2]) / D + EPS)
    at = iota((8, 2 * PITCH), 1)
    pos = at - PITCH * jnp.where(at >= PITCH, 1, 0)
    for h in range(2):
        a, b = quarters[2 * h], quarters[2 * h + 1]
        gate = jnp.where(at < PITCH, a, b) * scale
        up = pltpu.roll(jnp.where(at < PITCH, b, a), PITCH, 1) * scale
        hg[0, z, :, 2 * PITCH * h : 2 * PITCH * (h + 1)] = jnp.where(pos < HID, silu(gate) * up, 0.0).astype(BF)
    share(hg.at[0], z, AG1, z_peers)
    y_pass(mw, MW)
    y_done(d1, D1)

    def gathered_hidden(i, k):
        arrived(hg.at[i, pl.ds(0, NZ - 1)], k)
        return hg[i].astype(F32).reshape(64, FFP).astype(BF)

    def swap(part, i, k, between):
        pa_src[i] = part.reshape(2, 4, 8, ROWS).astype(BF)
        put(pa_src.at[i, 1 - core], pa_rcv.at[i], k, (kv, ts[0][1]))
        mine = jnp.where(core == 0, part[0:32], part[32:64])
        between()
        arrived(pa_rcv.at[i], k)
        pb[i, t] = (mine.reshape(4, 8, ROWS) + pa_rcv[i].astype(F32)).astype(BF)

    def everyones(i, k):
        arrived(pb.at[i, pl.ds(0, NT - 1)], k)
        branch = []
        for c in range(2):
            half = pb[i, c].astype(F32)
            for j in range(1, 4):
                half = half + pb[i, 2 * j + c].astype(F32)
            branch.append(half.reshape(32, ROWS))
        return jnp.concatenate(branch, axis=0)

    h = gathered_hidden(0, AG1)
    swap(dot(h, d1[...].reshape(ROWS, FFP), 1, 1), 0, PR1, lambda: y_pass(mv, MV))
    share(pb.at[0], t, X2, t_peers)
    y_done(mw, MW)
    x1 = xrow[:, y].astype(F32).reshape(64, ROWS)
    x1 = (x1 + 0.5 * everyones(0, X2)).astype(BF).astype(F32)
    scaled, coarse, fine = scaled_of(x1, 1)
    last = iota((64, 128), 1)
    part = dot(scaled, mw[:, :, 0:512].reshape(ROWS, 512), 1, 0)
    m_src[:, :, 0:512] = part.reshape(NZ, 8, 512).astype(BF)
    part = dot(scaled, mw[:, :, 512:QK].reshape(ROWS, 128), 1, 0)
    part = part + jnp.where(last == 8, coarse, 0.0) + jnp.where(last == 9, fine, 0.0)
    m_src[:, :, 512:QK] = part.reshape(NZ, 8, 128).astype(BF)
    deal(m_src, m_rcv, z, MIX, z_peers)
    y_done(mv, MV)
    part = dot(scaled, mv[...].reshape(ROWS, VGC), 1, 0)
    v_src[...] = part.reshape(NZ, 8, 1024).astype(BF)
    deal(v_src, v_rcv, z, VG, z_peers)
    ready(I_WO, I_W2, I_D2, I_RB, I_HEAD, I_STATE)
    y_start(wo, WO)
    gu2[y] = jnp.concatenate([w2[0].astype(F32), w2[1].astype(F32)], axis=1).astype(BF)
    y_start(gu2, GU2)
    arrived(m_rcv.at[pl.ds(0, NZ - 1)], MIX)

    mixed = jnp.sum(m_rcv[...].astype(F32), axis=0)
    ext = mixed[:, 512:QK]
    rowscale = lax.rsqrt((ext[:, 8:9] + ext[:, 9:10]) / D + EPS)
    heads = [mixed[:, 128 * i : 128 * (i + 1)] * rowscale for i in range(4)]

    def factor(v):
        return lax.rsqrt(jnp.sum(v * v, axis=-1, keepdims=True) + EPS)

    q = [silu(heads[m]) for m in range(2)]
    k = [silu(heads[2 + m]) for m in range(2)]
    q_t = [jnp.transpose(v) for v in q]
    k_t = [jnp.transpose(v) for v in k]
    q_f = [factor(v) * HEAD**-0.5 for v in q]
    k_f = [factor(v) for v in k]
    kq = [jnp.sum(k[m] * q[m], axis=-1, keepdims=True) * k_f[m] * q_f[m] for m in range(2)]
    ext = ext * rowscale
    by_k, by_q = [[] for _ in range(4)], [[] for _ in range(4)]
    for m in range(2):
        for i in range(8):
            k_col = jnp.broadcast_to(k_t[m][:, i : i + 1], (HEAD, HEAD))
            q_col = jnp.broadcast_to(q_t[m][:, i : i + 1], (HEAD, HEAD))
            for h in (2 * m, 2 * m + 1):
                s = s_buf[i, h]
                by_k[h].append(jnp.sum(s * k_col, axis=0, keepdims=True))
                by_q[h].append(jnp.sum(s * q_col, axis=0, keepdims=True))
    gates = []
    for h in range(4):
        beta = 1.0 / (1.0 + jnp.exp(-ext[:, h : h + 1]))
        pre = ext[:, 4 + h : 5 + h] + rb[1, :, h : h + 1]
        soft = jnp.maximum(pre, 0.0) + jnp.log1p(jnp.exp(-jnp.abs(pre)))
        decay = jnp.exp(-jnp.exp(rb[0, :, h : h + 1]) * soft)
        by_k[h] = decay * k_f[h // 2] * jnp.concatenate(by_k[h], axis=0)
        by_q[h] = decay * q_f[h // 2] * jnp.concatenate(by_q[h], axis=0)
        gates.append((beta, decay))
    arrived(v_rcv.at[pl.ds(0, NZ - 1)], VG)
    mixed = jnp.sum(v_rcv[...].astype(F32), axis=0)
    heads = [mixed[:, 128 * i : 128 * (i + 1)] * rowscale for i in range(8)]
    new = []
    for h in range(4):
        m = h // 2
        beta, decay = gates[h]
        val = silu(heads[h])
        gate = silu(heads[4 + h])
        corr = beta * (val - by_k[h])
        reading = by_q[h] + kq[m] * corr
        norm = lax.rsqrt(jnp.mean(reading * reading, axis=-1, keepdims=True) + EPS)
        nb[z, :, 128 * h : 128 * (h + 1)] = (reading * norm * hgain[...] * gate).astype(BF)
        new.append((decay, corr * k_f[m]))
    share(nb, z, NRM, z_peers)
    y_pass(wo, WO)
    y_pass(gu2, GU2)
    y_start(d2, D2, DOWN2)
    for i in range(8):
        for m in range(2):
            k_col = jnp.broadcast_to(k_t[m][:, i : i + 1], (HEAD, HEAD))
            for h in (2 * m, 2 * m + 1):
                decay, corr = new[h]
                state_out[i, h] = s_buf[i, h] * decay[i : i + 1] + k_col * corr[i : i + 1]
    y_done(wo, WO)
    arrived(nb.at[pl.ds(0, NZ - 1)], NRM)
    normed = nb[...].astype(F32).reshape(64, 512).astype(BF)
    part = dot(normed, wo[...].reshape(ROWS, 512), 1, 1)
    swap(part, 1, PR2, lambda: None)
    share(pb.at[1], t, X3, t_peers)
    y_done(gu2, GU2)

    x3 = (x1 + everyones(1, X3)).astype(BF).astype(F32)
    scaled, coarse, fine = scaled_of(x3, 2)
    squares = jnp.where(last == 0, coarse, jnp.where(last == 1, fine, 0.0))
    sq_src[...] = squares.reshape(NZ, 8, 128).astype(BF)
    deal(sq_src, sq_rcv, z, SQ, z_peers)
    part = dot(scaled, gu2[...].reshape(ROWS, 2 * FFT), 1, 0)
    rs2_src[...] = part.reshape(NZ, 8, 2 * FFT).astype(BF)
    deal(rs2_src, rs2_rcv, z, RS2, z_peers)
    y_pass(d2, D2, DOWN2)
    x3_t = jnp.transpose(jnp.concatenate([jnp.zeros((64, ROWS), F32), x3], axis=0))
    arrived(sq_rcv.at[pl.ds(0, NZ - 1)], SQ)
    squares = jnp.sum(sq_rcv[...].astype(F32), axis=0)
    scale = lax.rsqrt((squares[:, 0:1] + squares[:, 1:2]) / D + EPS)
    arrived(rs2_rcv.at[pl.ds(0, NZ - 1)], RS2)
    both = jnp.sum(rs2_rcv[...].astype(F32), axis=0) * scale
    hidden = silu(both[:, 0:FFT]) * both[:, FFT:]
    hg[1, z] = jnp.concatenate([hidden, jnp.zeros((8, FFP - FFT), F32)], axis=1).astype(BF)
    share(hg.at[1], z, AG2, z_peers)
    y_done(d2, D2)
    h = gathered_hidden(1, AG2)[:, 0:FFT]
    h = jnp.concatenate([h, jnp.zeros((64, FFT), BF)], axis=0)
    part = dot(d2[...].reshape(ROWS, FFT), h, 1, 1) + x3_t
    pr3_src[...] = part.reshape(PLANE, 8, 128).astype(BF)
    deal(pr3_src, pr3_rcv, me, PR3, plane_peers)
    arrived(pr3_rcv.at[pl.ds(0, PLANE - 1)], PR3)
    for p in range(NY):
        total = jnp.sum(pr3_rcv[NT * p : NT * (p + 1)].astype(F32), axis=0)
        base = pltpu.roll(pr3_rcv[NT * p].astype(F32), 64, 1)
        out[:, 128 * p : 128 * (p + 1)] = (base + 0.5 * total).astype(BF)
    assert sum(counted) == SENT * 2048, sum(counted) / 2048
    left(tiles, TILES)
    left(gn.at[pl.ds(0, NY - 1)], GAINS)
    left(d2.at[pl.ds(0, NY - 1)], DOWN2)


def deliver(out_in, state_in, out, state_out, placed, sems):
    copies = [pltpu.make_async_copy(state_in, state_out, sems.at[0])]
    copies[0].start()
    line, b = iota((128, ROWS), 0), iota((128, ROWS), 1)
    final = jnp.zeros((8, ROWS), F32)
    for p in range(NY):
        place = one_hot((b == line + 24 * lax.shift_right_logical(line, 3) + 8 * p) & (line < 64))
        final = final + dot(out_in[:, 128 * p : 128 * (p + 1)], place, 1, 0)
    placed[...] = final.astype(BF)
    copies.append(pltpu.make_async_copy(placed, out, sems.at[1]))
    copies[-1].start()
    for copy in copies:
        copy.wait()


def layer(res, state, gain1, gate1, up1, down1, gain2, wq, wk, wv, wg, wbeta, wdecay, rate, bias, hgain, wo, gain3, gate2, up2, down2):
    vmem = pl.BlockSpec(memory_space=pltpu.VMEM)
    args = (
        res.T, state, gain1[None], gain2[None], gain3[None], gate1, up1, down1.T, gate2, up2, down2.T,
        wq, wk, wv, wg, wbeta.T, wdecay.T, rate[None], bias[None], hgain[None], wo.T,
    )
    args = tuple(pltpu.with_memory_space_constraint(a, pltpu.HBM) for a in args)
    hbm = pl.BlockSpec(memory_space=pltpu.HBM)
    shapes = (jax.ShapeDtypeStruct((8, ROWS), BF), jax.ShapeDtypeStruct(state.shape, F32))
    out, new_state = pl.pallas_call(
        kernel,
        out_shape=(pltpu.VMEM((8, NY * 128), BF), pltpu.VMEM(state.shape, F32)),
        in_specs=[hbm] * len(args),
        out_specs=(vmem, vmem),
        scratch_shapes=[
            pltpu.VMEM((8, ROWS), BF),
            pltpu.VMEM(state.shape, F32),
            pltpu.VMEM((3, 1, 64), F32),
            pltpu.VMEM((3, 64, FFT), BF),
            pltpu.VMEM((2, 64, FFT), BF),
            pltpu.VMEM((2, 32, 64), BF),
            pltpu.VMEM((2, 1, 4), F32),
            pltpu.VMEM((1, HEAD), F32),
            pltpu.SemaphoreType.DMA((13,)),
            pltpu.SemaphoreType.DMA((3,)),
            pltpu.SemaphoreType.DMA((28,)),
            pltpu.VMEM((SENT, 8, 128), BF),
            pltpu.VMEM((NY, 64, 2 * PITCH), BF),
            pltpu.VMEM((NY, 64, 2 * PITCH), BF),
            pltpu.VMEM((NY, 8, 64), F32),
            pltpu.VMEM((NY, 64, FFP), BF),
            pltpu.VMEM((NY, 64, QK), BF),
            pltpu.VMEM((NY, 64, VGC), BF),
            pltpu.VMEM((NY, 64, 512), BF),
            pltpu.VMEM((NY, 64, 2 * FFT), BF),
            pltpu.VMEM((NY, 64, FFT), BF),
            pltpu.VMEM((3, 8, ROWS), F32),
            pltpu.VMEM((NZ, NY, 8, ROWS), BF),
            pltpu.VMEM((PLANE, 8, ROWS), BF),
            pltpu.VMEM((KV, 8, 2 * PITCH), BF),
            pltpu.VMEM((KV, 8, 2 * PITCH), BF),
            pltpu.VMEM((2, NZ, 8, FFP), BF),
            pltpu.VMEM((2, 2, 4, 8, ROWS), BF),
            pltpu.VMEM((2, 4, 8, ROWS), BF),
            pltpu.VMEM((2, NT, 4, 8, ROWS), BF),
            pltpu.VMEM((NZ, 8, QK), BF),
            pltpu.VMEM((NZ, 8, QK), BF),
            pltpu.VMEM((NZ, 8, 1024), BF),
            pltpu.VMEM((NZ, 8, 1024), BF),
            pltpu.VMEM((NZ, 8, 512), BF),
            pltpu.VMEM((NZ, 8, 128), BF),
            pltpu.VMEM((NZ, 8, 128), BF),
            pltpu.VMEM((NZ, 8, 2 * FFT), BF),
            pltpu.VMEM((NZ, 8, 2 * FFT), BF),
            pltpu.VMEM((PLANE, 8, 128), BF),
            pltpu.VMEM((PLANE, 8, 128), BF),
        ],
        compiler_params=pltpu.CompilerParams(collective_id=0, has_side_effects=True, vmem_limit_bytes=40 << 20),
    )(*args)
    out, new_state = pl.pallas_call(
        deliver,
        out_shape=shapes,
        in_specs=[vmem, vmem],
        out_specs=(hbm, hbm),
        scratch_shapes=[pltpu.VMEM((8, ROWS), BF), pltpu.SemaphoreType.DMA((2,))],
        compiler_params=pltpu.CompilerParams(vmem_limit_bytes=40 << 20),
    )(out, new_state)
    return out.T, new_state


def solution(mesh):
    placed = (
        P(None, ("kv", "tp")),
        P("kv", "tp", None, None),
        P("kv"),
        P("kv", "tp"),
        P("kv", "tp"),
        P("tp", "kv"),
        P("kv"),
        P("kv", "tp"),
        P("kv", "tp"),
        P("kv", "tp"),
        P("kv", "tp"),
        P("kv", None),
        P("kv", None),
        P("tp"),
        P("tp"),
        P(),
        P("tp", "kv"),
        P("kv"),
        P("kv", "tp"),
        P("kv", "tp"),
        P("tp", "kv"),
    )
    return jax.shard_map(
        layer,
        mesh=mesh,
        in_specs=placed,
        out_specs=(P(None, ("kv", "tp")), P("kv", "tp", None, None)),
        check_vma=False,
    )
```

```python
import jax
import jax.numpy as jnp
from jax import lax
from jax.experimental import pallas as pl
from jax.experimental.pallas import tpu as pltpu
from jax.sharding import PartitionSpec as P

MESH = pl.DeviceIdType.MESH
BF, F32 = jnp.bfloat16, jnp.float32
D, EPS = 2048, 1e-6
NZ, NY, NT = 8, 4, 8
PLANE = NY * NT
KV = NZ * NY
ROWS = 256
HID, PITCH = 176, 192
HEAD = 128

X1, X2, X3, RS1, RS2, AG1, AG2, PR1, PR2, PR3, MIX, VG, NRM, GU1, GN, SQ, EXT = range(17)
D1, MW, WO, GU2, D2, MV = range(17, 29, 2)
TILES, GAINS, DOWN2 = range(3)
I_W1, I_RES, I_GAIN, I_DOWN, I_BD, I_QK, I_VG, I_WO, I_W2, I_D2, I_RB, I_HEAD, I_STATE = range(13)
QK, VGC = 640, 1024
FFT, FFP = 704, 768
SENT = 31 * 2 + 3 * 24 + 31 * 3 + 14 * 6 + 2 * 8 + 14 * 8 + 7 * (5 + 8 + 4 + 1 + 11) + 31 + 3 * 8 * (6 + 5 + 8 + 4 + 11)
RING_Z = (4, 3, 5, 2, 6, 1, 7)
FAR, FAR_Z = (0, 1, 2, 1), (0, 1, 2, 3, 4, 3, 2, 1)


def dot(a, b, ca, cb):
    return lax.dot_general(a, b, (((ca,), (cb,)), ((), ())), preferred_element_type=F32)


def iota(shape, dim):
    return lax.broadcasted_iota(jnp.int32, shape, dim)


def one_hot(cond):
    return jnp.where(cond, 1.0, 0.0).astype(BF)


def silu(v):
    return v / (1.0 + jnp.exp(-v))


def kernel(
    res_h, state, gain1_h, gain2_h, gain3_h, gate1_h, up1_h, down1_h, gate2_h, up2_h, down2_h,
    wq_h, wk_h, wv_h, wg_h, wbeta_h, wdecay_h, rate_h, bias_h, hgain_h, wo_h,
    out, state_out,
    res, s_buf, gains, w1, w2, bd, rb, hgain,
    in_sem, send, recv, tiles,
    gu_src, gu_rcv, gn, d1, mw, mv, wo, gu2, d2,
    g_row, xrow, xg, f_src, f_rcv, hg, pa_src, pa_rcv, pb,
    m_src, m_rcv, e_src, e_rcv, v_src, v_rcv, nb, sq_src, sq_rcv, rs2_src, rs2_rcv, pr3_src, pr3_rcv,
):
    kv = lax.axis_index("kv")
    t = lax.axis_index("tp")
    z, y = lax.div(kv, NY), lax.rem(kv, NY)
    x, core = lax.div(t, 2), lax.rem(t, 2)
    me = y * NT + t
    zs = [lax.rem(z + o, NZ) for o in range(NZ)]
    ys = [lax.rem(y + o, NY) for o in range(NY)]
    ts = [[lax.rem(x + o, 4) * 2 + c for c in (core, 1 - core)] for o in range(4)]

    z_peers = [(zs[o], (zs[o] * NY + y, t)) for o in RING_Z]
    y_peers = [(ys[o], (z * NY + ys[o], t)) for o in (2, 1, 3)]
    t_peers = [(ts[dx][dc], (kv, ts[dx][dc])) for dx in (2, 1, 3, 0) for dc in (0, 1) if dx or dc]
    kv_peers = [(dz, dy) for dz in range(NZ) for dy in range(NY) if dz or dy]
    kv_peers.sort(key=lambda o: -(FAR_Z[o[0]] + FAR[o[1]]))
    kv_peers = [(zs[dz] * NY + ys[dy], (zs[dz] * NY + ys[dy], t)) for dz, dy in kv_peers]
    plane = [(dy, dx, dc) for dy in range(4) for dx in range(4) for dc in range(2) if dy or dx or dc]
    plane.sort(key=lambda o: -(FAR[o[0]] + FAR[o[1]]))
    plane_peers = [(ys[dy] * NT + ts[dx][dc], (z * NY + ys[dy], ts[dx][dc])) for dy, dx, dc in plane]

    inputs = (
        (I_W1, w1.at[pl.ds(0, 2)], (gate1_h, w1.at[0]), (up1_h, w1.at[1])),
        (I_RES, res, (res_h, res)),
        (I_GAIN, gains, (gain1_h, gains.at[0]), (gain2_h, gains.at[1]), (gain3_h, gains.at[2])),
        (I_DOWN, w1.at[2], (down1_h, w1.at[2])),
        (I_BD, bd, (wbeta_h, bd.at[0]), (wdecay_h, bd.at[1])),
        (I_QK, mw.at[y, :, 0:512], (wq_h, mw.at[y, :, 0:256]), (wk_h, mw.at[y, :, 256:512])),
        (I_VG, mv.at[y], (wv_h, mv.at[y, :, 0:512]), (wg_h, mv.at[y, :, 512:VGC])),
        (I_WO, wo.at[y], (wo_h, wo.at[y])),
        (I_W2, w2, (gate2_h, w2.at[0]), (up2_h, w2.at[1])),
        (I_D2, d2.at[y], (down2_h, d2.at[y])),
        (I_RB, rb, (rate_h, rb.at[0]), (bias_h, rb.at[1])),
        (I_HEAD, hgain, (hgain_h, hgain)),
        (I_STATE, s_buf, (state, s_buf)),
    )

    def fetch(groups):
        for i, _, *copies in groups:
            for src, dst in copies:
                pltpu.make_async_copy(src, dst, in_sem.at[i]).start()

    def ready(*groups):
        for i in groups:
            whole = inputs[i][1]
            pltpu.make_async_copy(whole, whole, in_sem.at[i]).wait()

    fetch(inputs[:3])

    barrier = pltpu.get_barrier_semaphore()
    greet = z_peers[:3] + plane_peers[:10] + z_peers[3:5] + plane_peers[10:] + z_peers[5:]
    for _, peer in greet:
        pl.semaphore_signal(barrier, inc=1, device_id=peer, device_id_type=MESH)

    counted = []

    def put(src, dst, k, peer, by=TILES):
        if by == TILES:
            counted.append(src.size * src.dtype.itemsize)
        pltpu.make_async_remote_copy(
            src_ref=src, dst_ref=dst, send_sem=send.at[by], recv_sem=recv.at[k], device_id=peer, device_id_type=MESH
        ).start()

    def arrived(part, k):
        pltpu.make_async_copy(part, part, recv.at[k]).wait()

    def left(part, k):
        pltpu.make_async_copy(part, part, send.at[k]).wait()

    def share(buf, own, k, peers, by=TILES):
        for _, peer in peers:
            put(buf.at[own], buf.at[own], k, peer, by)

    def deal(src, dst, own, k, peers):
        for p, peer in peers:
            put(src.at[p], dst.at[own], k, peer)
        dst[own] = src[own]

    above, below = (z * NY + ys[1], t), (z * NY + ys[3], t)

    def y_start(buf, k, by=TILES):
        put(buf.at[y], buf.at[y], k, above, by)
        put(buf.at[y], buf.at[y], k, below, by)

    def halves(buf, p):
        n = buf.shape[1] // 2
        return buf.at[p, pl.ds(0, n)], buf.at[p, pl.ds(n, n)]

    def y_pass(buf, k, by=TILES):
        arrived(buf.at[pl.ds(0, 2)], k)
        first, _ = halves(buf, ys[3])
        put(first, first, k + 1, above, by)
        _, second = halves(buf, ys[1])
        put(second, second, k + 1, below, by)

    def y_done(buf, k):
        arrived(buf.at[0], k + 1)

    lane = iota((64, FFP), 1)
    pos = lane - PITCH * sum(jnp.where(lane >= PITCH * p, 1, 0) for p in range(1, NY))

    def spread(v):
        v = jnp.concatenate([v.astype(F32), jnp.zeros((64, FFP - FFT), F32)], axis=1)
        w = v
        for p in range(1, NY):
            w = jnp.where(lane >= PITCH * p, pltpu.roll(v, (PITCH - HID) * p, 1), w)
        return jnp.where(pos < HID, w, 0.0)

    ready(I_W1)
    gate, up = spread(w1[0]), spread(w1[1])
    first = iota((64, 2 * PITCH), 1) < PITCH
    for h in range(2):
        a = gate[:, 2 * PITCH * h : 2 * PITCH * (h + 1)]
        b = pltpu.roll(up[:, 2 * PITCH * h : 2 * PITCH * (h + 1)], PITCH, 1)
        gu_src[2 * h] = jnp.where(first, a, b).astype(BF)
        gu_src[2 * h + 1] = jnp.where(first, b, a).astype(BF)
    ready(I_RES, I_GAIN)
    xg[me] = res[...]
    gn[y, 0:1] = gains[0]
    gn[y, 1:2] = gains[1]
    gn[y, 2:3] = gains[2]

    pl.semaphore_wait(barrier, len(greet))

    share(gn, y, GN, y_peers, GAINS)
    share(xg, me, X1, plane_peers)
    deal(gu_src, gu_rcv, y, GU1, y_peers)

    fetch(inputs[3:])
    ready(I_DOWN)
    d1[y] = spread(w1[2]).astype(BF)
    sel_b = one_hot((iota((32, 128), 0) == iota((32, 128), 1) + 4 * t) & (iota((32, 128), 1) < 4))
    sel_d = one_hot((iota((32, 128), 0) == iota((32, 128), 1) - 4 + 4 * t) & (iota((32, 128), 1) >= 4) & (iota((32, 128), 1) < 8))
    ready(I_BD)
    mw[y, :, 512:QK] = (dot(bd[0], sel_b, 0, 0) + dot(bd[1], sel_d, 0, 0)).astype(BF)

    eye64 = iota((64, 64), 0) == iota((64, 64), 1)
    lane64 = iota((64, 128), 1)

    def column(p, i):
        row = gn[p, i : i + 1]
        return jnp.sum(jnp.where(eye64, jnp.broadcast_to(row, (64, 64)), 0.0), axis=1, keepdims=True)

    arrived(gn.at[pl.ds(0, NY - 1)], GN)
    for i in range(3):
        for h in range(2):
            wide = jnp.where(lane64 == iota((64, 128), 0), column(2 * h, i), 0.0)
            wide = wide + jnp.where(lane64 == iota((64, 128), 0) + 64, column(2 * h + 1, i), 0.0)
            g_row[i, :, 128 * h : 128 * (h + 1)] = jnp.broadcast_to(jnp.sum(wide, axis=0, keepdims=True), (8, 128))

    def scaled_of(v, i):
        squares = jnp.sum(v * v, axis=1, keepdims=True)
        coarse = squares.astype(BF).astype(F32)
        return (v * g_row[i, 0:1]).astype(BF), coarse, squares - coarse

    arrived(xg.at[pl.ds(0, PLANE - 1)], X1)
    x0 = jnp.transpose(xg[...].astype(F32).reshape(ROWS, ROWS))
    scaled, coarse, fine = scaled_of(x0, 0)
    arrived(gu_rcv.at[pl.ds(0, NY - 1)], GU1)
    part = dot(scaled, gu_rcv[...].reshape(ROWS, 2 * PITCH), 1, 0)
    at = iota((ROWS, 2 * PITCH), 1)
    part = part + jnp.where(at == HID, coarse, 0.0) + jnp.where(at == HID + 1, fine, 0.0)
    f_src[...] = part.reshape(KV, 8, 2 * PITCH).astype(BF)
    deal(f_src, f_rcv, kv, RS1, kv_peers)
    y_start(d1, D1)
    ready(I_QK)
    y_start(mw, MW)
    xrow[...] = x0.reshape(NZ, NY, 8, ROWS).astype(BF)
    y_pass(d1, D1)
    ready(I_VG)
    y_start(mv, MV)
    arrived(f_rcv.at[pl.ds(0, KV - 1)], RS1)
    quarters = jnp.sum(f_rcv[...].astype(F32).reshape(NZ, NY, 8, 2 * PITCH), axis=0)
    scale = lax.rsqrt((quarters[0, :, HID : HID + 1] + quarters[0, :, HID + 1 : HID + 2]) / D + EPS)
    at = iota((8, 2 * PITCH), 1)
    pos = at - PITCH * jnp.where(at >= PITCH, 1, 0)
    for h in range(2):
        a, b = quarters[2 * h], quarters[2 * h + 1]
        gate = jnp.where(at < PITCH, a, b) * scale
        up = pltpu.roll(jnp.where(at < PITCH, b, a), PITCH, 1) * scale
        hg[0, z, :, 2 * PITCH * h : 2 * PITCH * (h + 1)] = jnp.where(pos < HID, silu(gate) * up, 0.0).astype(BF)
    share(hg.at[0], z, AG1, z_peers)
    y_pass(mw, MW)
    y_done(d1, D1)

    def gathered_hidden(i, k):
        arrived(hg.at[i, pl.ds(0, NZ - 1)], k)
        return hg[i].astype(F32).reshape(64, FFP).astype(BF)

    def swap(part, i, k, between):
        pa_src[i] = part.reshape(2, 4, 8, ROWS).astype(BF)
        put(pa_src.at[i, 1 - core], pa_rcv.at[i], k, (kv, ts[0][1]))
        mine = jnp.where(core == 0, part[0:32], part[32:64])
        between()
        arrived(pa_rcv.at[i], k)
        pb[i, t] = (mine.reshape(4, 8, ROWS) + pa_rcv[i].astype(F32)).astype(BF)

    def everyones(i, k):
        arrived(pb.at[i, pl.ds(0, NT - 1)], k)
        branch = []
        for c in range(2):
            half = pb[i, c].astype(F32)
            for j in range(1, 4):
                half = half + pb[i, 2 * j + c].astype(F32)
            branch.append(half.reshape(32, ROWS))
        return jnp.concatenate(branch, axis=0)

    h = gathered_hidden(0, AG1)
    swap(dot(h, d1[...].reshape(ROWS, FFP), 1, 1), 0, PR1, lambda: y_pass(mv, MV))
    share(pb.at[0], t, X2, t_peers)
    y_done(mw, MW)
    x1 = xrow[:, y].astype(F32).reshape(64, ROWS)
    x1 = (x1 + 0.5 * everyones(0, X2)).astype(BF).astype(F32)
    scaled, coarse, fine = scaled_of(x1, 1)
    last = iota((64, 128), 1)
    part = dot(scaled, mw[:, :, 512:QK].reshape(ROWS, 128), 1, 0)
    part = part + jnp.where(last == 8, coarse, 0.0) + jnp.where(last == 9, fine, 0.0)
    e_src[...] = part.reshape(NZ, 8, 128).astype(BF)
    deal(e_src, e_rcv, z, EXT, z_peers)
    part = dot(scaled, mw[:, :, 0:512].reshape(ROWS, 512), 1, 0)
    m_src[...] = part.reshape(NZ, 8, 512).astype(BF)
    deal(m_src, m_rcv, z, MIX, z_peers)
    y_done(mv, MV)
    part = dot(scaled, mv[...].reshape(ROWS, VGC), 1, 0)
    v_src[...] = part.reshape(NZ, 8, 1024).astype(BF)
    deal(v_src, v_rcv, z, VG, z_peers)
    ready(I_WO, I_W2, I_D2, I_RB, I_HEAD, I_STATE)
    y_start(wo, WO)
    gu2[y] = jnp.concatenate([w2[0].astype(F32), w2[1].astype(F32)], axis=1).astype(BF)
    y_start(gu2, GU2)
    arrived(e_rcv.at[pl.ds(0, NZ - 1)], EXT)
    ext = jnp.sum(e_rcv[...].astype(F32), axis=0)
    rowscale = lax.rsqrt((ext[:, 8:9] + ext[:, 9:10]) / D + EPS)
    arrived(m_rcv.at[pl.ds(0, NZ - 1)], MIX)
    mixed = jnp.sum(m_rcv[...].astype(F32), axis=0)
    heads = [mixed[:, 128 * i : 128 * (i + 1)] * rowscale for i in range(4)]

    def factor(v):
        return lax.rsqrt(jnp.sum(v * v, axis=-1, keepdims=True) + EPS)

    q = [silu(heads[m]) for m in range(2)]
    k = [silu(heads[2 + m]) for m in range(2)]
    q_t = [jnp.transpose(v) for v in q]
    k_t = [jnp.transpose(v) for v in k]
    q_f = [factor(v) * HEAD**-0.5 for v in q]
    k_f = [factor(v) for v in k]
    kq = [jnp.sum(k[m] * q[m], axis=-1, keepdims=True) * k_f[m] * q_f[m] for m in range(2)]
    ext = ext * rowscale
    by_k, by_q = [[] for _ in range(4)], [[] for _ in range(4)]
    for m in range(2):
        for i in range(8):
            k_col = jnp.broadcast_to(k_t[m][:, i : i + 1], (HEAD, HEAD))
            q_col = jnp.broadcast_to(q_t[m][:, i : i + 1], (HEAD, HEAD))
            for h in (2 * m, 2 * m + 1):
                s = s_buf[i, h]
                by_k[h].append(jnp.sum(s * k_col, axis=0, keepdims=True))
                by_q[h].append(jnp.sum(s * q_col, axis=0, keepdims=True))
    gates = []
    for h in range(4):
        beta = 1.0 / (1.0 + jnp.exp(-ext[:, h : h + 1]))
        pre = ext[:, 4 + h : 5 + h] + rb[1, :, h : h + 1]
        soft = jnp.maximum(pre, 0.0) + jnp.log1p(jnp.exp(-jnp.abs(pre)))
        decay = jnp.exp(-jnp.exp(rb[0, :, h : h + 1]) * soft)
        by_k[h] = decay * k_f[h // 2] * jnp.concatenate(by_k[h], axis=0)
        by_q[h] = decay * q_f[h // 2] * jnp.concatenate(by_q[h], axis=0)
        gates.append((beta, decay))
    arrived(v_rcv.at[pl.ds(0, NZ - 1)], VG)
    mixed = jnp.sum(v_rcv[...].astype(F32), axis=0)
    heads = [mixed[:, 128 * i : 128 * (i + 1)] * rowscale for i in range(8)]
    new = []
    for h in range(4):
        m = h // 2
        beta, decay = gates[h]
        val = silu(heads[h])
        gate = silu(heads[4 + h])
        corr = beta * (val - by_k[h])
        reading = by_q[h] + kq[m] * corr
        norm = lax.rsqrt(jnp.mean(reading * reading, axis=-1, keepdims=True) + EPS)
        nb[z, :, 128 * h : 128 * (h + 1)] = (reading * norm * hgain[...] * gate).astype(BF)
        new.append((decay, corr * k_f[m]))
    share(nb, z, NRM, z_peers)
    y_pass(wo, WO)
    y_pass(gu2, GU2)
    y_start(d2, D2, DOWN2)
    for i in range(8):
        for m in range(2):
            k_col = jnp.broadcast_to(k_t[m][:, i : i + 1], (HEAD, HEAD))
            for h in (2 * m, 2 * m + 1):
                decay, corr = new[h]
                state_out[i, h] = s_buf[i, h] * decay[i : i + 1] + k_col * corr[i : i + 1]
    y_done(wo, WO)
    arrived(nb.at[pl.ds(0, NZ - 1)], NRM)
    normed = nb[...].astype(F32).reshape(64, 512).astype(BF)
    part = dot(normed, wo[...].reshape(ROWS, 512), 1, 1)
    swap(part, 1, PR2, lambda: None)
    share(pb.at[1], t, X3, t_peers)
    y_done(gu2, GU2)

    x3 = (x1 + everyones(1, X3)).astype(BF).astype(F32)
    scaled, coarse, fine = scaled_of(x3, 2)
    squares = jnp.where(last == 0, coarse, jnp.where(last == 1, fine, 0.0))
    sq_src[...] = squares.reshape(NZ, 8, 128).astype(BF)
    deal(sq_src, sq_rcv, z, SQ, z_peers)
    part = dot(scaled, gu2[...].reshape(ROWS, 2 * FFT), 1, 0)
    rs2_src[...] = part.reshape(NZ, 8, 2 * FFT).astype(BF)
    deal(rs2_src, rs2_rcv, z, RS2, z_peers)
    y_pass(d2, D2, DOWN2)
    x3_t = jnp.transpose(jnp.concatenate([jnp.zeros((64, ROWS), F32), x3], axis=0))
    arrived(sq_rcv.at[pl.ds(0, NZ - 1)], SQ)
    squares = jnp.sum(sq_rcv[...].astype(F32), axis=0)
    scale = lax.rsqrt((squares[:, 0:1] + squares[:, 1:2]) / D + EPS)
    arrived(rs2_rcv.at[pl.ds(0, NZ - 1)], RS2)
    both = jnp.sum(rs2_rcv[...].astype(F32), axis=0) * scale
    hidden = silu(both[:, 0:FFT]) * both[:, FFT:]
    hg[1, z] = jnp.concatenate([hidden, jnp.zeros((8, FFP - FFT), F32)], axis=1).astype(BF)
    share(hg.at[1], z, AG2, z_peers)
    y_done(d2, D2)
    h = gathered_hidden(1, AG2)[:, 0:FFT]
    h = jnp.concatenate([h, jnp.zeros((64, FFT), BF)], axis=0)
    part = dot(d2[...].reshape(ROWS, FFT), h, 1, 1) + x3_t
    pr3_src[...] = part.reshape(PLANE, 8, 128).astype(BF)
    deal(pr3_src, pr3_rcv, me, PR3, plane_peers)
    arrived(pr3_rcv.at[pl.ds(0, PLANE - 1)], PR3)
    for p in range(NY):
        total = jnp.sum(pr3_rcv[NT * p : NT * (p + 1)].astype(F32), axis=0)
        base = pltpu.roll(pr3_rcv[NT * p].astype(F32), 64, 1)
        out[:, 128 * p : 128 * (p + 1)] = (base + 0.5 * total).astype(BF)
    assert sum(counted) == SENT * 2048, sum(counted) / 2048
    left(tiles, TILES)
    left(gn.at[pl.ds(0, NY - 1)], GAINS)
    left(d2.at[pl.ds(0, NY - 1)], DOWN2)


def deliver(out_in, state_in, out, state_out, placed, sems):
    copies = [pltpu.make_async_copy(state_in, state_out, sems.at[0])]
    copies[0].start()
    line, b = iota((128, ROWS), 0), iota((128, ROWS), 1)
    final = jnp.zeros((8, ROWS), F32)
    for p in range(NY):
        place = one_hot((b == line + 24 * lax.shift_right_logical(line, 3) + 8 * p) & (line < 64))
        final = final + dot(out_in[:, 128 * p : 128 * (p + 1)], place, 1, 0)
    placed[...] = final.astype(BF)
    copies.append(pltpu.make_async_copy(placed, out, sems.at[1]))
    copies[-1].start()
    for copy in copies:
        copy.wait()


def layer(res, state, gain1, gate1, up1, down1, gain2, wq, wk, wv, wg, wbeta, wdecay, rate, bias, hgain, wo, gain3, gate2, up2, down2):
    vmem = pl.BlockSpec(memory_space=pltpu.VMEM)
    args = (
        res.T, state, gain1[None], gain2[None], gain3[None], gate1, up1, down1.T, gate2, up2, down2.T,
        wq, wk, wv, wg, wbeta.T, wdecay.T, rate[None], bias[None], hgain[None], wo.T,
    )
    args = tuple(pltpu.with_memory_space_constraint(a, pltpu.HBM) for a in args)
    hbm = pl.BlockSpec(memory_space=pltpu.HBM)
    shapes = (jax.ShapeDtypeStruct((8, ROWS), BF), jax.ShapeDtypeStruct(state.shape, F32))
    out, new_state = pl.pallas_call(
        kernel,
        out_shape=(pltpu.VMEM((8, NY * 128), BF), pltpu.VMEM(state.shape, F32)),
        in_specs=[hbm] * len(args),
        out_specs=(vmem, vmem),
        scratch_shapes=[
            pltpu.VMEM((8, ROWS), BF),
            pltpu.VMEM(state.shape, F32),
            pltpu.VMEM((3, 1, 64), F32),
            pltpu.VMEM((3, 64, FFT), BF),
            pltpu.VMEM((2, 64, FFT), BF),
            pltpu.VMEM((2, 32, 64), BF),
            pltpu.VMEM((2, 1, 4), F32),
            pltpu.VMEM((1, HEAD), F32),
            pltpu.SemaphoreType.DMA((13,)),
            pltpu.SemaphoreType.DMA((3,)),
            pltpu.SemaphoreType.DMA((29,)),
            pltpu.VMEM((SENT, 8, 128), BF),
            pltpu.VMEM((NY, 64, 2 * PITCH), BF),
            pltpu.VMEM((NY, 64, 2 * PITCH), BF),
            pltpu.VMEM((NY, 8, 64), F32),
            pltpu.VMEM((NY, 64, FFP), BF),
            pltpu.VMEM((NY, 64, QK), BF),
            pltpu.VMEM((NY, 64, VGC), BF),
            pltpu.VMEM((NY, 64, 512), BF),
            pltpu.VMEM((NY, 64, 2 * FFT), BF),
            pltpu.VMEM((NY, 64, FFT), BF),
            pltpu.VMEM((3, 8, ROWS), F32),
            pltpu.VMEM((NZ, NY, 8, ROWS), BF),
            pltpu.VMEM((PLANE, 8, ROWS), BF),
            pltpu.VMEM((KV, 8, 2 * PITCH), BF),
            pltpu.VMEM((KV, 8, 2 * PITCH), BF),
            pltpu.VMEM((2, NZ, 8, FFP), BF),
            pltpu.VMEM((2, 2, 4, 8, ROWS), BF),
            pltpu.VMEM((2, 4, 8, ROWS), BF),
            pltpu.VMEM((2, NT, 4, 8, ROWS), BF),
            pltpu.VMEM((NZ, 8, 512), BF),
            pltpu.VMEM((NZ, 8, 512), BF),
            pltpu.VMEM((NZ, 8, 128), BF),
            pltpu.VMEM((NZ, 8, 128), BF),
            pltpu.VMEM((NZ, 8, 1024), BF),
            pltpu.VMEM((NZ, 8, 1024), BF),
            pltpu.VMEM((NZ, 8, 512), BF),
            pltpu.VMEM((NZ, 8, 128), BF),
            pltpu.VMEM((NZ, 8, 128), BF),
            pltpu.VMEM((NZ, 8, 2 * FFT), BF),
            pltpu.VMEM((NZ, 8, 2 * FFT), BF),
            pltpu.VMEM((PLANE, 8, 128), BF),
            pltpu.VMEM((PLANE, 8, 128), BF),
        ],
        compiler_params=pltpu.CompilerParams(collective_id=0, has_side_effects=True, vmem_limit_bytes=40 << 20),
    )(*args)
    out, new_state = pl.pallas_call(
        deliver,
        out_shape=shapes,
        in_specs=[vmem, vmem],
        out_specs=(hbm, hbm),
        scratch_shapes=[pltpu.VMEM((8, ROWS), BF), pltpu.SemaphoreType.DMA((2,))],
        compiler_params=pltpu.CompilerParams(vmem_limit_bytes=40 << 20),
    )(out, new_state)
    return out.T, new_state


def solution(mesh):
    placed = (
        P(None, ("kv", "tp")),
        P("kv", "tp", None, None),
        P("kv"),
        P("kv", "tp"),
        P("kv", "tp"),
        P("tp", "kv"),
        P("kv"),
        P("kv", "tp"),
        P("kv", "tp"),
        P("kv", "tp"),
        P("kv", "tp"),
        P("kv", None),
        P("kv", None),
        P("tp"),
        P("tp"),
        P(),
        P("tp", "kv"),
        P("kv"),
        P("kv", "tp"),
        P("kv", "tp"),
        P("tp", "kv"),
    )
    return jax.shard_map(
        layer,
        mesh=mesh,
        in_specs=placed,
        out_specs=(P(None, ("kv", "tp")), P("kv", "tp", None, None)),
        check_vma=False,
    )
```
